32 devices in a mesh: ep: 4 (over z), tp: 8 (over y, x, core).
Axes of the slice: x: 2, y: 2, z: 4, core: 2. Of those that a mesh axis runs over, the one named last changes fastest.
Arguments:
- tokens: bfloat16 [256, 4096], P('ep', 'tp'), may hold values from -24 to 24, as said below
- state_real: float32 [256, 128, 64], P('ep', 'tp'), may hold values from -3 to 3
- state_imag: float32 [256, 128, 64], P('ep', 'tp'), may hold values from -3 to 3
- mix_gain: bfloat16 [4096], replicated, may hold values from 0.099609375 to 1.8984375
- in_weight: bfloat16 [2048, 4096], P('tp'), may hold values from -0.09375 to 0.09375
- eig_real: float32 [128, 64], P('tp'), may hold values from -1 to -0.1
- eig_imag: float32 [128, 64], P('tp'), may hold values from 0 to 200
- log_step: float32 [128], P('tp'), may hold values from -4 to 0
- input_real: float32 [128, 64, 16], P('tp'), may hold values from -1 to 1
- input_imag: float32 [128, 64, 16], P('tp'), may hold values from -1 to 1
- output_matrix_real: float32 [128, 16, 64], P('tp'), may hold values from -0.5 to 0.5
- output_matrix_imag: float32 [128, 16, 64], P('tp'), may hold values from -0.5 to 0.5
- skip_weight: float32 [2048], P('tp'), may hold values from -3 to 3
- glu_weight: bfloat16 [2048, 2048], P('tp'), may hold values from -0.375 to 0.375
- glu_bias: float32 [2048], P('tp'), may hold values from -3 to 3
- out_weight: bfloat16 [2048, 4096], P('tp'), may hold values from -0.25 to 0.25
- moe_gain: bfloat16 [4096], replicated, may hold values from 0.099609375 to 1.8984375
- routes: int32 [256, 2], P('ep'), may hold values from 0 to 7, all different within a row; in each aligned block of 64 rows (0 to 63, 64 to 127, ...) at most 24 rows name the same one
- route_weight: float32 [256, 2], P('ep'), may hold values from 0.2 to 1
- gate_weight: bfloat16 [8, 2048, 4096], P('ep', 'tp'), may hold values from -0.09375 to 0.09375
- up_weight: bfloat16 [8, 2048, 4096], P('ep', 'tp'), may hold values from -0.09375 to 0.09375
- down_weight: bfloat16 [8, 2048, 4096], P('ep', 'tp'), may hold values from -0.125 to 0.125
Outputs:
- result: bfloat16 [256, 4096], P('ep', 'tp')
- updated_state_real: float32 [256, 128, 64], P('ep', 'tp')
- updated_state_imag: float32 [256, 128, 64], P('ep', 'tp')
The draws below stay inside these ranges and needn't reach their ends.
Inputs may be any that keep to these rules, and one draw needn't show every extreme that they name: `routes`: each row names 2 different experts. Among the rows of one index of ep, no expert is named by more than 24 rows, a bound that some expert reaches in some such blocks. `tokens`: feature blocks of the stream have scales that differ by up to a factor of ten.
All inputs are finite; a program needn't handle non-finite values.
Results may differ from the reference program's by a relative error of at most 0.013.
Values may be sent and summed in bfloat16 or wider, within the bound.
No kernel may reach another device: no remote copies, remote signals or barrier semaphores. Data moves between devices by JAX's collectives and lax.ppermute only.
A program may use at most 64 MiB of HBM per device.

```python
import math
import jax
import jax.numpy as jnp
import numpy as np
from jax import lax

D = 4096
S5_GROUP = 16
S5_GROUPS = 128
S5_STATE = 64
S5_WIDTH = 2048
D_EXPERT = 2048
EXPERTS = 8
TOP = 2
B_DEV = 64
TOKENS = 256
CAP = 24
N_EP = 4
N_TP = 8


def draw_tokens(key, part):
    key_base = jax.random.fold_in(key, 11)
    key_scale = jax.random.fold_in(key, 12)
    block_scale = jnp.exp(jax.random.uniform(key_scale, (32,), jnp.float32, math.log(0.3), math.log(3.0)))
    col_scale = jnp.repeat(block_scale, D // 32)
    base = jnp.clip(jax.random.normal(key_base, (TOKENS, D), jnp.float32), -4.0, 4.0)
    return (base * col_scale[None, :]).astype(jnp.bfloat16)


def steps_of(stream_key, dims, shards, low, top_value):
    loudness = 1.0
    for axis_at, parts in shards:
        heights = jax.random.uniform(jax.random.fold_in(jax.random.fold_in(stream_key, 6), axis_at), (parts,), jnp.float32, low / len(shards), top_value / len(shards))
        loudness = loudness * jnp.repeat(jnp.exp(heights), dims[axis_at] // parts).reshape((-1,) + (1,) * (len(dims) - 1 - axis_at))
    return loudness


def shared_out(key, own, number, rows, amount, top, reach, skew):
    ranking = jax.random.permutation(key, amount)
    crowded, usual = portions_of(amount, rows * top, reach, skew, True), portions_of(amount, rows * top, reach, skew, False)
    places = jnp.arange(amount)

    def named(sizes, rotation):
        used = int((sizes > 0).sum())
        fixed = max(1, used // 4)
        passed = fixed + (places - fixed + rotation * (used - fixed)) % max(1, amount - fixed)
        return jnp.zeros((amount,), jnp.int32).at[ranking[jnp.where(places < fixed, places, passed)]].set(jnp.asarray(sizes, jnp.int32))

    sizes = jnp.where(number % 4 == 0, named(crowded, number // 4), named(usual, number - number // 4 - 1))
    mixed = jax.random.permutation(jax.random.fold_in(own, 3), amount)
    source_of, sink = mixed[0:amount // 2 * 2:2], mixed[1:amount // 2 * 2:2]
    margin = jnp.minimum(sizes[source_of] - 1, reach - sizes[sink]) // 2
    margin = jnp.where((source_of == ranking[0]) | (sink == ranking[0]) | (sizes[sink] == 0), 0, jnp.maximum(margin, 0))
    passed = jax.random.randint(jax.random.fold_in(own, 4), (amount // 2,), 0, 1 << 20) % (margin + 1)
    sizes = sizes.at[source_of].add(-passed).at[sink].add(passed)
    members = jnp.searchsorted(jnp.cumsum(sizes), jnp.arange(rows * top), side="right").astype(jnp.int32)
    listing = members.reshape(top, rows).T
    listing = listing[jax.random.permutation(jax.random.fold_in(own, 1), rows)]
    rotation = jax.random.randint(jax.random.fold_in(own, 2), (rows, 1), 0, top)
    return jnp.take_along_axis(listing, (jnp.arange(top)[None, :] + rotation) % top, axis=1)


def portions_of(count, total, most, slope, full):
    portions = [(1 << 20) // math.isqrt(rank ** slope) + 1 for rank in range(1, count + 1)]
    largest = most if full else min(most, max(-(-total // count), total * portions[0] // sum(portions)))
    least = 1 if total - largest >= count - 1 else 0
    holding, spare = [largest] + [least] * (count - 1), total - largest - least * (count - 1)
    while spare > 0:
        free = [i for i in range(1, count) if holding[i] < largest] or [i for i in range(1, count) if holding[i] < most]
        whole, budget = sum([portions[i] for i in free]), spare
        for i in free:
            addition = min(most - holding[i], max(1, budget * portions[i] // whole), spare)
            holding[i] = holding[i] + addition
            spare = spare - addition
    return np.array(holding)


def bell_draw(rng, extent, width, limit, shards=(), held_as=jnp.bfloat16):
    array = width * jax.random.normal(rng, extent, jnp.float32)
    if shards:
        array = array * steps_of(rng, extent, shards, -0.22, 0.18)
    return jnp.clip(array, -limit, limit).astype(held_as)


def setup_inputs(seed: int = 0) -> dict:
    streams_of = jax.random.split(jax.random.key(seed), 23)
    tokens = draw_tokens(jax.random.fold_in(streams_of[22], 71), 0)
    state_real = bell_draw(streams_of[1], (TOKENS, S5_GROUPS, S5_STATE), 0.5, 3.0, ((0, 4), (1, 8)), jnp.float32)
    state_imag = bell_draw(streams_of[2], (TOKENS, S5_GROUPS, S5_STATE), 0.5, 3.0, ((0, 4), (1, 8)), jnp.float32)
    mix_gain = jnp.clip(1.0 + 0.18 * jax.random.normal(streams_of[3], (D,), jnp.float32), 0.099609375, 1.8984375).astype(jnp.bfloat16)
    in_weight = bell_draw(streams_of[4], (S5_WIDTH, D), D ** -0.5, 0.09375, ((0, 8),))
    eig_real = jnp.clip(-1.0 + 0.9 * jax.random.uniform(streams_of[5], (S5_GROUPS, S5_STATE), jnp.float32) ** steps_of(streams_of[5], (S5_GROUPS, S5_STATE), ((0, 8),), -0.2, 0.2), -1.0, -0.1)
    eig_imag = jnp.clip(200.0 * jax.random.uniform(streams_of[6], (S5_GROUPS, S5_STATE), jnp.float32) ** steps_of(streams_of[6], (S5_GROUPS, S5_STATE), ((0, 8),), -0.2, 0.2), 0.0, 200.0)
    log_step = jnp.clip(-4.0 + 4.0 * jax.random.uniform(streams_of[7], (S5_GROUPS,), jnp.float32) ** steps_of(streams_of[7], (S5_GROUPS,), ((0, 8),), -0.2, 0.2), -4.0, 0.0)
    input_real = bell_draw(streams_of[8], (S5_GROUPS, S5_STATE, S5_GROUP), (2 * S5_GROUP) ** -0.5, 1.0, ((0, 8),), jnp.float32)
    input_imag = bell_draw(streams_of[9], (S5_GROUPS, S5_STATE, S5_GROUP), (2 * S5_GROUP) ** -0.5, 1.0, ((0, 8),), jnp.float32)
    output_matrix_real = bell_draw(streams_of[10], (S5_GROUPS, S5_GROUP, S5_STATE), (2 * S5_STATE) ** -0.5, 0.5, ((0, 8),), jnp.float32)
    output_matrix_imag = bell_draw(streams_of[11], (S5_GROUPS, S5_GROUP, S5_STATE), (2 * S5_STATE) ** -0.5, 0.5, ((0, 8),), jnp.float32)
    skip_weight = bell_draw(streams_of[12], (S5_WIDTH,), 0.5, 3.0, ((0, 8),), jnp.float32)
    glu_weight = bell_draw(streams_of[13], (S5_WIDTH, S5_WIDTH), (S5_WIDTH // 8) ** -0.5, 0.375, ((0, 8),))
    glu_bias = bell_draw(streams_of[14], (S5_WIDTH,), 1.0, 3.0, ((0, 8),), jnp.float32)
    out_weight = bell_draw(streams_of[15], (S5_WIDTH, D), (S5_WIDTH // 4) ** -0.5, 0.25, ((0, 8),))
    moe_gain = jnp.clip(1.0 + 0.18 * jax.random.normal(streams_of[16], (D,), jnp.float32), 0.099609375, 1.8984375).astype(jnp.bfloat16)
    routes_keys = jax.random.split(jax.random.fold_in(streams_of[17], 1), TOKENS // B_DEV)
    routes_turns = jax.random.permutation(jax.random.fold_in(streams_of[17], 3), TOKENS // B_DEV)
    routes = jax.vmap(lambda own, number: shared_out(jax.random.fold_in(streams_of[17], 2), own, number, B_DEV, EXPERTS, TOP, CAP, 2))(routes_keys, routes_turns).reshape((TOKENS, TOP))
    route_weight = jnp.clip(0.2 + 0.8 * jax.random.uniform(streams_of[18], (TOKENS, TOP), jnp.float32) ** steps_of(streams_of[18], (TOKENS, TOP), ((0, 4),), -0.2, 0.2), 0.2, 1.0)
    gate_weight = bell_draw(streams_of[19], (EXPERTS, D_EXPERT, D), D ** -0.5, 0.09375, ((0, 4), (1, 8)))
    up_weight = bell_draw(streams_of[20], (EXPERTS, D_EXPERT, D), D ** -0.5, 0.09375, ((0, 4), (1, 8)))
    down_weight = bell_draw(streams_of[21], (EXPERTS, D_EXPERT, D), D_EXPERT ** -0.5, 0.125, ((0, 4), (1, 8)))
    return {"tokens": tokens, "state_real": state_real, "state_imag": state_imag, "mix_gain": mix_gain, "in_weight": in_weight, "eig_real": eig_real, "eig_imag": eig_imag, "log_step": log_step, "input_real": input_real, "input_imag": input_imag, "output_matrix_real": output_matrix_real, "output_matrix_imag": output_matrix_imag, "skip_weight": skip_weight, "glu_weight": glu_weight, "glu_bias": glu_bias, "out_weight": out_weight, "moe_gain": moe_gain, "routes": routes, "route_weight": route_weight, "gate_weight": gate_weight, "up_weight": up_weight, "down_weight": down_weight}


norm_eps = 1e-06

def ssm_step(driven, state_real, state_imag, eig_real, eig_imag, log_step, input_real, input_imag, output_matrix_real, output_matrix_imag, skip_weight):
    highest_precision = lax.Precision.HIGHEST
    count_of_rows = driven.shape[0]
    groups = eig_real.shape[0]
    group_width = input_real.shape[2]
    time_step = jnp.exp(log_step)[:, None]
    magnitude = jnp.exp(eig_real * time_step)
    angle_now = eig_imag * time_step
    bar_real = magnitude * jnp.cos(angle_now)
    bar_imag = magnitude * jnp.sin(angle_now)
    modulus = eig_real * eig_real + eig_imag * eig_imag
    fac_real = ((bar_real - 1.0) * eig_real + bar_imag * eig_imag) / modulus
    fac_imag = (bar_imag * eig_real - (bar_real - 1.0) * eig_imag) / modulus
    ib_real = fac_real[..., None] * input_real - fac_imag[..., None] * input_imag
    ib_imag = fac_real[..., None] * input_imag + fac_imag[..., None] * input_real
    grouped = driven.astype(jnp.float32).reshape(count_of_rows, groups, group_width)
    push_real = jnp.einsum('gpc,ngc->ngp', ib_real, grouped, precision=highest_precision)
    push_imag = jnp.einsum('gpc,ngc->ngp', ib_imag, grouped, precision=highest_precision)
    updated_state_real = bar_real[None] * state_real - bar_imag[None] * state_imag + push_real
    updated_state_imag = bar_real[None] * state_imag + bar_imag[None] * state_real + push_imag
    state_readout = jnp.einsum('jiy,sjy->sji', output_matrix_real, updated_state_real, precision=highest_precision) - jnp.einsum('jiy,sjy->sji', output_matrix_imag, updated_state_imag, precision=highest_precision)
    state_readout = state_readout.reshape(count_of_rows, groups * group_width) + skip_weight[None, :] * driven.astype(jnp.float32)
    activated = jax.nn.gelu(state_readout).astype(jnp.bfloat16)
    return (updated_state_real, updated_state_imag, activated)

def block_sum(left_side, right_side, block_count):
    block_width = left_side.shape[1] // block_count
    left_blocks = left_side.reshape(left_side.shape[0], block_count, block_width).transpose(1, 0, 2)
    right_blocks = right_side.reshape(block_count, block_width, right_side.shape[1])

    def add_block(running, operands):
        partial_value = jnp.dot(operands[0], operands[1], preferred_element_type=jnp.float32).astype(jnp.bfloat16)
        return (running + partial_value.astype(jnp.float32), None)
    start_sum = jnp.zeros((left_side.shape[0], right_side.shape[1]), jnp.float32)
    running, _ = lax.scan(add_block, start_sum, (left_blocks, right_blocks))
    return running

def reference(tokens, state_real, state_imag, mix_gain, in_weight, eig_real, eig_imag, log_step, input_real, input_imag, output_matrix_real, output_matrix_imag, skip_weight, glu_weight, glu_bias, out_weight, moe_gain, routes, route_weight, gate_weight, up_weight, down_weight):
    token_float = tokens.astype(jnp.float32)
    first_scale = lax.rsqrt(lax.optimization_barrier(jnp.mean(token_float * token_float, axis=1, keepdims=True)) + norm_eps)
    normed = (token_float * first_scale * mix_gain.astype(jnp.float32)).astype(jnp.bfloat16)
    driven = jnp.dot(normed, in_weight.T, preferred_element_type=jnp.float32).astype(jnp.bfloat16)
    updated_state_real, updated_state_imag, activated = ssm_step(driven, state_real, state_imag, eig_real, eig_imag, log_step, input_real, input_imag, output_matrix_real, output_matrix_imag, skip_weight)
    gate_pre = jnp.dot(activated, glu_weight.T, preferred_element_type=jnp.float32) + glu_bias
    glued = (activated.astype(jnp.float32) * jax.nn.sigmoid(gate_pre)).astype(jnp.bfloat16)
    mixed = block_sum(glued, out_weight, N_TP)
    residual = (token_float + mixed).astype(jnp.bfloat16)
    resid_float = residual.astype(jnp.float32)
    second_scale = lax.rsqrt(lax.optimization_barrier(jnp.mean(resid_float * resid_float, axis=1, keepdims=True)) + norm_eps)
    expert_in = (resid_float * second_scale * moe_gain.astype(jnp.float32)).astype(jnp.bfloat16)
    experts = gate_weight.shape[0]
    token_count = routes.shape[0]
    per_block = token_count // N_EP
    chosen = routes.reshape(N_EP, per_block * TOP)
    onehot = (chosen[..., None] == jnp.arange(experts, dtype=jnp.int32)[None, None, :]).astype(jnp.int32)
    rank_index = lax.optimization_barrier(jnp.sum((jnp.cumsum(onehot, axis=1) - onehot) * onehot, axis=2))
    source = jnp.arange(N_EP, dtype=jnp.int32)[:, None]
    slot_index = (chosen * (N_EP * CAP) + source * CAP + rank_index).reshape(token_count, TOP).astype(jnp.int32)
    buffer = jnp.zeros((experts * N_EP * CAP, expert_in.shape[1]), jnp.bfloat16)
    buffer = buffer.at[slot_index.reshape(-1)].set(jnp.repeat(expert_in, TOP, axis=0))
    buffer = buffer.reshape(experts, N_EP * CAP, expert_in.shape[1])

    def run_expert(expert_item):
        expert_rows, gate_rows, up_rows, down_rows = expert_item
        gate_sum = jnp.dot(expert_rows, gate_rows.T, preferred_element_type=jnp.float32)
        up_sum = jnp.dot(expert_rows, up_rows.T, preferred_element_type=jnp.float32)
        hidden_width = (jax.nn.silu(gate_sum) * up_sum).astype(jnp.bfloat16)
        return block_sum(hidden_width, down_rows, N_TP).astype(jnp.bfloat16)
    results = lax.map(run_expert, (buffer, gate_weight, up_weight, down_weight))
    flattened = results.reshape(experts * N_EP * CAP, expert_in.shape[1])
    picked = flattened[slot_index]
    result = (resid_float + lax.optimization_barrier(jnp.sum(route_weight[..., None] * picked.astype(jnp.float32), axis=1))).astype(jnp.bfloat16)
    return (result, updated_state_real, updated_state_imag)
```

```python
import functools
import jax
import jax.numpy as jnp
from jax import lax
from jax.experimental import pallas as pl
from jax.experimental.pallas import tpu as pltpu
from jax.sharding import PartitionSpec as P

norm_eps = 1e-06
f32 = jnp.float32
bf16 = jnp.bfloat16
NT = (((1,), (1,)), ((), ()))
NN = (((1,), (0,)), ((), ()))
WHOLE = pl.BlockSpec(memory_space=pltpu.VMEM)
PLACE = pl.BlockSpec(memory_space=pl.ANY)


def dot(a, b, dims):
    return lax.dot_general(a, b, dims, preferred_element_type=f32)


def swap(x, axis, k):
    return lax.ppermute(x, axis, [(i, i ^ k) for i in range(lax.axis_size(axis))])


def gather_swaps(x, n):
    pieces = [None] * n
    pieces[0] = x
    for k in range(2, n, 2):
        pieces[k] = swap(x, "tp", k)
    for k in range(0, n, 2):
        pieces[k ^ 1] = swap(pieces[k], "tp", 1)
    return pieces


def reduce_swaps(parts, n):
    pair = [None] * n
    for k in range(0, n, 2):
        other = swap(parts[k ^ 1], "tp", 1)
        pair[k] = parts[k].astype(f32) + other.astype(f32)
    terms = [pair[0]]
    for k in range(2, n, 2):
        terms.append(swap(pair[k].astype(bf16), "tp", k))
    return terms


def call(body, out_shape, in_specs, scratch=(), limit=None, flops=10**7, name=None):
    single = not isinstance(out_shape, (list, tuple))
    return pl.pallas_call(
        body,
        out_shape=out_shape,
        in_specs=in_specs,
        out_specs=WHOLE if single else [WHOLE] * len(out_shape),
        scratch_shapes=list(scratch),
        compiler_params=pltpu.CompilerParams(vmem_limit_bytes=limit),
        cost_estimate=pl.CostEstimate(flops=flops, bytes_accessed=10**6, transcendentals=0),
        name=name,
    )


def place(k, width):
    return pl.ds(pl.multiple_of((lax.axis_index("tp") ^ k) * width, width), width)


def mixer_body(n, *refs):
    pieces = refs[:n]
    gain, weight, bt_r, bt_i, coef, st_r, st_i, cm_r, cm_i, skip = refs[n : n + 10]
    new_r_ref, new_i_ref, act_ref, rows = refs[n + 10 :]
    width = pieces[0].shape[1]
    for k in range(n):
        rows[:, place(k, width)] = pieces[k][...]
    x = rows[...].astype(f32)
    scale = lax.rsqrt(jnp.mean(x * x, axis=1, keepdims=True) + norm_eps)
    normed = (x * scale * gain[...].astype(f32)).astype(bf16)
    driven = dot(normed, weight[...], NT).astype(bf16)
    u_r = dot(driven, bt_r[...], NT)
    u_i = dot(driven, bt_i[...], NT)
    bar_r, bar_i = coef[0:1, :], coef[1:2, :]
    fac_r, fac_i = coef[2:3, :], coef[3:4, :]
    s_r, s_i = st_r[...], st_i[...]
    new_r = bar_r * s_r - bar_i * s_i + fac_r * u_r - fac_i * u_i
    new_i = bar_r * s_i + bar_i * s_r + fac_r * u_i + fac_i * u_r
    new_r_ref[...] = new_r
    new_i_ref[...] = new_i
    readout = dot(new_r.astype(bf16), cm_r[...], NT) - dot(new_i.astype(bf16), cm_i[...], NT)
    readout = readout + skip[...] * driven.astype(f32)
    act_ref[...] = jax.nn.gelu(readout).astype(bf16)


def glu_body(n, *refs):
    pieces = refs[:n]
    glu, bias, out_w = refs[n : n + 3]
    outs = refs[n + 3 : 2 * n + 3]
    rows = refs[2 * n + 3]
    width = pieces[0].shape[1]
    for k in range(n):
        rows[:, place(k, width)] = pieces[k][...]
    gate = dot(rows[...], glu[...], NT) + bias[...]
    glued = (pieces[0][...].astype(f32) * jax.nn.sigmoid(gate)).astype(bf16)
    wide = outs[0].shape[1]
    for k in range(n):
        outs[k][...] = dot(glued, out_w[:, place(k, wide)], NN).astype(bf16)


def dispatch_body(m, terms, *refs):
    tokens = refs[0]
    sums = refs[1 : 1 + terms]
    table = refs[1 + terms]
    resid_ref = refs[2 + terms]
    outs = refs[3 + terms :]
    mixed = sums[0][...]
    for s in sums[1:]:
        mixed = mixed + s[...].astype(f32)
    resid = (tokens[...].astype(f32) + mixed).astype(bf16)
    resid_ref[...] = resid
    experts, cap, wide = outs[0].shape
    count = experts * cap
    for j in range(m):
        at = pl.multiple_of((lax.axis_index("ep") ^ j) * count, count)
        picked = dot(table[pl.ds(at, count), :], resid, NN).astype(bf16)
        outs[j][...] = picked.reshape(experts, cap, wide)


def expert_body(n, *refs):
    pieces = refs[:n]
    gain, gate_hbm, up_hbm, down_hbm = refs[n : n + 4]
    outs = refs[n + 4 : 2 * n + 4]
    rows, gate_w, up_w, down_w, sems = refs[2 * n + 4 :]
    experts, count, width = pieces[0].shape
    copies = []
    for which, (src, dst) in enumerate(((gate_hbm, gate_w), (up_hbm, up_w), (down_hbm, down_w))):
        copies.append(
            [pltpu.make_async_copy(src.at[i], dst.at[i], sems.at[which, i]) for i in range(experts)]
        )
    for i in range(experts):
        copies[0][i].start()
        copies[1][i].start()
    for i in range(experts):
        copies[2][i].start()
    for k in range(n):
        rows[:, :, place(k, width)] = pieces[k][...]
    hidden = []
    for i in range(experts):
        x = rows[i].astype(f32)
        scale = lax.rsqrt(jnp.mean(x * x, axis=1, keepdims=True) + norm_eps)
        normed = (x * scale * gain[...].astype(f32)).astype(bf16)
        copies[0][i].wait()
        g = dot(normed, gate_w[i], NT)
        copies[1][i].wait()
        u = dot(normed, up_w[i], NT)
        hidden.append((jax.nn.silu(g) * u).astype(bf16))
    for i in range(experts):
        copies[2][i].wait()
        for k in range(n):
            outs[k][i] = dot(hidden[i], down_w[i, :, place(k, width)], NN).astype(bf16)


def total_body(m, terms, *refs):
    sums = refs[:terms]
    outs = refs[terms:]
    total = sums[0][...]
    for s in sums[1:]:
        total = total + s[...].astype(f32)
    total = total.astype(bf16)
    cap = outs[0].shape[1]
    for j in range(m):
        outs[j][...] = total[:, j * cap : (j + 1) * cap, :]


def combine_body(m, *refs):
    resid, choose, weight = refs[:3]
    back = refs[3 : 3 + m]
    out, rows = refs[3 + m :]
    experts, cap, wide = back[0].shape
    count = experts * cap
    for j in range(m):
        at = pl.multiple_of((lax.axis_index("ep") ^ j) * count, count)
        rows[pl.ds(at, count), :] = back[j][...].reshape(count, wide)
    picked = dot(choose[...], rows[...], NN)
    tokens = resid.shape[0]
    total = resid[...].astype(f32)
    for r in range(weight.shape[1]):
        total = total + weight[:, r : r + 1] * picked[r * tokens : (r + 1) * tokens]
    out[...] = total.astype(bf16)


def spread(blocks, inner, groups):
    rows = blocks.shape[0]
    columns = groups * inner
    copy = (jnp.arange(columns)[None, :] % inner == jnp.arange(inner)[:, None]).astype(bf16)
    wide = jnp.dot(blocks.astype(bf16), copy, preferred_element_type=f32)
    own = (jnp.arange(rows)[:, None] // (rows // groups)) == (jnp.arange(columns)[None, :] // inner)
    return jnp.where(own, wide, 0.0).astype(bf16)


def local_swaps(
    tokens,
    state_real,
    state_imag,
    mix_gain,
    in_weight,
    eig_real,
    eig_imag,
    log_step,
    input_real,
    input_imag,
    output_matrix_real,
    output_matrix_imag,
    skip_weight,
    glu_weight,
    glu_bias,
    out_weight,
    moe_gain,
    routes,
    route_weight,
    gate_weight,
    up_weight,
    down_weight,
):
    count, wide = tokens.shape
    n = lax.axis_size("tp")
    m = lax.axis_size("ep")
    groups, entries = eig_real.shape
    inner = input_real.shape[2]
    states = groups * entries
    channels = groups * inner
    full = wide * n
    exp_dev = gate_weight.shape[0]
    experts = exp_dev * m
    top = routes.shape[1]
    cap = max(2, (3 * top * count + 2 * experts - 1) // (2 * experts))
    slots = experts * cap

    pieces = gather_swaps(tokens, n)

    step = jnp.exp(log_step)[:, None]
    size = jnp.exp(eig_real * step)
    angle = eig_imag * step
    bar_r = size * jnp.cos(angle)
    bar_i = size * jnp.sin(angle)
    modulus = eig_real * eig_real + eig_imag * eig_imag
    fac_r = ((bar_r - 1.0) * eig_real + bar_i * eig_imag) / modulus
    fac_i = (bar_i * eig_real - (bar_r - 1.0) * eig_imag) / modulus
    coef = jnp.stack([bar_r, bar_i, fac_r, fac_i]).reshape(4, states)
    bt_r = spread(input_real.reshape(states, inner), inner, groups)
    bt_i = spread(input_imag.reshape(states, inner), inner, groups)
    cm_r = spread(output_matrix_real.reshape(channels, entries), entries, groups)
    cm_i = spread(output_matrix_imag.reshape(channels, entries), entries, groups)
    st_r = state_real.reshape(count, states)
    st_i = state_imag.reshape(count, states)

    chosen = routes.reshape(-1)
    onehot = (chosen[:, None] == jnp.arange(experts, dtype=jnp.int32)[None, :]).astype(jnp.int32)
    rank = jnp.sum((jnp.cumsum(onehot, axis=0) - onehot) * onehot, axis=1)
    slot = (chosen * cap + rank).reshape(count, top)
    names = jnp.arange(slots, dtype=jnp.int32)
    choose = (slot.T[:, :, None] == names[None, None, :]).astype(bf16).reshape(top * count, slots)
    hit = slot[None, :, :] == names[:, None, None]
    table = jnp.sum(hit.astype(f32), axis=2).astype(bf16)

    new_r, new_i, activated = call(
        functools.partial(mixer_body, n),
        [
            jax.ShapeDtypeStruct((count, states), f32),
            jax.ShapeDtypeStruct((count, states), f32),
            jax.ShapeDtypeStruct((count, channels), bf16),
        ],
        [WHOLE] * (n + 10),
        [pltpu.VMEM((count, full), bf16)],
        limit=24 * 2**20,
        name="mixer",
    )(
        *pieces,
        mix_gain.reshape(1, full),
        in_weight,
        bt_r,
        bt_i,
        coef,
        st_r,
        st_i,
        cm_r,
        cm_i,
        skip_weight.reshape(1, channels),
    )

    acts = gather_swaps(activated, n)
    parts = call(
        functools.partial(glu_body, n),
        [jax.ShapeDtypeStruct((count, wide), bf16)] * n,
        [WHOLE] * (n + 3),
        [pltpu.VMEM((count, channels * n), bf16)],
        limit=16 * 2**20,
        name="glu",
    )(*acts, glu_weight, glu_bias.reshape(1, channels), out_weight)

    terms = reduce_swaps(parts, n)
    resid, *packed = call(
        functools.partial(dispatch_body, m, len(terms)),
        [jax.ShapeDtypeStruct((count, wide), bf16)]
        + [jax.ShapeDtypeStruct((exp_dev, cap, wide), bf16)] * m,
        [WHOLE] * (2 + len(terms)),
        limit=8 * 2**20,
        name="dispatch",
    )(tokens, *terms, table)

    arrived = [packed[0]] + [swap(packed[j], "ep", j) for j in range(1, m)]
    arrived = jnp.concatenate(arrived, axis=1)
    fragments = gather_swaps(arrived, n)
    hidden = gate_weight.shape[1]
    outs = call(
        functools.partial(expert_body, n),
        [jax.ShapeDtypeStruct((exp_dev, m * cap, wide), bf16)] * n,
        [WHOLE] * (n + 1) + [PLACE] * 3,
        [
            pltpu.VMEM((exp_dev, m * cap, full), bf16),
            pltpu.VMEM((exp_dev, hidden, full), bf16),
            pltpu.VMEM((exp_dev, hidden, full), bf16),
            pltpu.VMEM((exp_dev, hidden, full), bf16),
            pltpu.SemaphoreType.DMA((3, exp_dev)),
        ],
        limit=40 * 2**20,
        name="experts",
    )(*fragments, moe_gain.reshape(1, full), gate_weight, up_weight, down_weight)

    terms = reduce_swaps(outs, n)
    totals = call(
        functools.partial(total_body, m, len(terms)),
        [jax.ShapeDtypeStruct((exp_dev, cap, wide), bf16)] * m,
        [WHOLE] * len(terms),
        limit=8 * 2**20,
        name="total",
    )(*terms)
    back = [totals[0]] + [swap(totals[j], "ep", j) for j in range(1, m)]
    result = call(
        functools.partial(combine_body, m),
        jax.ShapeDtypeStruct((count, wide), bf16),
        [WHOLE] * (3 + m),
        [pltpu.VMEM((slots, wide), bf16)],
        limit=8 * 2**20,
        name="combine",
    )(resid, choose, route_weight, *back)
    return (
        result,
        new_r.reshape(count, groups, entries),
        new_i.reshape(count, groups, entries),
    )


def ssm_step(
    driven,
    state_real,
    state_imag,
    eig_real,
    eig_imag,
    log_step,
    input_real,
    input_imag,
    output_matrix_real,
    output_matrix_imag,
    skip_weight,
):
    highest_precision = lax.Precision.HIGHEST
    count_of_rows = driven.shape[0]
    groups = eig_real.shape[0]
    group_width = input_real.shape[2]
    time_step = jnp.exp(log_step)[:, None]
    magnitude = jnp.exp(eig_real * time_step)
    angle_now = eig_imag * time_step
    bar_real = magnitude * jnp.cos(angle_now)
    bar_imag = magnitude * jnp.sin(angle_now)
    modulus = eig_real * eig_real + eig_imag * eig_imag
    fac_real = ((bar_real - 1.0) * eig_real + bar_imag * eig_imag) / modulus
    fac_imag = (bar_imag * eig_real - (bar_real - 1.0) * eig_imag) / modulus
    ib_real = fac_real[..., None] * input_real - fac_imag[..., None] * input_imag
    ib_imag = fac_real[..., None] * input_imag + fac_imag[..., None] * input_real
    grouped = driven.astype(jnp.float32).reshape(count_of_rows, groups, group_width)
    push_real = jnp.einsum("gpc,ngc->ngp", ib_real, grouped, precision=highest_precision)
    push_imag = jnp.einsum("gpc,ngc->ngp", ib_imag, grouped, precision=highest_precision)
    updated_state_real = bar_real[None] * state_real - bar_imag[None] * state_imag + push_real
    updated_state_imag = bar_real[None] * state_imag + bar_imag[None] * state_real + push_imag
    state_readout = jnp.einsum(
        "jiy,sjy->sji", output_matrix_real, updated_state_real, precision=highest_precision
    ) - jnp.einsum(
        "jiy,sjy->sji", output_matrix_imag, updated_state_imag, precision=highest_precision
    )
    state_readout = state_readout.reshape(count_of_rows, groups * group_width) + skip_weight[
        None, :
    ] * driven.astype(jnp.float32)
    activated = jax.nn.gelu(state_readout).astype(jnp.bfloat16)
    return (updated_state_real, updated_state_imag, activated)


def local(
    tokens,
    state_real,
    state_imag,
    mix_gain,
    in_weight,
    eig_real,
    eig_imag,
    log_step,
    input_real,
    input_imag,
    output_matrix_real,
    output_matrix_imag,
    skip_weight,
    glu_weight,
    glu_bias,
    out_weight,
    moe_gain,
    routes,
    route_weight,
    gate_weight,
    up_weight,
    down_weight,
):
    count_of_rows = tokens.shape[0]
    n_ep = lax.axis_size("ep")
    width_tp = lax.axis_size("tp")
    whole_rows = lax.all_gather(tokens, "tp", axis=1, tiled=True)
    whole_float = whole_rows.astype(jnp.float32)
    first_scale = lax.rsqrt(jnp.mean(whole_float * whole_float, axis=1, keepdims=True) + norm_eps)
    normed = (whole_float * first_scale * mix_gain.astype(jnp.float32)).astype(jnp.bfloat16)
    driven = jnp.einsum("rd,cd->rc", normed, in_weight, preferred_element_type=jnp.float32).astype(
        jnp.bfloat16
    )
    updated_state_real, updated_state_imag, activated = ssm_step(
        driven,
        state_real,
        state_imag,
        eig_real,
        eig_imag,
        log_step,
        input_real,
        input_imag,
        output_matrix_real,
        output_matrix_imag,
        skip_weight,
    )
    gate_pre = (
        jnp.einsum(
            "rc,oc->ro",
            lax.all_gather(activated, "tp", axis=1, tiled=True),
            glu_weight,
            preferred_element_type=jnp.float32,
        )
        + glu_bias
    )
    glued = (activated.astype(jnp.float32) * jax.nn.sigmoid(gate_pre)).astype(jnp.bfloat16)
    partial_value = jnp.dot(glued, out_weight, preferred_element_type=jnp.float32)
    mixed = lax.psum_scatter(
        partial_value.astype(jnp.bfloat16), "tp", scatter_dimension=1, tiled=True
    ).astype(jnp.float32)
    residual = (tokens.astype(jnp.float32) + mixed).astype(jnp.bfloat16)
    resid_float = residual.astype(jnp.float32)
    exp_dev = gate_weight.shape[0]
    experts = exp_dev * n_ep
    top_count = routes.shape[1]
    capacity = max(2, (3 * top_count * count_of_rows + 2 * experts - 1) // (2 * experts))
    chosen = routes.reshape(-1)
    onehot = (chosen[:, None] == jnp.arange(experts, dtype=jnp.int32)[None, :]).astype(jnp.int32)
    rank_index = jnp.sum((jnp.cumsum(onehot, axis=0) - onehot) * onehot, axis=1)
    slot_index = (chosen * capacity + rank_index).reshape(count_of_rows, top_count)
    slots_all = experts * capacity
    choose = slot_index[:, :, None] == jnp.arange(slots_all, dtype=jnp.int32)[None, None, :]
    dispatch = jnp.sum(choose.astype(jnp.float32), axis=1).astype(jnp.bfloat16)
    local_sq = jnp.sum(resid_float * resid_float, axis=1)
    total_sq = lax.psum(local_sq, "tp")
    dim_full = residual.shape[1] * width_tp
    second_scale = lax.rsqrt(total_sq[:, None] / dim_full + norm_eps)
    gain_part = lax.dynamic_slice_in_dim(
        moe_gain, lax.axis_index("tp") * residual.shape[1], residual.shape[1], 0
    )
    expert_in = (resid_float * second_scale * gain_part.astype(jnp.float32)).astype(jnp.bfloat16)
    packed = jnp.einsum(
        "rs,rd->sd", dispatch, expert_in, preferred_element_type=jnp.float32
    ).astype(jnp.bfloat16)
    packed = packed.reshape(n_ep, exp_dev * capacity, residual.shape[1])
    arrived = lax.all_to_all(packed, "ep", split_axis=0, concat_axis=0, tiled=True)
    arrived = arrived.reshape(n_ep, exp_dev, capacity, residual.shape[1])
    fragment = lax.all_gather(arrived, "tp", axis=3, tiled=True)
    gate_part = jnp.einsum(
        "necd,efd->necf", fragment, gate_weight, preferred_element_type=jnp.float32
    )
    up_part = jnp.einsum("necd,efd->necf", fragment, up_weight, preferred_element_type=jnp.float32)
    hidden_width = (jax.nn.silu(gate_part) * up_part).astype(jnp.bfloat16)
    partial_out = jnp.einsum(
        "necf,efd->necd", hidden_width, down_weight, preferred_element_type=jnp.float32
    )
    summed = lax.psum_scatter(
        partial_out.astype(jnp.bfloat16), "tp", scatter_dimension=3, tiled=True
    )
    summed = summed.reshape(n_ep, exp_dev * capacity, summed.shape[3])
    returned = lax.all_to_all(summed, "ep", split_axis=0, concat_axis=0, tiled=True)
    returned = returned.reshape(slots_all, returned.shape[2])
    gathered_k = jnp.einsum(
        "rks,sd->rkd", choose.astype(jnp.bfloat16), returned, preferred_element_type=jnp.float32
    )
    result = (resid_float + jnp.sum(route_weight[..., None] * gathered_k, axis=1)).astype(
        jnp.bfloat16
    )
    return (result, updated_state_real, updated_state_imag)


def solution(mesh):
    n, m = mesh.shape["tp"], mesh.shape["ep"]
    small = n in (4, 8) and m in (2, 4)
    return jax.shard_map(
        local_swaps if small else local,
        mesh=mesh,
        in_specs=(
            P("ep", "tp"),
            P("ep", "tp", None),
            P("ep", "tp", None),
            P(),
            P("tp", None),
            P("tp", None),
            P("tp", None),
            P("tp"),
            P("tp", None, None),
            P("tp", None, None),
            P("tp", None, None),
            P("tp", None, None),
            P("tp"),
            P("tp", None),
            P("tp"),
            P("tp", None),
            P(),
            P("ep", None),
            P("ep", None),
            P("ep", "tp", None),
            P("ep", "tp", None),
            P("ep", "tp", None),
        ),
        out_specs=(P("ep", "tp"), P("ep", "tp", None), P("ep", "tp", None)),
        check_vma=False,
    )
```

```python
import functools
import jax
import jax.numpy as jnp
from jax import lax
from jax.experimental import pallas as pl
from jax.experimental.pallas import tpu as pltpu
from jax.sharding import PartitionSpec as P

norm_eps = 1e-06
f32 = jnp.float32
bf16 = jnp.bfloat16
NT = (((1,), (1,)), ((), ()))
NN = (((1,), (0,)), ((), ()))
TN = (((0,), (0,)), ((), ()))
WHOLE = pl.BlockSpec(memory_space=pltpu.VMEM)
FAR = pl.BlockSpec(memory_space=pltpu.HBM)
LANES = 128


def stay(x):
    return pltpu.with_memory_space_constraint(x, pltpu.HBM)


def dot(a, b, dims):
    return lax.dot_general(a, b, dims, preferred_element_type=f32)


def swap(x, axis, k):
    return lax.ppermute(x, axis, [(i, i ^ k) for i in range(lax.axis_size(axis))])


def gather_swaps(x, n):
    pieces = [None] * n
    pieces[0] = x
    for k in range(2, n, 2):
        pieces[k] = swap(x, "tp", k)
    for k in range(0, n, 2):
        pieces[k ^ 1] = swap(pieces[k], "tp", 1)
    return pieces


def reduce_swaps(parts, n):
    pair = [None] * n
    for k in range(0, n, 2):
        other = swap(parts[k ^ 1], "tp", 1)
        pair[k] = parts[k].astype(f32) + other.astype(f32)
    terms = [pair[0]]
    for k in range(2, n, 2):
        terms.append(swap(pair[k].astype(bf16), "tp", k))
    return terms


def call(body, out_shape, in_specs, scratch=(), limit=None, flops=10**7, name=None):
    single = not isinstance(out_shape, (list, tuple))
    return pl.pallas_call(
        body,
        out_shape=out_shape,
        in_specs=in_specs,
        out_specs=WHOLE if single else [WHOLE] * len(out_shape),
        scratch_shapes=list(scratch),
        compiler_params=pltpu.CompilerParams(vmem_limit_bytes=limit),
        cost_estimate=pl.CostEstimate(flops=flops, bytes_accessed=10**6, transcendentals=0),
        name=name,
    )


def place(k, width):
    return pl.ds(pl.multiple_of((lax.axis_index("tp") ^ k) * width, width), width)


def prep_body(cap, *refs):
    bar_r, bar_i, fac_r, fac_i, routes = refs[:5]
    far = refs[5:15]
    dec_r, dec_i, bt_r, bt_i, cm_r, cm_i, fac, choose, table = refs[15:24]
    flat = refs[24:28]
    held = refs[28:38]
    sems = refs[38]
    copies = [pltpu.make_async_copy(a, b, sems.at[i]) for i, (a, b) in enumerate(zip(far, held))]
    for copy in copies:
        copy.start()
    slots, count = table.shape
    top = routes.shape[0]
    experts = slots // cap
    names = lax.broadcasted_iota(jnp.int32, (16, count), 0)
    marks = [(routes[r : r + 1, :] == names).astype(f32) for r in range(top)]
    total = marks[0]
    for r in range(1, top):
        total = total + marks[r]
    row = lax.broadcasted_iota(jnp.int32, (count, count), 0)
    col = lax.broadcasted_iota(jnp.int32, (count, count), 1)
    before = dot(total.astype(bf16), (row < col).astype(bf16), NN)
    places = lax.broadcasted_iota(jnp.int32, (slots, count), 0).astype(f32)
    used = jnp.zeros((slots, count), f32)
    for r in range(top):
        rank = jnp.sum(before * marks[r], axis=0, keepdims=True)
        slot = routes[r : r + 1, :].astype(f32) * cap + rank
        hit = (places == slot).astype(f32)
        choose[r] = hit.astype(bf16)
        used = used + hit
    table[...] = used.astype(bf16)
    st_r, st_i, in_r, in_i, om_r, om_i = held[:6]
    groups, inner, entries = in_r.shape
    pack = LANES // inner
    for i, dst in ((2, bt_r), (3, bt_i), (4, cm_r), (5, cm_i)):
        copies[i].wait()
        spread(held[i][...].reshape(groups * inner, entries), dst, inner, pack)
    copies[0].wait()
    copies[1].wait()
    for g in range(groups):
        cols = slice(g * entries, (g + 1) * entries)
        s_r, s_i = st_r[:, g, :], st_i[:, g, :]
        b_r, b_i = bar_r[g : g + 1, :], bar_i[g : g + 1, :]
        dec_r[:, cols] = b_r * s_r - b_i * s_i
        dec_i[:, cols] = b_r * s_i + b_i * s_r
        fac[0:1, cols] = fac_r[g : g + 1, :]
        fac[1:2, cols] = fac_i[g : g + 1, :]
    for i in range(len(flat)):
        copies[6 + i].wait()
        rows = held[6 + i][...].astype(f32)
        for r in range(rows.shape[0]):
            flat[i][0:1, r * LANES : (r + 1) * LANES] = rows[r : r + 1, :]


def spread(blocks, out, height, pack):
    rows, inner = blocks.shape
    columns = pack * inner
    at = lax.broadcasted_iota(jnp.int32, (inner, columns), 0)
    to = lax.broadcasted_iota(jnp.int32, (inner, columns), 1)
    wide = dot(blocks.astype(bf16), (to % inner == at).astype(bf16), NN)
    row = lax.broadcasted_iota(jnp.int32, (rows, columns), 0)
    col = lax.broadcasted_iota(jnp.int32, (rows, columns), 1)
    own = (row // height) % pack == col // inner
    out[...] = jnp.where(own, wide, 0.0).astype(bf16)


def load(src, dst, sems, n, width):
    copies = []
    for k in range(n):
        part = src.at[:, place(k, width)] if len(src.shape) == 2 else src.at[:, :, place(k, width)]
        copies.append(pltpu.make_async_copy(part, dst.at[k], sems.at[k]))
    for copy in copies:
        copy.start()
    return copies


def mixer_body(n, *refs):
    pieces = refs[:n]
    gain, weight_hbm, bt_r, bt_i, fac, dec_r, dec_i, cm_r, cm_i, skip = refs[n : n + 10]
    new_r_ref, new_i_ref, act_ref, weight, sems = refs[n + 10 :]
    width = pieces[0].shape[1]
    copies = load(weight_hbm, weight, sems, n, width)
    square = 0.0
    for k in range(n):
        x = pieces[k][...].astype(f32)
        square = square + jnp.sum(x * x, axis=1, keepdims=True)
    scale = lax.rsqrt(square / (n * width) + norm_eps)
    total = 0.0
    for k in range(n):
        part = gain[:, place(k, width)]
        normed = (pieces[k][...].astype(f32) * scale * part).astype(bf16)
        copies[k].wait()
        total = total + dot(normed, weight[k], NT)
    driven = total.astype(bf16)
    high = cm_r.shape[1]
    for b in range(driven.shape[1] // LANES):
        rows = slice(b * high, (b + 1) * high)
        lanes = slice(b * LANES, (b + 1) * LANES)
        u_r = dot(driven[:, lanes], bt_r[lanes, :], NN)
        u_i = dot(driven[:, lanes], bt_i[lanes, :], NN)
        f_r, f_i = fac[0:1, rows], fac[1:2, rows]
        new_r = dec_r[:, rows] + f_r * u_r - f_i * u_i
        new_i = dec_i[:, rows] + f_r * u_i + f_i * u_r
        new_r_ref[:, rows] = new_r
        new_i_ref[:, rows] = new_i
        out = dot(new_r.astype(bf16), cm_r[lanes, :], NT) - dot(new_i.astype(bf16), cm_i[lanes, :], NT)
        out = out + skip[:, lanes] * driven[:, lanes].astype(f32)
        act_ref[:, lanes] = jax.nn.gelu(out).astype(bf16)


def unpack_body(*refs):
    half = len(refs) // 2
    for src, dst in zip(refs[:half], refs[half:]):
        entries = dst.shape[2]
        for g in range(dst.shape[1]):
            dst[:, g, :] = src[:, g * entries : (g + 1) * entries]


def glu_body(n, *refs):
    pieces = refs[:n]
    glu_hbm, bias, out_hbm = refs[n : n + 3]
    outs = refs[n + 3 : 2 * n + 3]
    glu, out_w, glu_sems, out_sems = refs[2 * n + 3 :]
    width, wide = pieces[0].shape[1], outs[0].shape[1]
    first = load(glu_hbm, glu, glu_sems, n, width)
    later = load(out_hbm, out_w, out_sems, n, wide)
    gate = bias[...]
    for k in range(n):
        first[k].wait()
        gate = gate + dot(pieces[k][...], glu[k], NT)
    glued = (pieces[0][...].astype(f32) * jax.nn.sigmoid(gate)).astype(bf16)
    for k in range(n):
        later[k].wait()
        outs[k][...] = dot(glued, out_w[k], NN).astype(bf16)


def dispatch_body(m, terms, *refs):
    tokens = refs[0]
    sums = refs[1 : 1 + terms]
    table = refs[1 + terms]
    resid_ref = refs[2 + terms]
    outs = refs[3 + terms :]
    mixed = sums[0][...]
    for s in sums[1:]:
        mixed = mixed + s[...].astype(f32)
    resid = (tokens[...].astype(f32) + mixed).astype(bf16)
    resid_ref[...] = resid
    experts, cap, wide = outs[0].shape
    count = experts * cap
    for j in range(m):
        at = pl.multiple_of((lax.axis_index("ep") ^ j) * count, count)
        picked = dot(table[pl.ds(at, count), :], resid, NN).astype(bf16)
        outs[j][...] = picked.reshape(experts, cap, wide)


def expert_body(n, *refs):
    pieces = refs[:n]
    gain, gate_hbm, up_hbm, down_hbm = refs[n : n + 4]
    outs = refs[n + 4 : 2 * n + 4]
    gate_w, up_w, down_w, gate_sems, up_sems, down_sems = refs[2 * n + 4 :]
    experts, count, width = pieces[0].shape
    gates = load(gate_hbm, gate_w, gate_sems, n, width)
    ups = load(up_hbm, up_w, up_sems, n, width)
    downs = load(down_hbm, down_w, down_sems, n, width)
    g, u, square = [0.0] * experts, [0.0] * experts, [0.0] * experts
    for k in range(n):
        part = gain[:, place(k, width)]
        gates[k].wait()
        ups[k].wait()
        for i in range(experts):
            x = pieces[k][i].astype(f32)
            square[i] = square[i] + jnp.sum(x * x, axis=1, keepdims=True)
            x = (x * part).astype(bf16)
            g[i] = g[i] + dot(x, gate_w[k, i], NT)
            u[i] = u[i] + dot(x, up_w[k, i], NT)
    hidden = []
    for i in range(experts):
        scale = lax.rsqrt(square[i] / (n * width) + norm_eps)
        hidden.append((jax.nn.silu(g[i] * scale) * (u[i] * scale)).astype(bf16))
    for k in range(n):
        downs[k].wait()
        for i in range(experts):
            outs[k][i] = dot(hidden[i], down_w[k, i], NN).astype(bf16)


def total_body(m, terms, *refs):
    sums = refs[:terms]
    outs = refs[terms:]
    total = sums[0][...]
    for s in sums[1:]:
        total = total + s[...].astype(f32)
    total = total.astype(bf16)
    cap = outs[0].shape[1]
    for j in range(m):
        outs[j][...] = total[:, j * cap : (j + 1) * cap, :]


def combine_body(m, *refs):
    resid, choose, weight = refs[:3]
    back = refs[3 : 3 + m]
    out, rows = refs[3 + m :]
    experts, cap, wide = back[0].shape
    count = experts * cap
    for j in range(m):
        at = pl.multiple_of((lax.axis_index("ep") ^ j) * count, count)
        rows[pl.ds(at, count), :] = back[j][...].reshape(count, wide)
    total = resid[...].astype(f32)
    for r in range(weight.shape[1]):
        picked = dot(choose[r], rows[...], TN)
        total = total + weight[:, r : r + 1] * picked
    out[...] = total.astype(bf16)


def local_swaps(
    tokens,
    state_real,
    state_imag,
    mix_gain,
    in_weight,
    eig_real,
    eig_imag,
    log_step,
    input_real,
    input_imag,
    output_matrix_real,
    output_matrix_imag,
    skip_weight,
    glu_weight,
    glu_bias,
    out_weight,
    moe_gain,
    routes,
    route_weight,
    gate_weight,
    up_weight,
    down_weight,
):
    count, wide = tokens.shape
    n = lax.axis_size("tp")
    m = lax.axis_size("ep")
    groups, entries = eig_real.shape
    inner = input_real.shape[2]
    states = groups * entries
    channels = groups * inner
    full = wide * n
    exp_dev = gate_weight.shape[0]
    experts = exp_dev * m
    top = routes.shape[1]
    cap = max(2, (3 * top * count + 2 * experts - 1) // (2 * experts))
    slots = experts * cap

    pieces = gather_swaps(tokens, n)

    step = jnp.exp(log_step)[:, None]
    size = jnp.exp(eig_real * step)
    angle = eig_imag * step
    bar_r = size * jnp.cos(angle)
    bar_i = size * jnp.sin(angle)
    modulus = eig_real * eig_real + eig_imag * eig_imag
    fac_r = ((bar_r - 1.0) * eig_real + bar_i * eig_imag) / modulus
    fac_i = (bar_i * eig_real - (bar_r - 1.0) * eig_imag) / modulus
    pack = LANES // inner
    far = [
        state_real,
        state_imag,
        input_real.transpose(0, 2, 1),
        input_imag.transpose(0, 2, 1),
        output_matrix_real,
        output_matrix_imag,
        skip_weight.reshape(-1, LANES),
        glu_bias.reshape(-1, LANES),
        mix_gain.reshape(-1, LANES),
        moe_gain.reshape(-1, LANES),
    ]
    dec_r, dec_i, bt_r, bt_i, cm_r, cm_i, fac, choose, table, skip, bias, gain1, gain2 = call(
        functools.partial(prep_body, cap),
        [jax.ShapeDtypeStruct((count, states), f32)] * 2
        + [jax.ShapeDtypeStruct((channels, pack * entries), bf16)] * 4
        + [
            jax.ShapeDtypeStruct((2, states), f32),
            jax.ShapeDtypeStruct((top, slots, count), bf16),
            jax.ShapeDtypeStruct((slots, count), bf16),
        ]
        + [jax.ShapeDtypeStruct((1, channels), f32)] * 2
        + [jax.ShapeDtypeStruct((1, full), f32)] * 2,
        [WHOLE] * 5 + [FAR] * 10,
        [pltpu.VMEM(x.shape, x.dtype) for x in far] + [pltpu.SemaphoreType.DMA((10,))],
        limit=12 * 2**20,
        name="prep",
    )(bar_r, bar_i, fac_r, fac_i, routes.T, *[stay(x) for x in far])

    new_r, new_i, activated = call(
        functools.partial(mixer_body, n),
        [
            jax.ShapeDtypeStruct((count, states), f32),
            jax.ShapeDtypeStruct((count, states), f32),
            jax.ShapeDtypeStruct((count, channels), bf16),
        ],
        [WHOLE] * (n + 1) + [FAR] + [WHOLE] * 8,
        [pltpu.VMEM((n, channels, wide), bf16), pltpu.SemaphoreType.DMA((n,))],
        limit=12 * 2**20,
        name="mixer",
    )(
        *pieces,
        gain1,
        stay(in_weight),
        bt_r,
        bt_i,
        fac,
        dec_r,
        dec_i,
        cm_r,
        cm_i,
        skip,
    )

    acts = gather_swaps(activated, n)
    new_r, new_i = call(
        unpack_body,
        [jax.ShapeDtypeStruct((count, groups, entries), f32)] * 2,
        [WHOLE] * 2,
        limit=4 * 2**20,
        name="unpack",
    )(new_r, new_i)
    parts = call(
        functools.partial(glu_body, n),
        [jax.ShapeDtypeStruct((count, wide), bf16)] * n,
        [WHOLE] * n + [FAR, WHOLE, FAR],
        [
            pltpu.VMEM((n, channels, channels), bf16),
            pltpu.VMEM((n, channels, wide), bf16),
            pltpu.SemaphoreType.DMA((n,)),
            pltpu.SemaphoreType.DMA((n,)),
        ],
        limit=12 * 2**20,
        name="glu",
    )(*acts, stay(glu_weight), bias, stay(out_weight))

    terms = reduce_swaps(parts, n)
    resid, *packed = call(
        functools.partial(dispatch_body, m, len(terms)),
        [jax.ShapeDtypeStruct((count, wide), bf16)]
        + [jax.ShapeDtypeStruct((exp_dev, cap, wide), bf16)] * m,
        [WHOLE] * (2 + len(terms)),
        limit=8 * 2**20,
        name="dispatch",
    )(tokens, *terms, table)

    arrived = [packed[0]] + [swap(packed[j], "ep", j) for j in range(1, m)]
    arrived = jnp.concatenate(arrived, axis=1)
    fragments = gather_swaps(arrived, n)
    hidden = gate_weight.shape[1]
    outs = call(
        functools.partial(expert_body, n),
        [jax.ShapeDtypeStruct((exp_dev, m * cap, wide), bf16)] * n,
        [WHOLE] * (n + 1) + [FAR] * 3,
        [pltpu.VMEM((n, exp_dev, hidden, wide), bf16)] * 3 + [pltpu.SemaphoreType.DMA((n,))] * 3,
        limit=40 * 2**20,
        name="experts",
    )(*fragments, gain2, stay(gate_weight), stay(up_weight), stay(down_weight))

    terms = reduce_swaps(outs, n)
    totals = call(
        functools.partial(total_body, m, len(terms)),
        [jax.ShapeDtypeStruct((exp_dev, cap, wide), bf16)] * m,
        [WHOLE] * len(terms),
        limit=8 * 2**20,
        name="total",
    )(*terms)
    back = [totals[0]] + [swap(totals[j], "ep", j) for j in range(1, m)]
    result = call(
        functools.partial(combine_body, m),
        jax.ShapeDtypeStruct((count, wide), bf16),
        [WHOLE] * (3 + m),
        [pltpu.VMEM((slots, wide), bf16)],
        limit=8 * 2**20,
        name="combine",
    )(resid, choose, route_weight, *back)
    return (
        result,
        new_r,
        new_i,
    )


def ssm_step(
    driven,
    state_real,
    state_imag,
    eig_real,
    eig_imag,
    log_step,
    input_real,
    input_imag,
    output_matrix_real,
    output_matrix_imag,
    skip_weight,
):
    highest_precision = lax.Precision.HIGHEST
    count_of_rows = driven.shape[0]
    groups = eig_real.shape[0]
    group_width = input_real.shape[2]
    time_step = jnp.exp(log_step)[:, None]
    magnitude = jnp.exp(eig_real * time_step)
    angle_now = eig_imag * time_step
    bar_real = magnitude * jnp.cos(angle_now)
    bar_imag = magnitude * jnp.sin(angle_now)
    modulus = eig_real * eig_real + eig_imag * eig_imag
    fac_real = ((bar_real - 1.0) * eig_real + bar_imag * eig_imag) / modulus
    fac_imag = (bar_imag * eig_real - (bar_real - 1.0) * eig_imag) / modulus
    ib_real = fac_real[..., None] * input_real - fac_imag[..., None] * input_imag
    ib_imag = fac_real[..., None] * input_imag + fac_imag[..., None] * input_real
    grouped = driven.astype(jnp.float32).reshape(count_of_rows, groups, group_width)
    push_real = jnp.einsum("gpc,ngc->ngp", ib_real, grouped, precision=highest_precision)
    push_imag = jnp.einsum("gpc,ngc->ngp", ib_imag, grouped, precision=highest_precision)
    updated_state_real = bar_real[None] * state_real - bar_imag[None] * state_imag + push_real
    updated_state_imag = bar_real[None] * state_imag + bar_imag[None] * state_real + push_imag
    state_readout = jnp.einsum(
        "jiy,sjy->sji", output_matrix_real, updated_state_real, precision=highest_precision
    ) - jnp.einsum(
        "jiy,sjy->sji", output_matrix_imag, updated_state_imag, precision=highest_precision
    )
    state_readout = state_readout.reshape(count_of_rows, groups * group_width) + skip_weight[
        None, :
    ] * driven.astype(jnp.float32)
    activated = jax.nn.gelu(state_readout).astype(jnp.bfloat16)
    return (updated_state_real, updated_state_imag, activated)


def local(
    tokens,
    state_real,
    state_imag,
    mix_gain,
    in_weight,
    eig_real,
    eig_imag,
    log_step,
    input_real,
    input_imag,
    output_matrix_real,
    output_matrix_imag,
    skip_weight,
    glu_weight,
    glu_bias,
    out_weight,
    moe_gain,
    routes,
    route_weight,
    gate_weight,
    up_weight,
    down_weight,
):
    count_of_rows = tokens.shape[0]
    n_ep = lax.axis_size("ep")
    width_tp = lax.axis_size("tp")
    whole_rows = lax.all_gather(tokens, "tp", axis=1, tiled=True)
    whole_float = whole_rows.astype(jnp.float32)
    first_scale = lax.rsqrt(jnp.mean(whole_float * whole_float, axis=1, keepdims=True) + norm_eps)
    normed = (whole_float * first_scale * mix_gain.astype(jnp.float32)).astype(jnp.bfloat16)
    driven = jnp.einsum("rd,cd->rc", normed, in_weight, preferred_element_type=jnp.float32).astype(
        jnp.bfloat16
    )
    updated_state_real, updated_state_imag, activated = ssm_step(
        driven,
        state_real,
        state_imag,
        eig_real,
        eig_imag,
        log_step,
        input_real,
        input_imag,
        output_matrix_real,
        output_matrix_imag,
        skip_weight,
    )
    gate_pre = (
        jnp.einsum(
            "rc,oc->ro",
            lax.all_gather(activated, "tp", axis=1, tiled=True),
            glu_weight,
            preferred_element_type=jnp.float32,
        )
        + glu_bias
    )
    glued = (activated.astype(jnp.float32) * jax.nn.sigmoid(gate_pre)).astype(jnp.bfloat16)
    partial_value = jnp.dot(glued, out_weight, preferred_element_type=jnp.float32)
    mixed = lax.psum_scatter(
        partial_value.astype(jnp.bfloat16), "tp", scatter_dimension=1, tiled=True
    ).astype(jnp.float32)
    residual = (tokens.astype(jnp.float32) + mixed).astype(jnp.bfloat16)
    resid_float = residual.astype(jnp.float32)
    exp_dev = gate_weight.shape[0]
    experts = exp_dev * n_ep
    top_count = routes.shape[1]
    capacity = max(2, (3 * top_count * count_of_rows + 2 * experts - 1) // (2 * experts))
    chosen = routes.reshape(-1)
    onehot = (chosen[:, None] == jnp.arange(experts, dtype=jnp.int32)[None, :]).astype(jnp.int32)
    rank_index = jnp.sum((jnp.cumsum(onehot, axis=0) - onehot) * onehot, axis=1)
    slot_index = (chosen * capacity + rank_index).reshape(count_of_rows, top_count)
    slots_all = experts * capacity
    choose = slot_index[:, :, None] == jnp.arange(slots_all, dtype=jnp.int32)[None, None, :]
    dispatch = jnp.sum(choose.astype(jnp.float32), axis=1).astype(jnp.bfloat16)
    local_sq = jnp.sum(resid_float * resid_float, axis=1)
    total_sq = lax.psum(local_sq, "tp")
    dim_full = residual.shape[1] * width_tp
    second_scale = lax.rsqrt(total_sq[:, None] / dim_full + norm_eps)
    gain_part = lax.dynamic_slice_in_dim(
        moe_gain, lax.axis_index("tp") * residual.shape[1], residual.shape[1], 0
    )
    expert_in = (resid_float * second_scale * gain_part.astype(jnp.float32)).astype(jnp.bfloat16)
    packed = jnp.einsum(
        "rs,rd->sd", dispatch, expert_in, preferred_element_type=jnp.float32
    ).astype(jnp.bfloat16)
    packed = packed.reshape(n_ep, exp_dev * capacity, residual.shape[1])
    arrived = lax.all_to_all(packed, "ep", split_axis=0, concat_axis=0, tiled=True)
    arrived = arrived.reshape(n_ep, exp_dev, capacity, residual.shape[1])
    fragment = lax.all_gather(arrived, "tp", axis=3, tiled=True)
    gate_part = jnp.einsum(
        "necd,efd->necf", fragment, gate_weight, preferred_element_type=jnp.float32
    )
    up_part = jnp.einsum("necd,efd->necf", fragment, up_weight, preferred_element_type=jnp.float32)
    hidden_width = (jax.nn.silu(gate_part) * up_part).astype(jnp.bfloat16)
    partial_out = jnp.einsum(
        "necf,efd->necd", hidden_width, down_weight, preferred_element_type=jnp.float32
    )
    summed = lax.psum_scatter(
        partial_out.astype(jnp.bfloat16), "tp", scatter_dimension=3, tiled=True
    )
    summed = summed.reshape(n_ep, exp_dev * capacity, summed.shape[3])
    returned = lax.all_to_all(summed, "ep", split_axis=0, concat_axis=0, tiled=True)
    returned = returned.reshape(slots_all, returned.shape[2])
    gathered_k = jnp.einsum(
        "rks,sd->rkd", choose.astype(jnp.bfloat16), returned, preferred_element_type=jnp.float32
    )
    result = (resid_float + jnp.sum(route_weight[..., None] * gathered_k, axis=1)).astype(
        jnp.bfloat16
    )
    return (result, updated_state_real, updated_state_imag)


def solution(mesh):
    n, m = mesh.shape["tp"], mesh.shape["ep"]
    small = n in (4, 8) and m in (2, 4)
    return jax.shard_map(
        local_swaps if small else local,
        mesh=mesh,
        in_specs=(
            P("ep", "tp"),
            P("ep", "tp", None),
            P("ep", "tp", None),
            P(),
            P("tp", None),
            P("tp", None),
            P("tp", None),
            P("tp"),
            P("tp", None, None),
            P("tp", None, None),
            P("tp", None, None),
            P("tp", None, None),
            P("tp"),
            P("tp", None),
            P("tp"),
            P("tp", None),
            P(),
            P("ep", None),
            P("ep", None),
            P("ep", "tp", None),
            P("ep", "tp", None),
            P("ep", "tp", None),
        ),
        out_specs=(P("ep", "tp"), P("ep", "tp", None), P("ep", "tp", None)),
        check_vma=False,
    )
```

```python
import functools
import jax
import jax.numpy as jnp
from jax import lax
from jax.experimental import pallas as pl
from jax.experimental.pallas import tpu as pltpu
from jax.sharding import PartitionSpec as P


norm_eps = 1e-06
f32 = jnp.float32
bf16 = jnp.bfloat16
NT = (((1,), (1,)), ((), ()))
NN = (((1,), (0,)), ((), ()))
TN = (((0,), (0,)), ((), ()))
WHOLE = pl.BlockSpec(memory_space=pltpu.VMEM)
FAR = pl.BlockSpec(memory_space=pltpu.HBM)
LANES = 128


def stay(x):
    return pltpu.with_memory_space_constraint(x, pltpu.HBM)


def dot(a, b, dims):
    return lax.dot_general(a, b, dims, preferred_element_type=f32)


def swap(x, axis, k):
    return lax.ppermute(x, axis, [(i, i ^ k) for i in range(lax.axis_size(axis))])


def gather_swaps(x, n):
    pieces = [None] * n
    pieces[0] = x
    for k in range(2, n, 2):
        pieces[k] = swap(x, "tp", k)
    for k in range(0, n, 2):
        pieces[k ^ 1] = swap(pieces[k], "tp", 1)
    return pieces


def pair_swaps(own, partner, n):
    other = swap(partner, "tp", 1)
    shape = own.shape[1:]
    return call(
        pair_body,
        [jax.ShapeDtypeStruct(shape, f32)] + [jax.ShapeDtypeStruct(shape, bf16)] * (n // 2 - 1),
        [WHOLE] * 2,
        limit=8 * 2**20,
    )(own, other)


def reduce_swaps(own, partner, n):
    first, *rest = pair_swaps(own, partner, n)
    return [first] + [swap(x, "tp", k) for x, k in zip(rest, range(2, n, 2))]


def pair_body(own, other, *outs):
    for i, out in enumerate(outs):
        out[...] = (own[i].astype(f32) + other[i].astype(f32)).astype(out.dtype)


def block_of(own, partner, k):
    return (partner if k % 2 else own), k // 2


def call(body, out_shape, in_specs, scratch=(), limit=None, flops=10**7):
    single = not isinstance(out_shape, (list, tuple))
    return pl.pallas_call(
        body,
        out_shape=out_shape,
        in_specs=in_specs,
        out_specs=WHOLE if single else [WHOLE] * len(out_shape),
        scratch_shapes=list(scratch),
        compiler_params=pltpu.CompilerParams(vmem_limit_bytes=limit),
        cost_estimate=pl.CostEstimate(flops=flops, bytes_accessed=10**6, transcendentals=0),
    )


def column(row):
    n = row.shape[1]
    at = lax.broadcasted_iota(jnp.int32, (n, n), 0)
    to = lax.broadcasted_iota(jnp.int32, (n, n), 1)
    return jnp.sum(jnp.where(at == to, jnp.broadcast_to(row, (n, n)), 0.0), axis=1, keepdims=True)


def place(k, width):
    return pl.ds(pl.multiple_of((lax.axis_index("tp") ^ k) * width, width), width)


def prep_body(n, cap, *refs):
    weight_hbm = refs[0]
    far = refs[1:16]
    dec_r, dec_i, bt_r, bt_i, cm_r, cm_i, fac, choose, table = refs[16:25]
    flat = refs[25:29]
    weight, tokens = refs[29:31]
    held = refs[31:45]
    sems, weight_sems = refs[45:]
    held = (*held, tokens)
    copies = [pltpu.make_async_copy(a, b, sems.at[i]) for i, (a, b) in enumerate(zip(far, held))]
    for copy in copies:
        copy.start()
    weights = load(weight_hbm, weight, weight_sems, n, weight.shape[2])
    copies[13].wait()
    routes = held[13]
    slots, count = table.shape
    top = routes.shape[0]
    names = lax.broadcasted_iota(jnp.int32, (16, count), 0)
    marks = [(routes[r : r + 1, :] == names).astype(f32) for r in range(top)]
    total = marks[0]
    for r in range(1, top):
        total = total + marks[r]
    row = lax.broadcasted_iota(jnp.int32, (count, count), 0)
    col = lax.broadcasted_iota(jnp.int32, (count, count), 1)
    before = dot(total.astype(bf16), (row < col).astype(bf16), NN)
    places = lax.broadcasted_iota(jnp.int32, (slots, count), 0).astype(f32)
    used = jnp.zeros((slots, count), f32)
    for r in range(top):
        rank = jnp.sum(before * marks[r], axis=0, keepdims=True)
        slot = routes[r : r + 1, :].astype(f32) * cap + rank
        hit = (places == slot).astype(f32)
        choose[r] = hit.astype(bf16)
        used = used + hit
    table[...] = used.astype(bf16)
    st_r, st_i, in_r, _, _, _ = held[:6]
    groups, inner, entries = in_r.shape
    pack = LANES // inner
    for i, dst in ((2, bt_r), (3, bt_i), (4, cm_r), (5, cm_i)):
        copies[i].wait()
        spread(held[i][...].reshape(groups * inner, entries), dst, inner, pack)
    for i in (0, 1, 10, 11, 12):
        copies[i].wait()
    real, imag, log_step = held[10][...], held[11][...], held[12][...]
    step = column(jnp.exp(log_step))
    size = jnp.exp(real * step)
    angle = imag * step
    bar_r = size * jnp.cos(angle)
    bar_i = size * jnp.sin(angle)
    modulus = real * real + imag * imag
    fac_r = ((bar_r - 1.0) * real + bar_i * imag) / modulus
    fac_i = (bar_i * real - (bar_r - 1.0) * imag) / modulus
    for g in range(groups):
        cols = slice(g * entries, (g + 1) * entries)
        s_r, s_i = st_r[:, g, :], st_i[:, g, :]
        b_r, b_i = bar_r[g : g + 1, :], bar_i[g : g + 1, :]
        dec_r[:, cols] = b_r * s_r - b_i * s_i
        dec_i[:, cols] = b_r * s_i + b_i * s_r
        fac[0:1, cols] = fac_r[g : g + 1, :]
        fac[1:2, cols] = fac_i[g : g + 1, :]
    for i in range(len(flat)):
        copies[6 + i].wait()
        rows = held[6 + i][...].astype(f32)
        for r in range(rows.shape[0]):
            flat[i][0:1, r * LANES : (r + 1) * LANES] = rows[r : r + 1, :]
    copies[14].wait()
    for copy in weights:
        copy.wait()


def spread(blocks, out, height, pack):
    rows, inner = blocks.shape
    columns = pack * inner
    at = lax.broadcasted_iota(jnp.int32, (inner, columns), 0)
    to = lax.broadcasted_iota(jnp.int32, (inner, columns), 1)
    wide = dot(blocks.astype(bf16), (to % inner == at).astype(bf16), NN)
    row = lax.broadcasted_iota(jnp.int32, (rows, columns), 0)
    col = lax.broadcasted_iota(jnp.int32, (rows, columns), 1)
    own = (row // height) % pack == col // inner
    out[...] = jnp.where(own, wide, 0.0).astype(bf16)


def load(src, dst, sems, n, width):
    copies = []
    for k in range(n):
        part = src.at[:, place(k, width)] if len(src.shape) == 2 else src.at[:, :, place(k, width)]
        copies.append(pltpu.make_async_copy(part, dst.at[k], sems.at[k]))
    for copy in copies:
        copy.start()
    return copies


def mixer_body(n, *refs):
    pieces = refs[:n]
    gain, weight, bt_r, bt_i, fac, dec_r, dec_i, cm_r, cm_i, skip = refs[n : n + 10]
    new_r_ref, new_i_ref, act_ref = refs[n + 10 :]
    width = pieces[0].shape[1]
    square = 0.0
    for k in range(n):
        x = pieces[k][...].astype(f32)
        square = square + jnp.sum(x * x, axis=1, keepdims=True)
    scale = lax.rsqrt(square / (n * width) + norm_eps)
    total = 0.0
    for k in range(n):
        part = gain[:, place(k, width)]
        normed = (pieces[k][...].astype(f32) * scale * part).astype(bf16)
        total = total + dot(normed, weight[k], NT)
    driven = total.astype(bf16)
    high = cm_r.shape[1]
    for b in range(driven.shape[1] // LANES):
        rows = slice(b * high, (b + 1) * high)
        lanes = slice(b * LANES, (b + 1) * LANES)
        u_r = dot(driven[:, lanes], bt_r[lanes, :], NN)
        u_i = dot(driven[:, lanes], bt_i[lanes, :], NN)
        f_r, f_i = fac[0:1, rows], fac[1:2, rows]
        new_r = dec_r[:, rows] + f_r * u_r - f_i * u_i
        new_i = dec_i[:, rows] + f_r * u_i + f_i * u_r
        new_r_ref[:, rows] = new_r
        new_i_ref[:, rows] = new_i
        out = dot(new_r.astype(bf16), cm_r[lanes, :], NT) - dot(new_i.astype(bf16), cm_i[lanes, :], NT)
        out = out + skip[:, lanes] * driven[:, lanes].astype(f32)
        act_ref[:, lanes] = jax.nn.gelu(out).astype(bf16)


def unpack_body(new_r, new_i, out_r, out_i):
    for src, dst in ((new_r, out_r), (new_i, out_i)):
        entries = dst.shape[2]
        for g in range(dst.shape[1]):
            dst[:, g, :] = src[:, g * entries : (g + 1) * entries]


def fetch_body(n, count, *refs):
    copies = []
    for i in range(count):
        src, dst, sems = refs[i], refs[count + i], refs[2 * count + i]
        copies += load(src, dst, sems, n, dst.shape[-1])
    for copy in copies:
        copy.wait()


def fetch(n, *sources):
    shapes = [(n, *x.shape[:-1], x.shape[-1] // n) for x in sources]
    return call(
        functools.partial(fetch_body, n, len(sources)),
        [pltpu.VMEM(x, bf16) for x in shapes],
        [FAR] * len(sources),
        [pltpu.SemaphoreType.DMA((n,))] * len(sources),
        limit=2**20,
    )(*[stay(x) for x in sources])


def glu_body(n, *refs):
    pieces = refs[:n]
    glu, bias, out_w = refs[n : n + 3]
    own, partner = refs[n + 3 :]
    gate = bias[...]
    for k in range(n):
        gate = gate + dot(pieces[k][...], glu[k], NT)
    glued = (pieces[0][...].astype(f32) * jax.nn.sigmoid(gate)).astype(bf16)
    for k in range(n):
        to, at = block_of(own, partner, k)
        to[at] = dot(glued, out_w[k], NN).astype(bf16)


def merge_body(*refs):
    out = refs[-1]
    cap = refs[0].shape[1]
    for j, x in enumerate(refs[:-1]):
        out[:, j * cap : (j + 1) * cap, :] = x[...]


def dispatch_body(m, terms, *refs):
    tokens = refs[0]
    sums = refs[1 : 1 + terms]
    table = refs[1 + terms]
    resid_ref = refs[2 + terms]
    outs = refs[3 + terms :]
    mixed = sums[0][...]
    for s in sums[1:]:
        mixed = mixed + s[...].astype(f32)
    resid = (tokens[...].astype(f32) + mixed).astype(bf16)
    resid_ref[...] = resid
    experts, cap, wide = outs[0].shape
    count = experts * cap
    for j in range(m):
        at = pl.multiple_of((lax.axis_index("ep") ^ j) * count, count)
        picked = dot(table[pl.ds(at, count), :], resid, NN).astype(bf16)
        outs[j][...] = picked.reshape(experts, cap, wide)


def up_body(n, *refs):
    near, far = refs[:n], refs[n : 2 * n]
    gain, gate_w, up_w, down_w = refs[2 * n : 2 * n + 4]
    later, own, partner = refs[2 * n + 4 :]
    experts, count, width = near[0].shape
    g, u, square = [0.0] * experts, [0.0] * experts, [0.0] * experts
    for k in range(n):
        part = gain[:, place(k, width)]
        for i in range(experts):
            x = jnp.concatenate([near[k][i], far[k][i]], axis=0).astype(f32)
            square[i] = square[i] + jnp.sum(x * x, axis=1, keepdims=True)
            x = (x * part).astype(bf16)
            g[i] = g[i] + dot(x, gate_w[k, i], NT)
            u[i] = u[i] + dot(x, up_w[k, i], NT)
    for i in range(experts):
        scale = lax.rsqrt(square[i] / (n * width) + norm_eps)
        hidden = (jax.nn.silu(g[i] * scale) * (u[i] * scale)).astype(bf16)
        later[i] = hidden[:count]
        for k in range(n):
            to, at = block_of(own, partner, k)
            to[at, i] = dot(hidden[count:], down_w[k, i], NN).astype(bf16)


def down_body(n, hidden, down_w, own, partner):
    for i in range(hidden.shape[0]):
        for k in range(n):
            to, at = block_of(own, partner, k)
            to[at, i] = dot(hidden[i], down_w[k, i], NN).astype(bf16)


def total_body(m, terms, *refs):
    sums = refs[:terms]
    outs = refs[terms:]
    total = sums[0][...]
    for s in sums[1:]:
        total = total + s[...].astype(f32)
    total = total.astype(bf16)
    cap = outs[0].shape[1]
    for j in range(m):
        outs[j][...] = total[:, j * cap : (j + 1) * cap, :]


def combine_body(m, *refs):
    resid, choose, weight = refs[:3]
    back = refs[3 : 3 + m]
    out, rows = refs[3 + m :]
    experts, cap, wide = back[0].shape
    count = experts * cap
    for j in range(m):
        at = pl.multiple_of((lax.axis_index("ep") ^ j) * count, count)
        rows[pl.ds(at, count), :] = back[j][...].reshape(count, wide)
    total = resid[...].astype(f32)
    for r in range(weight.shape[0]):
        picked = dot(choose[r], rows[...], TN)
        total = total + column(weight[r : r + 1, :]) * picked
    out[...] = total.astype(bf16)


def local_swaps(
    tokens,
    state_real,
    state_imag,
    mix_gain,
    in_weight,
    eig_real,
    eig_imag,
    log_step,
    input_real,
    input_imag,
    output_matrix_real,
    output_matrix_imag,
    skip_weight,
    glu_weight,
    glu_bias,
    out_weight,
    moe_gain,
    routes,
    route_weight,
    gate_weight,
    up_weight,
    down_weight,
):
    count, wide = tokens.shape
    n = lax.axis_size("tp")
    m = lax.axis_size("ep")
    groups, entries = eig_real.shape
    inner = input_real.shape[2]
    states = groups * entries
    channels = groups * inner
    full = wide * n
    exp_dev = gate_weight.shape[0]
    experts = exp_dev * m
    top = routes.shape[1]
    cap = max(2, (3 * top * count + 2 * experts - 1) // (2 * experts))
    slots = experts * cap

    pieces = gather_swaps(tokens, n)
    pack = LANES // inner
    far = [
        state_real,
        state_imag,
        input_real.transpose(0, 2, 1),
        input_imag.transpose(0, 2, 1),
        output_matrix_real,
        output_matrix_imag,
        skip_weight.reshape(-1, LANES),
        glu_bias.reshape(-1, LANES),
        mix_gain.reshape(-1, LANES),
        moe_gain.reshape(-1, LANES),
        eig_real,
        eig_imag,
        log_step.reshape(1, groups),
        routes.T,
        tokens,
    ]
    dec_r, dec_i, bt_r, bt_i, cm_r, cm_i, fac, choose, table, skip, bias, gain1, gain2, in_w, own = call(
        functools.partial(prep_body, n, cap),
        [jax.ShapeDtypeStruct((count, states), f32)] * 2
        + [jax.ShapeDtypeStruct((channels, pack * entries), bf16)] * 4
        + [
            jax.ShapeDtypeStruct((2, states), f32),
            jax.ShapeDtypeStruct((top, slots, count), bf16),
            jax.ShapeDtypeStruct((slots, count), bf16),
        ]
        + [jax.ShapeDtypeStruct((1, channels), f32)] * 2
        + [jax.ShapeDtypeStruct((1, full), f32)] * 2
        + [pltpu.VMEM((n, channels, wide), bf16), pltpu.VMEM((count, wide), bf16)],
        [FAR] * 16,
        [pltpu.VMEM(x.shape, x.dtype) for x in far[:-1]]
        + [pltpu.SemaphoreType.DMA((15,)), pltpu.SemaphoreType.DMA((n,))],
        limit=12 * 2**20,
    )(*[stay(x) for x in [in_weight] + far])
    pieces[0] = own

    new_r, new_i, activated = call(
        functools.partial(mixer_body, n),
        [
            jax.ShapeDtypeStruct((count, states), f32),
            jax.ShapeDtypeStruct((count, states), f32),
            jax.ShapeDtypeStruct((count, channels), bf16),
        ],
        [WHOLE] * (n + 10),
        limit=12 * 2**20,
    )(
        *pieces,
        gain1,
        in_w,
        bt_r,
        bt_i,
        fac,
        dec_r,
        dec_i,
        cm_r,
        cm_i,
        skip,
    )

    acts = gather_swaps(activated, n)
    glu_w, out_w = fetch(n, glu_weight, out_weight)
    parts = call(
        functools.partial(glu_body, n),
        [jax.ShapeDtypeStruct((n // 2, count, wide), bf16)] * 2,
        [WHOLE] * (n + 3),
        limit=12 * 2**20,
    )(*acts, glu_w, bias, out_w)

    terms = reduce_swaps(*parts, n)
    hidden = gate_weight.shape[1]
    gate_w, up_w, down_w = fetch(n, gate_weight, up_weight, down_weight)
    resid, *packed = call(
        functools.partial(dispatch_body, m, len(terms)),
        [jax.ShapeDtypeStruct((count, wide), bf16)]
        + [jax.ShapeDtypeStruct((exp_dev, cap, wide), bf16)] * m,
        [WHOLE] * (2 + len(terms)),
        limit=8 * 2**20,
    )(own, *terms, table)

    arrived = [packed[0]] + [swap(packed[j], "ep", j) for j in range(1, m)]
    half = m // 2
    fragments = []
    for group in (arrived[:half], arrived[half:]):
        merged = call(
            merge_body,
            jax.ShapeDtypeStruct((exp_dev, half * cap, wide), bf16),
            [WHOLE] * half,
            limit=2**20,
        )(*group)
        fragments += gather_swaps(merged, n)
    part = jax.ShapeDtypeStruct((n // 2, exp_dev, half * cap, wide), bf16)
    later, *far_outs = call(
        functools.partial(up_body, n),
        [jax.ShapeDtypeStruct((exp_dev, half * cap, hidden), bf16)] + [part] * 2,
        [WHOLE] * (2 * n + 4),
        limit=16 * 2**20,
    )(*fragments, gain2, gate_w, up_w, down_w)
    near_outs = call(
        functools.partial(down_body, n), [part] * 2, [WHOLE] * 2, limit=8 * 2**20
    )(later, down_w)
    back = [None] * m
    for outs, first in ((far_outs, half), (near_outs, 0)):
        terms = reduce_swaps(*outs, n)
        totals = call(
            functools.partial(total_body, half, len(terms)),
            [jax.ShapeDtypeStruct((exp_dev, cap, wide), bf16)] * half,
            [WHOLE] * len(terms),
            limit=4 * 2**20,
        )(*terms)
        for j in range(first, first + half):
            back[j] = swap(totals[j - first], "ep", j) if j else totals[0]
    new_r, new_i = call(
        unpack_body,
        [jax.ShapeDtypeStruct((count, groups, entries), f32)] * 2,
        [WHOLE] * 2,
        limit=4 * 2**20,
    )(new_r, new_i)
    result = call(
        functools.partial(combine_body, m),
        jax.ShapeDtypeStruct((count, wide), bf16),
        [WHOLE] * (3 + m),
        [pltpu.VMEM((slots, wide), bf16)],
        limit=8 * 2**20,
    )(resid, choose, route_weight.T, *back)
    return (
        result,
        new_r,
        new_i,
    )


def ssm_step(
    driven,
    state_real,
    state_imag,
    eig_real,
    eig_imag,
    log_step,
    input_real,
    input_imag,
    output_matrix_real,
    output_matrix_imag,
    skip_weight,
):
    highest_precision = lax.Precision.HIGHEST
    count_of_rows = driven.shape[0]
    groups = eig_real.shape[0]
    group_width = input_real.shape[2]
    time_step = jnp.exp(log_step)[:, None]
    magnitude = jnp.exp(eig_real * time_step)
    angle_now = eig_imag * time_step
    bar_real = magnitude * jnp.cos(angle_now)
    bar_imag = magnitude * jnp.sin(angle_now)
    modulus = eig_real * eig_real + eig_imag * eig_imag
    fac_real = ((bar_real - 1.0) * eig_real + bar_imag * eig_imag) / modulus
    fac_imag = (bar_imag * eig_real - (bar_real - 1.0) * eig_imag) / modulus
    ib_real = fac_real[..., None] * input_real - fac_imag[..., None] * input_imag
    ib_imag = fac_real[..., None] * input_imag + fac_imag[..., None] * input_real
    grouped = driven.astype(jnp.float32).reshape(count_of_rows, groups, group_width)
    push_real = jnp.einsum("gpc,ngc->ngp", ib_real, grouped, precision=highest_precision)
    push_imag = jnp.einsum("gpc,ngc->ngp", ib_imag, grouped, precision=highest_precision)
    updated_state_real = bar_real[None] * state_real - bar_imag[None] * state_imag + push_real
    updated_state_imag = bar_real[None] * state_imag + bar_imag[None] * state_real + push_imag
    state_readout = jnp.einsum(
        "jiy,sjy->sji", output_matrix_real, updated_state_real, precision=highest_precision
    ) - jnp.einsum(
        "jiy,sjy->sji", output_matrix_imag, updated_state_imag, precision=highest_precision
    )
    state_readout = state_readout.reshape(count_of_rows, groups * group_width) + skip_weight[
        None, :
    ] * driven.astype(jnp.float32)
    activated = jax.nn.gelu(state_readout).astype(jnp.bfloat16)
    return (updated_state_real, updated_state_imag, activated)


def local(
    tokens,
    state_real,
    state_imag,
    mix_gain,
    in_weight,
    eig_real,
    eig_imag,
    log_step,
    input_real,
    input_imag,
    output_matrix_real,
    output_matrix_imag,
    skip_weight,
    glu_weight,
    glu_bias,
    out_weight,
    moe_gain,
    routes,
    route_weight,
    gate_weight,
    up_weight,
    down_weight,
):
    count_of_rows = tokens.shape[0]
    n_ep = lax.axis_size("ep")
    width_tp = lax.axis_size("tp")
    whole_rows = lax.all_gather(tokens, "tp", axis=1, tiled=True)
    whole_float = whole_rows.astype(jnp.float32)
    first_scale = lax.rsqrt(jnp.mean(whole_float * whole_float, axis=1, keepdims=True) + norm_eps)
    normed = (whole_float * first_scale * mix_gain.astype(jnp.float32)).astype(jnp.bfloat16)
    driven = jnp.einsum("rd,cd->rc", normed, in_weight, preferred_element_type=jnp.float32).astype(
        jnp.bfloat16
    )
    updated_state_real, updated_state_imag, activated = ssm_step(
        driven,
        state_real,
        state_imag,
        eig_real,
        eig_imag,
        log_step,
        input_real,
        input_imag,
        output_matrix_real,
        output_matrix_imag,
        skip_weight,
    )
    gate_pre = (
        jnp.einsum(
            "rc,oc->ro",
            lax.all_gather(activated, "tp", axis=1, tiled=True),
            glu_weight,
            preferred_element_type=jnp.float32,
        )
        + glu_bias
    )
    glued = (activated.astype(jnp.float32) * jax.nn.sigmoid(gate_pre)).astype(jnp.bfloat16)
    partial_value = jnp.dot(glued, out_weight, preferred_element_type=jnp.float32)
    mixed = lax.psum_scatter(
        partial_value.astype(jnp.bfloat16), "tp", scatter_dimension=1, tiled=True
    ).astype(jnp.float32)
    residual = (tokens.astype(jnp.float32) + mixed).astype(jnp.bfloat16)
    resid_float = residual.astype(jnp.float32)
    exp_dev = gate_weight.shape[0]
    experts = exp_dev * n_ep
    top_count = routes.shape[1]
    capacity = max(2, (3 * top_count * count_of_rows + 2 * experts - 1) // (2 * experts))
    chosen = routes.reshape(-1)
    onehot = (chosen[:, None] == jnp.arange(experts, dtype=jnp.int32)[None, :]).astype(jnp.int32)
    rank_index = jnp.sum((jnp.cumsum(onehot, axis=0) - onehot) * onehot, axis=1)
    slot_index = (chosen * capacity + rank_index).reshape(count_of_rows, top_count)
    slots_all = experts * capacity
    choose = slot_index[:, :, None] == jnp.arange(slots_all, dtype=jnp.int32)[None, None, :]
    dispatch = jnp.sum(choose.astype(jnp.float32), axis=1).astype(jnp.bfloat16)
    local_sq = jnp.sum(resid_float * resid_float, axis=1)
    total_sq = lax.psum(local_sq, "tp")
    dim_full = residual.shape[1] * width_tp
    second_scale = lax.rsqrt(total_sq[:, None] / dim_full + norm_eps)
    gain_part = lax.dynamic_slice_in_dim(
        moe_gain, lax.axis_index("tp") * residual.shape[1], residual.shape[1], 0
    )
    expert_in = (resid_float * second_scale * gain_part.astype(jnp.float32)).astype(jnp.bfloat16)
    packed = jnp.einsum(
        "rs,rd->sd", dispatch, expert_in, preferred_element_type=jnp.float32
    ).astype(jnp.bfloat16)
    packed = packed.reshape(n_ep, exp_dev * capacity, residual.shape[1])
    arrived = lax.all_to_all(packed, "ep", split_axis=0, concat_axis=0, tiled=True)
    arrived = arrived.reshape(n_ep, exp_dev, capacity, residual.shape[1])
    fragment = lax.all_gather(arrived, "tp", axis=3, tiled=True)
    gate_part = jnp.einsum(
        "necd,efd->necf", fragment, gate_weight, preferred_element_type=jnp.float32
    )
    up_part = jnp.einsum("necd,efd->necf", fragment, up_weight, preferred_element_type=jnp.float32)
    hidden_width = (jax.nn.silu(gate_part) * up_part).astype(jnp.bfloat16)
    partial_out = jnp.einsum(
        "necf,efd->necd", hidden_width, down_weight, preferred_element_type=jnp.float32
    )
    summed = lax.psum_scatter(
        partial_out.astype(jnp.bfloat16), "tp", scatter_dimension=3, tiled=True
    )
    summed = summed.reshape(n_ep, exp_dev * capacity, summed.shape[3])
    returned = lax.all_to_all(summed, "ep", split_axis=0, concat_axis=0, tiled=True)
    returned = returned.reshape(slots_all, returned.shape[2])
    gathered_k = jnp.einsum(
        "rks,sd->rkd", choose.astype(jnp.bfloat16), returned, preferred_element_type=jnp.float32
    )
    result = (resid_float + jnp.sum(route_weight[..., None] * gathered_k, axis=1)).astype(
        jnp.bfloat16
    )
    return (result, updated_state_real, updated_state_imag)


def solution(mesh):
    n, m = mesh.shape["tp"], mesh.shape["ep"]
    small = n in (4, 8) and m in (2, 4)

    def whole(*args):
        if not small:
            return local(*args)
        return local_swaps(*args)

    return jax.shard_map(
        whole,
        mesh=mesh,
        in_specs=(
            P("ep", "tp"),
            P("ep", "tp", None),
            P("ep", "tp", None),
            P(),
            P("tp", None),
            P("tp", None),
            P("tp", None),
            P("tp"),
            P("tp", None, None),
            P("tp", None, None),
            P("tp", None, None),
            P("tp", None, None),
            P("tp"),
            P("tp", None),
            P("tp"),
            P("tp", None),
            P(),
            P("ep", None),
            P("ep", None),
            P("ep", "tp", None),
            P("ep", "tp", None),
            P("ep", "tp", None),
        ),
        out_specs=(P("ep", "tp"), P("ep", "tp", None), P("ep", "tp", None)),
        check_vma=False,
    )
```

```python
import functools
import jax
import jax.numpy as jnp
from jax import lax
from jax.experimental import pallas as pl
from jax.experimental.pallas import tpu as pltpu
from jax.sharding import PartitionSpec as P


norm_eps = 1e-06
f32 = jnp.float32
bf16 = jnp.bfloat16
NT = (((1,), (1,)), ((), ()))
NN = (((1,), (0,)), ((), ()))
WHOLE = pl.BlockSpec(memory_space=pltpu.VMEM)
FAR = pl.BlockSpec(memory_space=pltpu.HBM)
LANES = 128


def stay(x):
    return pltpu.with_memory_space_constraint(x, pltpu.HBM)


def dot(a, b, dims):
    return lax.dot_general(a, b, dims, preferred_element_type=f32)


def swap(x, axis, k):
    return lax.ppermute(x, axis, [(i, i ^ k) for i in range(lax.axis_size(axis))])


def gather_swaps(x, n):
    pieces = [None] * n
    pieces[0] = x
    for k in range(2, n, 2):
        pieces[k] = swap(x, "tp", k)
    for k in range(0, n, 2):
        pieces[k ^ 1] = swap(pieces[k], "tp", 1)
    return pieces


def pair_swaps(own, partner, n):
    other = swap(partner, "tp", 1)
    shape = own.shape[1:]
    return call(
        pair_body,
        [jax.ShapeDtypeStruct(shape, f32)] + [jax.ShapeDtypeStruct(shape, bf16)] * (n // 2 - 1),
        [WHOLE] * 2,
        limit=8 * 2**20,
    )(own, other)


def reduce_swaps(own, partner, n):
    first, *rest = pair_swaps(own, partner, n)
    return [first] + [swap(x, "tp", k) for x, k in zip(rest, range(2, n, 2))]


def pair_body(own, other, *outs):
    for i, out in enumerate(outs):
        out[...] = (own[i].astype(f32) + other[i].astype(f32)).astype(out.dtype)


def call(body, out_shape, in_specs, scratch=(), limit=None, flops=10**7):
    single = not isinstance(out_shape, (list, tuple))
    return pl.pallas_call(
        body,
        out_shape=out_shape,
        in_specs=in_specs,
        out_specs=WHOLE if single else [WHOLE] * len(out_shape),
        scratch_shapes=list(scratch),
        compiler_params=pltpu.CompilerParams(vmem_limit_bytes=limit),
        cost_estimate=pl.CostEstimate(flops=flops, bytes_accessed=10**6, transcendentals=0),
    )


def column(row):
    n = row.shape[1]
    at = lax.broadcasted_iota(jnp.int32, (n, n), 0)
    to = lax.broadcasted_iota(jnp.int32, (n, n), 1)
    return jnp.sum(jnp.where(at == to, jnp.broadcast_to(row, (n, n)), 0.0), axis=1, keepdims=True)


def place(k, width):
    return pl.ds(pl.multiple_of((lax.axis_index("tp") ^ k) * width, width), width)


def prep_body(n, cap, *refs):
    weight_hbm = refs[0]
    far = refs[1:16]
    dec_r, dec_i, bt_r, bt_i, base, mix, choose, table = refs[16:24]
    flat = refs[24:28]
    weight, tokens = refs[28:30]
    held = refs[30:44]
    sems, weight_sems, fac = refs[44:]
    held = (*held, tokens)
    copies = [pltpu.make_async_copy(a, b, sems.at[i]) for i, (a, b) in enumerate(zip(far, held))]
    for copy in copies:
        copy.start()
    weights = load(weight_hbm, weight, weight_sems, n, weight.shape[2])
    copies[13].wait()
    routes = held[13]
    slots, count = table.shape
    top = routes.shape[0]
    names = lax.broadcasted_iota(jnp.int32, (16, count), 0)
    marks = [(routes[r : r + 1, :] == names).astype(f32) for r in range(top)]
    total = marks[0]
    for r in range(1, top):
        total = total + marks[r]
    row = lax.broadcasted_iota(jnp.int32, (count, count), 0)
    col = lax.broadcasted_iota(jnp.int32, (count, count), 1)
    before = dot(total.astype(bf16), (row < col).astype(bf16), NN)
    same = (row == col).astype(bf16)
    places = lax.broadcasted_iota(jnp.int32, (slots, count), 0).astype(f32)
    used = jnp.zeros((slots, count), f32)
    for r in range(top):
        rank = jnp.sum(before * marks[r], axis=0, keepdims=True)
        slot = routes[r : r + 1, :].astype(f32) * cap + rank
        hit = (places == slot).astype(f32)
        choose[r] = dot(same, hit.astype(bf16), NT).astype(bf16)
        used = used + hit
    table[...] = used.astype(bf16)
    st_r, st_i, in_r, in_i, om_r, om_i = held[:6]
    groups, inner, entries = in_r.shape
    pack = LANES // inner
    in_r, in_i, om_r, om_i = (x for x in held[2:6])
    for i in range(2, 6):
        copies[i].wait()
    for i in (0, 1, 10, 11, 12):
        copies[i].wait()
    real, imag, log_step = held[10][...], held[11][...], held[12][...]
    step = column(jnp.exp(log_step))
    size = jnp.exp(real * step)
    angle = imag * step
    bar_r = size * jnp.cos(angle)
    bar_i = size * jnp.sin(angle)
    modulus = real * real + imag * imag
    fac_r = ((bar_r - 1.0) * real + bar_i * imag) / modulus
    fac_i = (bar_i * real - (bar_r - 1.0) * imag) / modulus
    for g in range(groups):
        cols = slice(g * entries, (g + 1) * entries)
        s_r, s_i = st_r[:, g, :], st_i[:, g, :]
        b_r, b_i = bar_r[g : g + 1, :], bar_i[g : g + 1, :]
        dec_r[:, cols] = b_r * s_r - b_i * s_i
        dec_i[:, cols] = b_r * s_i + b_i * s_r
        fac[0:1, cols] = fac_r[g : g + 1, :]
        fac[1:2, cols] = fac_i[g : g + 1, :]
    high = pack * entries
    for b in range(groups // pack):
        each = slice(b * pack, (b + 1) * pack)
        lanes = slice(b * LANES, (b + 1) * LANES)
        rows = slice(b * high, (b + 1) * high)
        b_r, b_i, c_r, c_i = (
            spread(x[each].reshape(LANES, entries), inner, pack) for x in (in_r, in_i, om_r, om_i)
        )
        f_r, f_i = fac[0:1, rows], fac[1:2, rows]
        i_r = (f_r * b_r - f_i * b_i).astype(bf16)
        i_i = (f_r * b_i + f_i * b_r).astype(bf16)
        c_r, c_i = c_r.astype(bf16), c_i.astype(bf16)
        bt_r[lanes, :] = i_r
        bt_i[lanes, :] = i_i
        mix[lanes, :] = (dot(i_r, c_r, NT) - dot(i_i, c_i, NT)).astype(bf16)
        base[:, lanes] = dot(dec_r[:, rows].astype(bf16), c_r, NT) - dot(
            dec_i[:, rows].astype(bf16), c_i, NT
        )
    for i in range(len(flat)):
        copies[6 + i].wait()
        rows = held[6 + i][...].astype(f32)
        for r in range(rows.shape[0]):
            flat[i][0:1, r * LANES : (r + 1) * LANES] = rows[r : r + 1, :]
    copies[14].wait()
    for copy in weights:
        copy.wait()


def spread(blocks, height, pack):
    rows, inner = blocks.shape
    columns = pack * inner
    at = lax.broadcasted_iota(jnp.int32, (inner, columns), 0)
    to = lax.broadcasted_iota(jnp.int32, (inner, columns), 1)
    wide = dot(blocks.astype(bf16), (to % inner == at).astype(bf16), NN)
    row = lax.broadcasted_iota(jnp.int32, (rows, columns), 0)
    col = lax.broadcasted_iota(jnp.int32, (rows, columns), 1)
    return jnp.where(row // height == col // inner, wide, 0.0)


def load(src, dst, sems, n, width):
    copies = []
    for k in range(n):
        part = src.at[:, place(k, width)] if len(src.shape) == 2 else src.at[:, :, place(k, width)]
        copies.append(pltpu.make_async_copy(part, dst.at[k], sems.at[k]))
    for copy in copies:
        copy.start()
    return copies


def mixer_body(n, *refs):
    pieces = refs[:n]
    gain, weight, base, mix, skip = refs[n : n + 5]
    driven_ref, act_ref = refs[n + 5 :]
    width = pieces[0].shape[1]
    square = 0.0
    for k in range(n):
        x = pieces[k][...].astype(f32)
        square = square + jnp.sum(x * x, axis=1, keepdims=True)
    scale = lax.rsqrt(square / (n * width) + norm_eps)
    total = 0.0
    for k in range(n):
        part = gain[:, place(k, width)]
        normed = (pieces[k][...].astype(f32) * scale * part).astype(bf16)
        total = total + dot(normed, weight[k], NT)
    driven = total.astype(bf16)
    driven_ref[...] = driven
    for b in range(driven.shape[1] // LANES):
        lanes = slice(b * LANES, (b + 1) * LANES)
        out = base[:, lanes] + dot(driven[:, lanes], mix[lanes, :], NN)
        out = out + skip[:, lanes] * driven[:, lanes].astype(f32)
        act_ref[:, lanes] = jax.nn.gelu(out).astype(bf16)


def state_body(driven, dec_r, dec_i, bt_r, bt_i, out_r, out_i):
    groups, entries = out_r.shape[1:]
    high = bt_r.shape[1]
    pack = high // entries
    for dec, bt, out in ((dec_r, bt_r, out_r), (dec_i, bt_i, out_i)):
        for b in range(groups // pack):
            lanes = slice(b * LANES, (b + 1) * LANES)
            new = dec[:, b * high : (b + 1) * high] + dot(driven[:, lanes], bt[lanes, :], NN)
            for g in range(pack):
                out[:, b * pack + g, :] = new[:, g * entries : (g + 1) * entries]


def fetch_body(n, count, *refs):
    copies = []
    for i in range(count):
        src, dst, sems = refs[i], refs[count + i], refs[2 * count + i]
        copies += load(src, dst, sems, n, dst.shape[-1])
    for copy in copies:
        copy.wait()


def fetch(n, *sources):
    shapes = [(n, *x.shape[:-1], x.shape[-1] // n) for x in sources]
    return call(
        functools.partial(fetch_body, n, len(sources)),
        [pltpu.VMEM(x, bf16) for x in shapes],
        [FAR] * len(sources),
        [pltpu.SemaphoreType.DMA((n,))] * len(sources),
        limit=2**20,
    )(*[stay(x) for x in sources])


def glu_body(n, *refs):
    pieces = refs[:n]
    glu, bias, out_w = refs[n : n + 3]
    glued_ref, partner = refs[n + 3 :]
    gate = bias[...]
    for k in range(n):
        gate = gate + dot(pieces[k][...], glu[k], NT)
    glued = (pieces[0][...].astype(f32) * jax.nn.sigmoid(gate)).astype(bf16)
    glued_ref[...] = glued
    for k in range(1, n, 2):
        partner[k // 2] = dot(glued, out_w[k], NN).astype(bf16)


def out_body(n, glued, out_w, own):
    for k in range(0, n, 2):
        own[k // 2] = dot(glued[...], out_w[k], NN).astype(bf16)


def merge_body(*refs):
    out = refs[-1]
    cap = refs[0].shape[1]
    for j, x in enumerate(refs[:-1]):
        out[:, j * cap : (j + 1) * cap, :] = x[...]


def dispatch_body(m, terms, *refs):
    tokens = refs[0]
    sums = refs[1 : 1 + terms]
    table = refs[1 + terms]
    resid_ref = refs[2 + terms]
    outs = refs[3 + terms :]
    mixed = sums[0][...]
    for s in sums[1:]:
        mixed = mixed + s[...].astype(f32)
    resid = (tokens[...].astype(f32) + mixed).astype(bf16)
    resid_ref[...] = resid
    experts, cap, wide = outs[0].shape
    count = experts * cap
    for j in range(m):
        at = pl.multiple_of((lax.axis_index("ep") ^ j) * count, count)
        picked = dot(table[pl.ds(at, count), :], resid, NN).astype(bf16)
        outs[j][...] = picked.reshape(experts, cap, wide)


def up_body(n, *refs):
    near, far = refs[:n], refs[n : 2 * n]
    gain, gate_w, up_w, down_w = refs[2 * n : 2 * n + 4]
    later, partner = refs[2 * n + 4 :]
    experts, count, width = near[0].shape
    g, u, square = [0.0] * experts, [0.0] * experts, [0.0] * experts
    for k in range(n):
        part = gain[:, place(k, width)]
        for i in range(experts):
            x = jnp.concatenate([near[k][i], far[k][i]], axis=0).astype(f32)
            square[i] = square[i] + jnp.sum(x * x, axis=1, keepdims=True)
            x = (x * part).astype(bf16)
            g[i] = g[i] + dot(gate_w[k, i], x, NT)
            u[i] = u[i] + dot(up_w[k, i], x, NT)
    for i in range(experts):
        scale = lax.rsqrt(square[i] / (n * width) + norm_eps)
        hidden = (jax.nn.silu(g[i].T * scale) * (u[i].T * scale)).astype(bf16)
        later[i] = hidden
        for k in range(1, n, 2):
            partner[k // 2, i] = dot(hidden[count:], down_w[k, i], NN).astype(bf16)


def down_body(n, hidden, down_w, far_own, own, partner):
    count = own.shape[2]
    for i in range(hidden.shape[0]):
        near, far = hidden[i, :count], hidden[i, count:]
        for k in range(0, n, 2):
            far_own[k // 2, i] = dot(far, down_w[k, i], NN).astype(bf16)
        for k in range(1, n, 2):
            partner[k // 2, i] = dot(near, down_w[k, i], NN).astype(bf16)
        for k in range(0, n, 2):
            own[k // 2, i] = dot(near, down_w[k, i], NN).astype(bf16)


def total_body(m, terms, *refs):
    sums = refs[:terms]
    outs = refs[terms:]
    total = sums[0][...]
    for s in sums[1:]:
        total = total + s[...].astype(f32)
    total = total.astype(bf16)
    cap = outs[0].shape[1]
    for j in range(m):
        outs[j][...] = total[:, j * cap : (j + 1) * cap, :]


def combine_body(m, *refs):
    resid, choose, weight = refs[:3]
    back = refs[3 : 3 + m]
    out, rows = refs[3 + m :]
    experts, cap, wide = back[0].shape
    count = experts * cap
    for j in range(m):
        at = pl.multiple_of((lax.axis_index("ep") ^ j) * count, count)
        rows[pl.ds(at, count), :] = back[j][...].reshape(count, wide)
    total = resid[...].astype(f32)
    for r in range(weight.shape[0]):
        picked = dot(choose[r], rows[...], NN)
        total = total + column(weight[r : r + 1, :]) * picked
    out[...] = total.astype(bf16)


def local_swaps(
    tokens,
    state_real,
    state_imag,
    mix_gain,
    in_weight,
    eig_real,
    eig_imag,
    log_step,
    input_real,
    input_imag,
    output_matrix_real,
    output_matrix_imag,
    skip_weight,
    glu_weight,
    glu_bias,
    out_weight,
    moe_gain,
    routes,
    route_weight,
    gate_weight,
    up_weight,
    down_weight,
):
    count, wide = tokens.shape
    n = lax.axis_size("tp")
    m = lax.axis_size("ep")
    groups, entries = eig_real.shape
    inner = input_real.shape[2]
    states = groups * entries
    channels = groups * inner
    full = wide * n
    exp_dev = gate_weight.shape[0]
    experts = exp_dev * m
    top = routes.shape[1]
    cap = max(2, (3 * top * count + 2 * experts - 1) // (2 * experts))
    slots = experts * cap

    pieces = gather_swaps(tokens, n)
    pack = LANES // inner
    far = [
        state_real,
        state_imag,
        input_real.transpose(0, 2, 1),
        input_imag.transpose(0, 2, 1),
        output_matrix_real,
        output_matrix_imag,
        skip_weight.reshape(-1, LANES),
        glu_bias.reshape(-1, LANES),
        mix_gain.reshape(-1, LANES),
        moe_gain.reshape(-1, LANES),
        eig_real,
        eig_imag,
        log_step.reshape(1, groups),
        routes.T,
        tokens,
    ]
    dec_r, dec_i, bt_r, bt_i, base, mix, choose, table, skip, bias, gain1, gain2, in_w, own = call(
        functools.partial(prep_body, n, cap),
        [jax.ShapeDtypeStruct((count, states), f32)] * 2
        + [jax.ShapeDtypeStruct((channels, pack * entries), bf16)] * 2
        + [
            jax.ShapeDtypeStruct((count, channels), f32),
            jax.ShapeDtypeStruct((channels, LANES), bf16),
            jax.ShapeDtypeStruct((top, count, slots), bf16),
            jax.ShapeDtypeStruct((slots, count), bf16),
        ]
        + [jax.ShapeDtypeStruct((1, channels), f32)] * 2
        + [jax.ShapeDtypeStruct((1, full), f32)] * 2
        + [pltpu.VMEM((n, channels, wide), bf16), pltpu.VMEM((count, wide), bf16)],
        [FAR] * 16,
        [pltpu.VMEM(x.shape, x.dtype) for x in far[:-1]]
        + [pltpu.SemaphoreType.DMA((15,)), pltpu.SemaphoreType.DMA((n,))]
        + [pltpu.VMEM((2, states), f32)],
        limit=12 * 2**20,
    )(*[stay(x) for x in [in_weight] + far])
    pieces[0] = own

    driven, activated = call(
        functools.partial(mixer_body, n),
        [jax.ShapeDtypeStruct((count, channels), bf16)] * 2,
        [WHOLE] * (n + 5),
        limit=12 * 2**20,
    )(*pieces, gain1, in_w, base, mix, skip)

    acts = gather_swaps(activated, n)
    glu_w, out_w = fetch(n, glu_weight, out_weight)
    block = jax.ShapeDtypeStruct((n // 2, count, wide), bf16)
    glued, partner = call(
        functools.partial(glu_body, n),
        [jax.ShapeDtypeStruct((count, channels), bf16), block],
        [WHOLE] * (n + 3),
        limit=12 * 2**20,
    )(*acts, glu_w, bias, out_w)
    sums = call(functools.partial(out_body, n), block, [WHOLE] * 2, limit=8 * 2**20)(glued, out_w)

    terms = reduce_swaps(sums, partner, n)
    hidden = gate_weight.shape[1]
    gate_w, up_w = fetch(n, gate_weight, up_weight)
    (down_w,) = fetch(n, down_weight)
    resid, *packed = call(
        functools.partial(dispatch_body, m, len(terms)),
        [jax.ShapeDtypeStruct((count, wide), bf16)]
        + [jax.ShapeDtypeStruct((exp_dev, cap, wide), bf16)] * m,
        [WHOLE] * (2 + len(terms)),
        limit=8 * 2**20,
    )(own, *terms, table)

    arrived = [packed[0]] + [swap(packed[j], "ep", j) for j in range(1, m)]
    half = m // 2
    fragments = []
    for group in (arrived[:half], arrived[half:]):
        merged = call(
            merge_body,
            jax.ShapeDtypeStruct((exp_dev, half * cap, wide), bf16),
            [WHOLE] * half,
            limit=2**20,
        )(*group)
        fragments += gather_swaps(merged, n)
    part = jax.ShapeDtypeStruct((n // 2, exp_dev, half * cap, wide), bf16)
    later, far_partner = call(
        functools.partial(up_body, n),
        [jax.ShapeDtypeStruct((exp_dev, 2 * half * cap, hidden), bf16), part],
        [WHOLE] * (2 * n + 4),
        limit=16 * 2**20,
    )(*fragments, gain2, gate_w, up_w, down_w)
    far_own, *near_outs = call(
        functools.partial(down_body, n), [part] * 3, [WHOLE] * 2, limit=8 * 2**20
    )(later, down_w)
    far_outs = [far_own, far_partner]
    back = [None] * m
    for outs, first in ((far_outs, half), (near_outs, 0)):
        terms = reduce_swaps(*outs, n)
        totals = call(
            functools.partial(total_body, half, len(terms)),
            [jax.ShapeDtypeStruct((exp_dev, cap, wide), bf16)] * half,
            [WHOLE] * len(terms),
            limit=4 * 2**20,
        )(*terms)
        for j in range(first, first + half):
            back[j] = swap(totals[j - first], "ep", j) if j else totals[0]
    new_r, new_i = call(
        state_body,
        [jax.ShapeDtypeStruct((count, groups, entries), f32)] * 2,
        [WHOLE] * 5,
        limit=4 * 2**20,
    )(driven, dec_r, dec_i, bt_r, bt_i)
    result = call(
        functools.partial(combine_body, m),
        jax.ShapeDtypeStruct((count, wide), bf16),
        [WHOLE] * (3 + m),
        [pltpu.VMEM((slots, wide), bf16)],
        limit=8 * 2**20,
    )(resid, choose, route_weight.T, *back)
    return (
        result,
        new_r,
        new_i,
    )


def ssm_step(
    driven,
    state_real,
    state_imag,
    eig_real,
    eig_imag,
    log_step,
    input_real,
    input_imag,
    output_matrix_real,
    output_matrix_imag,
    skip_weight,
):
    highest_precision = lax.Precision.HIGHEST
    count_of_rows = driven.shape[0]
    groups = eig_real.shape[0]
    group_width = input_real.shape[2]
    time_step = jnp.exp(log_step)[:, None]
    magnitude = jnp.exp(eig_real * time_step)
    angle_now = eig_imag * time_step
    bar_real = magnitude * jnp.cos(angle_now)
    bar_imag = magnitude * jnp.sin(angle_now)
    modulus = eig_real * eig_real + eig_imag * eig_imag
    fac_real = ((bar_real - 1.0) * eig_real + bar_imag * eig_imag) / modulus
    fac_imag = (bar_imag * eig_real - (bar_real - 1.0) * eig_imag) / modulus
    ib_real = fac_real[..., None] * input_real - fac_imag[..., None] * input_imag
    ib_imag = fac_real[..., None] * input_imag + fac_imag[..., None] * input_real
    grouped = driven.astype(jnp.float32).reshape(count_of_rows, groups, group_width)
    push_real = jnp.einsum("gpc,ngc->ngp", ib_real, grouped, precision=highest_precision)
    push_imag = jnp.einsum("gpc,ngc->ngp", ib_imag, grouped, precision=highest_precision)
    updated_state_real = bar_real[None] * state_real - bar_imag[None] * state_imag + push_real
    updated_state_imag = bar_real[None] * state_imag + bar_imag[None] * state_real + push_imag
    state_readout = jnp.einsum(
        "jiy,sjy->sji", output_matrix_real, updated_state_real, precision=highest_precision
    ) - jnp.einsum(
        "jiy,sjy->sji", output_matrix_imag, updated_state_imag, precision=highest_precision
    )
    state_readout = state_readout.reshape(count_of_rows, groups * group_width) + skip_weight[
        None, :
    ] * driven.astype(jnp.float32)
    activated = jax.nn.gelu(state_readout).astype(jnp.bfloat16)
    return (updated_state_real, updated_state_imag, activated)


def local(
    tokens,
    state_real,
    state_imag,
    mix_gain,
    in_weight,
    eig_real,
    eig_imag,
    log_step,
    input_real,
    input_imag,
    output_matrix_real,
    output_matrix_imag,
    skip_weight,
    glu_weight,
    glu_bias,
    out_weight,
    moe_gain,
    routes,
    route_weight,
    gate_weight,
    up_weight,
    down_weight,
):
    count_of_rows = tokens.shape[0]
    n_ep = lax.axis_size("ep")
    width_tp = lax.axis_size("tp")
    whole_rows = lax.all_gather(tokens, "tp", axis=1, tiled=True)
    whole_float = whole_rows.astype(jnp.float32)
    first_scale = lax.rsqrt(jnp.mean(whole_float * whole_float, axis=1, keepdims=True) + norm_eps)
    normed = (whole_float * first_scale * mix_gain.astype(jnp.float32)).astype(jnp.bfloat16)
    driven = jnp.einsum("rd,cd->rc", normed, in_weight, preferred_element_type=jnp.float32).astype(
        jnp.bfloat16
    )
    updated_state_real, updated_state_imag, activated = ssm_step(
        driven,
        state_real,
        state_imag,
        eig_real,
        eig_imag,
        log_step,
        input_real,
        input_imag,
        output_matrix_real,
        output_matrix_imag,
        skip_weight,
    )
    gate_pre = (
        jnp.einsum(
            "rc,oc->ro",
            lax.all_gather(activated, "tp", axis=1, tiled=True),
            glu_weight,
            preferred_element_type=jnp.float32,
        )
        + glu_bias
    )
    glued = (activated.astype(jnp.float32) * jax.nn.sigmoid(gate_pre)).astype(jnp.bfloat16)
    partial_value = jnp.dot(glued, out_weight, preferred_element_type=jnp.float32)
    mixed = lax.psum_scatter(
        partial_value.astype(jnp.bfloat16), "tp", scatter_dimension=1, tiled=True
    ).astype(jnp.float32)
    residual = (tokens.astype(jnp.float32) + mixed).astype(jnp.bfloat16)
    resid_float = residual.astype(jnp.float32)
    exp_dev = gate_weight.shape[0]
    experts = exp_dev * n_ep
    top_count = routes.shape[1]
    capacity = max(2, (3 * top_count * count_of_rows + 2 * experts - 1) // (2 * experts))
    chosen = routes.reshape(-1)
    onehot = (chosen[:, None] == jnp.arange(experts, dtype=jnp.int32)[None, :]).astype(jnp.int32)
    rank_index = jnp.sum((jnp.cumsum(onehot, axis=0) - onehot) * onehot, axis=1)
    slot_index = (chosen * capacity + rank_index).reshape(count_of_rows, top_count)
    slots_all = experts * capacity
    choose = slot_index[:, :, None] == jnp.arange(slots_all, dtype=jnp.int32)[None, None, :]
    dispatch = jnp.sum(choose.astype(jnp.float32), axis=1).astype(jnp.bfloat16)
    local_sq = jnp.sum(resid_float * resid_float, axis=1)
    total_sq = lax.psum(local_sq, "tp")
    dim_full = residual.shape[1] * width_tp
    second_scale = lax.rsqrt(total_sq[:, None] / dim_full + norm_eps)
    gain_part = lax.dynamic_slice_in_dim(
        moe_gain, lax.axis_index("tp") * residual.shape[1], residual.shape[1], 0
    )
    expert_in = (resid_float * second_scale * gain_part.astype(jnp.float32)).astype(jnp.bfloat16)
    packed = jnp.einsum(
        "rs,rd->sd", dispatch, expert_in, preferred_element_type=jnp.float32
    ).astype(jnp.bfloat16)
    packed = packed.reshape(n_ep, exp_dev * capacity, residual.shape[1])
    arrived = lax.all_to_all(packed, "ep", split_axis=0, concat_axis=0, tiled=True)
    arrived = arrived.reshape(n_ep, exp_dev, capacity, residual.shape[1])
    fragment = lax.all_gather(arrived, "tp", axis=3, tiled=True)
    gate_part = jnp.einsum(
        "necd,efd->necf", fragment, gate_weight, preferred_element_type=jnp.float32
    )
    up_part = jnp.einsum("necd,efd->necf", fragment, up_weight, preferred_element_type=jnp.float32)
    hidden_width = (jax.nn.silu(gate_part) * up_part).astype(jnp.bfloat16)
    partial_out = jnp.einsum(
        "necf,efd->necd", hidden_width, down_weight, preferred_element_type=jnp.float32
    )
    summed = lax.psum_scatter(
        partial_out.astype(jnp.bfloat16), "tp", scatter_dimension=3, tiled=True
    )
    summed = summed.reshape(n_ep, exp_dev * capacity, summed.shape[3])
    returned = lax.all_to_all(summed, "ep", split_axis=0, concat_axis=0, tiled=True)
    returned = returned.reshape(slots_all, returned.shape[2])
    gathered_k = jnp.einsum(
        "rks,sd->rkd", choose.astype(jnp.bfloat16), returned, preferred_element_type=jnp.float32
    )
    result = (resid_float + jnp.sum(route_weight[..., None] * gathered_k, axis=1)).astype(
        jnp.bfloat16
    )
    return (result, updated_state_real, updated_state_imag)


def solution(mesh):
    n, m = mesh.shape["tp"], mesh.shape["ep"]
    small = n in (4, 8) and m in (2, 4)

    def whole(*args):
        if not small:
            return local(*args)
        return local_swaps(*args)

    return jax.shard_map(
        whole,
        mesh=mesh,
        in_specs=(
            P("ep", "tp"),
            P("ep", "tp", None),
            P("ep", "tp", None),
            P(),
            P("tp", None),
            P("tp", None),
            P("tp", None),
            P("tp"),
            P("tp", None, None),
            P("tp", None, None),
            P("tp", None, None),
            P("tp", None, None),
            P("tp"),
            P("tp", None),
            P("tp"),
            P("tp", None),
            P(),
            P("ep", None),
            P("ep", None),
            P("ep", "tp", None),
            P("ep", "tp", None),
            P("ep", "tp", None),
        ),
        out_specs=(P("ep", "tp"), P("ep", "tp", None), P("ep", "tp", None)),
        check_vma=False,
    )
```

```python
import functools
import jax
import jax.numpy as jnp
from jax import lax
from jax.experimental import pallas as pl
from jax.experimental.pallas import tpu as pltpu
from jax.sharding import PartitionSpec as P


norm_eps = 1e-06
f32 = jnp.float32
bf16 = jnp.bfloat16
NT = (((1,), (1,)), ((), ()))
NN = (((1,), (0,)), ((), ()))
WHOLE = pl.BlockSpec(memory_space=pltpu.VMEM)
FAR = pl.BlockSpec(memory_space=pltpu.HBM)
LANES = 128


def stay(x):
    return pltpu.with_memory_space_constraint(x, pltpu.HBM)


def dot(a, b, dims):
    return lax.dot_general(a, b, dims, preferred_element_type=f32)


def swap(x, axis, k):
    return lax.ppermute(x, axis, [(i, i ^ k) for i in range(lax.axis_size(axis))])


def gather_swaps(x, n):
    pieces = [None] * n
    pieces[0] = x
    for k in range(2, n, 2):
        pieces[k] = swap(x, "tp", k)
    for k in range(0, n, 2):
        pieces[k ^ 1] = swap(pieces[k], "tp", 1)
    return pieces


def pair_swaps(own, partner, n):
    other = swap(partner, "tp", 1)
    shape = own.shape[1:]
    return call(
        pair_body,
        [jax.ShapeDtypeStruct(shape, f32)] + [jax.ShapeDtypeStruct(shape, bf16)] * (n // 2 - 1),
        [WHOLE] * 2,
        limit=8 * 2**20,
    )(own, other)


def reduce_swaps(own, partner, n):
    first, *rest = pair_swaps(own, partner, n)
    return [first] + [swap(x, "tp", k) for x, k in zip(rest, range(2, n, 2))]


def pair_body(own, other, *outs):
    for i, out in enumerate(outs):
        out[...] = (own[i].astype(f32) + other[i].astype(f32)).astype(out.dtype)


def call(body, out_shape, in_specs, scratch=(), limit=None, flops=10**7):
    single = not isinstance(out_shape, (list, tuple))
    return pl.pallas_call(
        body,
        out_shape=out_shape,
        in_specs=in_specs,
        out_specs=WHOLE if single else [WHOLE] * len(out_shape),
        scratch_shapes=list(scratch),
        compiler_params=pltpu.CompilerParams(vmem_limit_bytes=limit),
        cost_estimate=pl.CostEstimate(flops=flops, bytes_accessed=10**6, transcendentals=0),
    )


def fold(x):
    total = x[:, :LANES]
    for c in range(LANES, x.shape[1], LANES):
        total = total + x[:, c : c + LANES]
    return total


def column(row):
    n = row.shape[1]
    at = lax.broadcasted_iota(jnp.int32, (n, n), 0)
    to = lax.broadcasted_iota(jnp.int32, (n, n), 1)
    return jnp.sum(jnp.where(at == to, jnp.broadcast_to(row, (n, n)), 0.0), axis=1, keepdims=True)


def place(k, width):
    return pl.ds(pl.multiple_of((lax.axis_index("tp") ^ k) * width, width), width)


def prep_body(n, cap, *refs):
    weight_hbm = refs[0]
    far = refs[1:16]
    dec_r, dec_i, bt_r, bt_i, base, mix, choose, table = refs[16:24]
    flat = refs[24:28]
    weight, tokens = refs[28:30]
    held = refs[30:44]
    sems, weight_sems, fac = refs[44:]
    held = (*held, tokens)
    copies = [pltpu.make_async_copy(a, b, sems.at[i]) for i, (a, b) in enumerate(zip(far, held))]
    for copy in copies:
        copy.start()
    weights = load(weight_hbm, weight, weight_sems, n, weight.shape[2])
    copies[13].wait()
    routes = held[13]
    slots, count = table.shape
    top = routes.shape[0]
    names = lax.broadcasted_iota(jnp.int32, (16, count), 0)
    marks = [(routes[r : r + 1, :] == names).astype(f32) for r in range(top)]
    total = marks[0]
    for r in range(1, top):
        total = total + marks[r]
    row = lax.broadcasted_iota(jnp.int32, (count, count), 0)
    col = lax.broadcasted_iota(jnp.int32, (count, count), 1)
    before = dot(total.astype(bf16), (row < col).astype(bf16), NN)
    same = (row == col).astype(bf16)
    places = lax.broadcasted_iota(jnp.int32, (slots, count), 0).astype(f32)
    used = jnp.zeros((slots, count), f32)
    for r in range(top):
        rank = jnp.sum(before * marks[r], axis=0, keepdims=True)
        slot = routes[r : r + 1, :].astype(f32) * cap + rank
        hit = (places == slot).astype(f32)
        choose[r] = dot(same, hit.astype(bf16), NT).astype(bf16)
        used = used + hit
    table[...] = used.astype(bf16)
    st_r, st_i, in_r, in_i, om_r, om_i = held[:6]
    groups, inner, entries = in_r.shape
    pack = LANES // inner
    in_r, in_i, om_r, om_i = (x for x in held[2:6])
    for i in range(2, 6):
        copies[i].wait()
    for i in (0, 1, 10, 11, 12):
        copies[i].wait()
    real, imag, log_step = held[10][...], held[11][...], held[12][...]
    step = column(jnp.exp(log_step))
    size = jnp.exp(real * step)
    angle = imag * step
    bar_r = size * jnp.cos(angle)
    bar_i = size * jnp.sin(angle)
    modulus = real * real + imag * imag
    fac_r = ((bar_r - 1.0) * real + bar_i * imag) / modulus
    fac_i = (bar_i * real - (bar_r - 1.0) * imag) / modulus
    for g in range(groups):
        cols = slice(g * entries, (g + 1) * entries)
        s_r, s_i = st_r[:, g, :], st_i[:, g, :]
        b_r, b_i = bar_r[g : g + 1, :], bar_i[g : g + 1, :]
        dec_r[:, cols] = b_r * s_r - b_i * s_i
        dec_i[:, cols] = b_r * s_i + b_i * s_r
        fac[0:1, cols] = fac_r[g : g + 1, :]
        fac[1:2, cols] = fac_i[g : g + 1, :]
    high = pack * entries
    for b in range(groups // pack):
        each = slice(b * pack, (b + 1) * pack)
        lanes = slice(b * LANES, (b + 1) * LANES)
        rows = slice(b * high, (b + 1) * high)
        b_r, b_i, c_r, c_i = (
            spread(x[each].reshape(LANES, entries), inner, pack) for x in (in_r, in_i, om_r, om_i)
        )
        f_r, f_i = fac[0:1, rows], fac[1:2, rows]
        i_r = (f_r * b_r - f_i * b_i).astype(bf16)
        i_i = (f_r * b_i + f_i * b_r).astype(bf16)
        c_r, c_i = c_r.astype(bf16), c_i.astype(bf16)
        bt_r[lanes, :] = i_r
        bt_i[lanes, :] = i_i
        mix[lanes, :] = (dot(i_r, c_r, NT) - dot(i_i, c_i, NT)).astype(bf16)
        base[:, lanes] = dot(dec_r[:, rows].astype(bf16), c_r, NT) - dot(
            dec_i[:, rows].astype(bf16), c_i, NT
        )
    for i in range(len(flat)):
        copies[6 + i].wait()
        rows = held[6 + i][...].astype(f32)
        for r in range(rows.shape[0]):
            flat[i][0:1, r * LANES : (r + 1) * LANES] = rows[r : r + 1, :]
    copies[14].wait()
    for copy in weights:
        copy.wait()


def spread(blocks, height, pack):
    rows, inner = blocks.shape
    columns = pack * inner
    at = lax.broadcasted_iota(jnp.int32, (inner, columns), 0)
    to = lax.broadcasted_iota(jnp.int32, (inner, columns), 1)
    wide = dot(blocks.astype(bf16), (to % inner == at).astype(bf16), NN)
    row = lax.broadcasted_iota(jnp.int32, (rows, columns), 0)
    col = lax.broadcasted_iota(jnp.int32, (rows, columns), 1)
    return jnp.where(row // height == col // inner, wide, 0.0)


def load(src, dst, sems, n, width):
    copies = []
    for k in range(n):
        part = src.at[:, place(k, width)] if len(src.shape) == 2 else src.at[:, :, place(k, width)]
        copies.append(pltpu.make_async_copy(part, dst.at[k], sems.at[k]))
    for copy in copies:
        copy.start()
    return copies


def mixer_body(n, *refs):
    pieces = refs[:n]
    gain, weight, base, mix, skip = refs[n : n + 5]
    driven_ref, act_ref = refs[n + 5 :]
    width = pieces[0].shape[1]
    square = 0.0
    for k in range(n):
        x = pieces[k][...].astype(f32)
        square = square + fold(x * x)
    scale = lax.rsqrt(jnp.sum(square, axis=1, keepdims=True) / (n * width) + norm_eps)
    total, turned = 0.0, 0.0
    for k in range(n):
        part = gain[:, place(k, width)]
        normed = (pieces[k][...].astype(f32) * part).astype(bf16)
        if k % 2:
            turned = turned + dot(weight[k], normed, NT)
        else:
            total = total + dot(normed, weight[k], NT)
    driven = ((total + turned.T) * scale).astype(bf16)
    driven_ref[...] = driven
    for b in range(driven.shape[1] // LANES):
        lanes = slice(b * LANES, (b + 1) * LANES)
        out = base[:, lanes] + dot(driven[:, lanes], mix[lanes, :], NN)
        out = out + skip[:, lanes] * driven[:, lanes].astype(f32)
        act_ref[:, lanes] = jax.nn.gelu(out).astype(bf16)


def state_body(driven, dec_r, dec_i, bt_r, bt_i, out_r, out_i):
    groups, entries = out_r.shape[1:]
    high = bt_r.shape[1]
    pack = high // entries
    for dec, bt, out in ((dec_r, bt_r, out_r), (dec_i, bt_i, out_i)):
        for b in range(groups // pack):
            lanes = slice(b * LANES, (b + 1) * LANES)
            new = dec[:, b * high : (b + 1) * high] + dot(driven[:, lanes], bt[lanes, :], NN)
            for g in range(pack):
                out[:, b * pack + g, :] = new[:, g * entries : (g + 1) * entries]


PARTS = 8


def fetch_body(spans, *refs):
    count = len(spans)
    copies = []
    for i, (low, high) in enumerate(spans):
        src, dst, sems = refs[i], refs[count + i], refs[2 * count + i]
        step = (high - low) // PARTS
        for p in range(PARTS):
            copies.append(
                pltpu.make_async_copy(
                    src.at[pl.ds(low + p * step, step)], dst.at[pl.ds(p * step, step)], sems.at[p]
                )
            )
            copies[-1].start()
    for copy in copies:
        copy.wait()


def fetch(*sources):
    sources = [x if isinstance(x, tuple) else (x, 0, x.shape[0]) for x in sources]
    return call(
        functools.partial(fetch_body, [x[1:] for x in sources]),
        [pltpu.VMEM((high - low, x.shape[1]), bf16) for x, low, high in sources],
        [FAR] * len(sources),
        [pltpu.SemaphoreType.DMA((PARTS,))] * len(sources),
        limit=2**20,
    )(*[stay(x) for x, _, _ in sources])


def rows_of(weight, i, experts):
    height = weight.shape[0] // experts
    return slice(i * height, (i + 1) * height)


def glu_body(n, *refs):
    pieces = refs[:n]
    glu, bias, out_w = refs[n : n + 3]
    glued_ref, partner = refs[n + 3 :]
    gate, turned = bias[...], 0.0
    for k in range(n):
        block = glu[:, place(k, pieces[k].shape[1])]
        if k % 2:
            turned = turned + dot(block, pieces[k][...], NT)
        else:
            gate = gate + dot(pieces[k][...], block, NT)
    glued = (pieces[0][...].astype(f32) * jax.nn.sigmoid(gate + turned.T)).astype(bf16)
    glued_ref[...] = glued
    for k in range(1, n, 2):
        partner[k // 2] = dot(glued, out_w[:, place(k, partner.shape[2])], NN).astype(bf16)


def out_body(n, glued, out_w, own):
    for k in range(0, n, 2):
        own[k // 2] = dot(glued[...], out_w[:, place(k, own.shape[2])], NN).astype(bf16)


def merge_body(*refs):
    out = refs[-1]
    cap = refs[0].shape[1]
    for j, x in enumerate(refs[:-1]):
        out[:, j * cap : (j + 1) * cap, :] = x[...]


def dispatch_body(m, terms, *refs):
    tokens = refs[0]
    sums = refs[1 : 1 + terms]
    table = refs[1 + terms]
    resid_ref = refs[2 + terms]
    outs = refs[3 + terms :]
    mixed = sums[0][...]
    for s in sums[1:]:
        mixed = mixed + s[...].astype(f32)
    resid = (tokens[...].astype(f32) + mixed).astype(bf16)
    resid_ref[...] = resid
    experts, cap, wide = outs[0].shape
    count = experts * cap
    for j in range(m):
        at = pl.multiple_of((lax.axis_index("ep") ^ j) * count, count)
        picked = dot(table[pl.ds(at, count), :], resid, NN).astype(bf16)
        outs[j][...] = picked.reshape(experts, cap, wide)


def up_body(n, *refs):
    near, far = refs[:n], refs[n : 2 * n]
    gain, gate_w, up_low, up_high, down_w = refs[2 * n : 2 * n + 5]
    later, partner = refs[2 * n + 5 :]
    experts, count, width = near[0].shape
    g, u, square = [0.0] * experts, [0.0] * experts, [0.0] * experts
    for k in range(n):
        part = gain[:, place(k, width)]
        for i in range(experts):
            x = jnp.concatenate([near[k][i], far[k][i]], axis=0).astype(f32)
            square[i] = square[i] + fold(x * x)
            x = (x * part).astype(bf16)
            g[i] = g[i] + dot(x, gate_w[rows_of(gate_w, i, experts), place(k, width)], NT)
            height = gate_w.shape[0] // experts
            held = up_low.shape[0] // height
            up_w, at = (up_low, i) if i < held else (up_high, i - held)
            u[i] = u[i] + dot(up_w[at * height : (at + 1) * height, place(k, width)], x, NT)
    for i in range(experts):
        scale = lax.rsqrt(jnp.sum(square[i], axis=1, keepdims=True) / (n * width) + norm_eps)
        hidden = (jax.nn.silu(g[i] * scale) * (u[i].T * scale)).astype(bf16)
        later[i] = hidden
        for k in range(1, n, 2):
            partner[k // 2, i] = dot(hidden[count:], down_w[rows_of(down_w, i, experts), place(k, width)], NN).astype(bf16)


def down_body(n, hidden, down_w, far_own, own, partner):
    count, width = own.shape[2:]
    experts = hidden.shape[0]
    for i in range(experts):
        near, far = hidden[i, :count], hidden[i, count:]
        for k in range(0, n, 2):
            far_own[k // 2, i] = dot(far, down_w[rows_of(down_w, i, experts), place(k, width)], NN).astype(bf16)
        for k in range(1, n, 2):
            partner[k // 2, i] = dot(near, down_w[rows_of(down_w, i, experts), place(k, width)], NN).astype(bf16)
        for k in range(0, n, 2):
            own[k // 2, i] = dot(near, down_w[rows_of(down_w, i, experts), place(k, width)], NN).astype(bf16)


def total_body(m, terms, *refs):
    sums = refs[:terms]
    outs = refs[terms:]
    total = sums[0][...]
    for s in sums[1:]:
        total = total + s[...].astype(f32)
    total = total.astype(bf16)
    cap = outs[0].shape[1]
    for j in range(m):
        outs[j][...] = total[:, j * cap : (j + 1) * cap, :]


def combine_body(m, *refs):
    resid, choose, weight = refs[:3]
    back = refs[3 : 3 + m]
    out, rows = refs[3 + m :]
    experts, cap, wide = back[0].shape
    count = experts * cap
    for j in range(m):
        at = pl.multiple_of((lax.axis_index("ep") ^ j) * count, count)
        rows[pl.ds(at, count), :] = back[j][...].reshape(count, wide)
    total = resid[...].astype(f32)
    for r in range(weight.shape[0]):
        picked = dot(choose[r], rows[...], NN)
        total = total + column(weight[r : r + 1, :]) * picked
    out[...] = total.astype(bf16)


def local_swaps(
    tokens,
    state_real,
    state_imag,
    mix_gain,
    in_weight,
    eig_real,
    eig_imag,
    log_step,
    input_real,
    input_imag,
    output_matrix_real,
    output_matrix_imag,
    skip_weight,
    glu_weight,
    glu_bias,
    out_weight,
    moe_gain,
    routes,
    route_weight,
    gate_weight,
    up_weight,
    down_weight,
):
    count, wide = tokens.shape
    n = lax.axis_size("tp")
    m = lax.axis_size("ep")
    groups, entries = eig_real.shape
    inner = input_real.shape[2]
    states = groups * entries
    channels = groups * inner
    full = wide * n
    exp_dev = gate_weight.shape[0]
    experts = exp_dev * m
    top = routes.shape[1]
    cap = max(2, (3 * top * count + 2 * experts - 1) // (2 * experts))
    slots = experts * cap

    pieces = gather_swaps(tokens, n)
    pack = LANES // inner
    far = [
        state_real,
        state_imag,
        input_real.transpose(0, 2, 1),
        input_imag.transpose(0, 2, 1),
        output_matrix_real,
        output_matrix_imag,
        skip_weight.reshape(-1, LANES),
        glu_bias.reshape(-1, LANES),
        mix_gain.reshape(-1, LANES),
        moe_gain.reshape(-1, LANES),
        eig_real,
        eig_imag,
        log_step.reshape(1, groups),
        routes.T,
        tokens,
    ]
    dec_r, dec_i, bt_r, bt_i, base, mix, choose, table, skip, bias, gain1, gain2, in_w, own = call(
        functools.partial(prep_body, n, cap),
        [jax.ShapeDtypeStruct((count, states), f32)] * 2
        + [jax.ShapeDtypeStruct((channels, pack * entries), bf16)] * 2
        + [
            jax.ShapeDtypeStruct((count, channels), f32),
            jax.ShapeDtypeStruct((channels, LANES), bf16),
            jax.ShapeDtypeStruct((top, count, slots), bf16),
            jax.ShapeDtypeStruct((slots, count), bf16),
        ]
        + [jax.ShapeDtypeStruct((1, channels), f32)] * 2
        + [jax.ShapeDtypeStruct((1, full), f32)] * 2
        + [pltpu.VMEM((n, channels, wide), bf16), pltpu.VMEM((count, wide), bf16)],
        [FAR] * 16,
        [pltpu.VMEM(x.shape, x.dtype) for x in far[:-1]]
        + [pltpu.SemaphoreType.DMA((15,)), pltpu.SemaphoreType.DMA((n,))]
        + [pltpu.VMEM((2, states), f32)],
        limit=12 * 2**20,
    )(*[stay(x) for x in [in_weight] + far])
    pieces[0] = own

    driven, activated = call(
        functools.partial(mixer_body, n),
        [jax.ShapeDtypeStruct((count, channels), bf16)] * 2,
        [WHOLE] * (n + 5),
        limit=12 * 2**20,
    )(*pieces, gain1, in_w, base, mix, skip)

    acts = gather_swaps(activated, n)
    glu_w, out_w = fetch(glu_weight, out_weight)
    block = jax.ShapeDtypeStruct((n // 2, count, wide), bf16)
    glued, partner = call(
        functools.partial(glu_body, n),
        [jax.ShapeDtypeStruct((count, channels), bf16), block],
        [WHOLE] * (n + 3),
        limit=12 * 2**20,
    )(*acts, glu_w, bias, out_w)
    sums = call(functools.partial(out_body, n), block, [WHOLE] * 2, limit=8 * 2**20)(glued, out_w)

    terms = reduce_swaps(sums, partner, n)
    hidden = gate_weight.shape[1]
    flat_up = up_weight.reshape(-1, full)
    held = (exp_dev + 1) // 2 * hidden
    gate_w, up_low = fetch(gate_weight.reshape(-1, full), (flat_up, 0, held))
    (up_high,) = fetch((flat_up, held, exp_dev * hidden))
    (down_w,) = fetch(down_weight.reshape(-1, full))
    resid, *packed = call(
        functools.partial(dispatch_body, m, len(terms)),
        [jax.ShapeDtypeStruct((count, wide), bf16)]
        + [jax.ShapeDtypeStruct((exp_dev, cap, wide), bf16)] * m,
        [WHOLE] * (2 + len(terms)),
        limit=8 * 2**20,
    )(own, *terms, table)

    arrived = [packed[0]] + [swap(packed[j], "ep", j) for j in range(1, m)]
    half = m // 2
    fragments = []
    for group in (arrived[:half], arrived[half:]):
        merged = call(
            merge_body,
            jax.ShapeDtypeStruct((exp_dev, half * cap, wide), bf16),
            [WHOLE] * half,
            limit=2**20,
        )(*group)
        fragments += gather_swaps(merged, n)
    part = jax.ShapeDtypeStruct((n // 2, exp_dev, half * cap, wide), bf16)
    later, far_partner = call(
        functools.partial(up_body, n),
        [jax.ShapeDtypeStruct((exp_dev, 2 * half * cap, hidden), bf16), part],
        [WHOLE] * (2 * n + 5),
        limit=16 * 2**20,
    )(*fragments, gain2, gate_w, up_low, up_high, down_w)
    far_own, *near_outs = call(
        functools.partial(down_body, n), [part] * 3, [WHOLE] * 2, limit=8 * 2**20
    )(later, down_w)
    far_outs = [far_own, far_partner]
    back = [None] * m
    for outs, first in ((far_outs, half), (near_outs, 0)):
        terms = reduce_swaps(*outs, n)
        totals = call(
            functools.partial(total_body, half, len(terms)),
            [jax.ShapeDtypeStruct((exp_dev, cap, wide), bf16)] * half,
            [WHOLE] * len(terms),
            limit=4 * 2**20,
        )(*terms)
        for j in range(first, first + half):
            back[j] = swap(totals[j - first], "ep", j) if j else totals[0]
    new_r, new_i = call(
        state_body,
        [jax.ShapeDtypeStruct((count, groups, entries), f32)] * 2,
        [WHOLE] * 5,
        limit=4 * 2**20,
    )(driven, dec_r, dec_i, bt_r, bt_i)
    result = call(
        functools.partial(combine_body, m),
        jax.ShapeDtypeStruct((count, wide), bf16),
        [WHOLE] * (3 + m),
        [pltpu.VMEM((slots, wide), bf16)],
        limit=8 * 2**20,
    )(resid, choose, route_weight.T, *back)
    return (
        result,
        new_r,
        new_i,
    )


def ssm_step(
    driven,
    state_real,
    state_imag,
    eig_real,
    eig_imag,
    log_step,
    input_real,
    input_imag,
    output_matrix_real,
    output_matrix_imag,
    skip_weight,
):
    highest_precision = lax.Precision.HIGHEST
    count_of_rows = driven.shape[0]
    groups = eig_real.shape[0]
    group_width = input_real.shape[2]
    time_step = jnp.exp(log_step)[:, None]
    magnitude = jnp.exp(eig_real * time_step)
    angle_now = eig_imag * time_step
    bar_real = magnitude * jnp.cos(angle_now)
    bar_imag = magnitude * jnp.sin(angle_now)
    modulus = eig_real * eig_real + eig_imag * eig_imag
    fac_real = ((bar_real - 1.0) * eig_real + bar_imag * eig_imag) / modulus
    fac_imag = (bar_imag * eig_real - (bar_real - 1.0) * eig_imag) / modulus
    ib_real = fac_real[..., None] * input_real - fac_imag[..., None] * input_imag
    ib_imag = fac_real[..., None] * input_imag + fac_imag[..., None] * input_real
    grouped = driven.astype(jnp.float32).reshape(count_of_rows, groups, group_width)
    push_real = jnp.einsum("gpc,ngc->ngp", ib_real, grouped, precision=highest_precision)
    push_imag = jnp.einsum("gpc,ngc->ngp", ib_imag, grouped, precision=highest_precision)
    updated_state_real = bar_real[None] * state_real - bar_imag[None] * state_imag + push_real
    updated_state_imag = bar_real[None] * state_imag + bar_imag[None] * state_real + push_imag
    state_readout = jnp.einsum(
        "jiy,sjy->sji", output_matrix_real, updated_state_real, precision=highest_precision
    ) - jnp.einsum(
        "jiy,sjy->sji", output_matrix_imag, updated_state_imag, precision=highest_precision
    )
    state_readout = state_readout.reshape(count_of_rows, groups * group_width) + skip_weight[
        None, :
    ] * driven.astype(jnp.float32)
    activated = jax.nn.gelu(state_readout).astype(jnp.bfloat16)
    return (updated_state_real, updated_state_imag, activated)


def local(
    tokens,
    state_real,
    state_imag,
    mix_gain,
    in_weight,
    eig_real,
    eig_imag,
    log_step,
    input_real,
    input_imag,
    output_matrix_real,
    output_matrix_imag,
    skip_weight,
    glu_weight,
    glu_bias,
    out_weight,
    moe_gain,
    routes,
    route_weight,
    gate_weight,
    up_weight,
    down_weight,
):
    count_of_rows = tokens.shape[0]
    n_ep = lax.axis_size("ep")
    width_tp = lax.axis_size("tp")
    whole_rows = lax.all_gather(tokens, "tp", axis=1, tiled=True)
    whole_float = whole_rows.astype(jnp.float32)
    first_scale = lax.rsqrt(jnp.mean(whole_float * whole_float, axis=1, keepdims=True) + norm_eps)
    normed = (whole_float * first_scale * mix_gain.astype(jnp.float32)).astype(jnp.bfloat16)
    driven = jnp.einsum("rd,cd->rc", normed, in_weight, preferred_element_type=jnp.float32).astype(
        jnp.bfloat16
    )
    updated_state_real, updated_state_imag, activated = ssm_step(
        driven,
        state_real,
        state_imag,
        eig_real,
        eig_imag,
        log_step,
        input_real,
        input_imag,
        output_matrix_real,
        output_matrix_imag,
        skip_weight,
    )
    gate_pre = (
        jnp.einsum(
            "rc,oc->ro",
            lax.all_gather(activated, "tp", axis=1, tiled=True),
            glu_weight,
            preferred_element_type=jnp.float32,
        )
        + glu_bias
    )
    glued = (activated.astype(jnp.float32) * jax.nn.sigmoid(gate_pre)).astype(jnp.bfloat16)
    partial_value = jnp.dot(glued, out_weight, preferred_element_type=jnp.float32)
    mixed = lax.psum_scatter(
        partial_value.astype(jnp.bfloat16), "tp", scatter_dimension=1, tiled=True
    ).astype(jnp.float32)
    residual = (tokens.astype(jnp.float32) + mixed).astype(jnp.bfloat16)
    resid_float = residual.astype(jnp.float32)
    exp_dev = gate_weight.shape[0]
    experts = exp_dev * n_ep
    top_count = routes.shape[1]
    capacity = max(2, (3 * top_count * count_of_rows + 2 * experts - 1) // (2 * experts))
    chosen = routes.reshape(-1)
    onehot = (chosen[:, None] == jnp.arange(experts, dtype=jnp.int32)[None, :]).astype(jnp.int32)
    rank_index = jnp.sum((jnp.cumsum(onehot, axis=0) - onehot) * onehot, axis=1)
    slot_index = (chosen * capacity + rank_index).reshape(count_of_rows, top_count)
    slots_all = experts * capacity
    choose = slot_index[:, :, None] == jnp.arange(slots_all, dtype=jnp.int32)[None, None, :]
    dispatch = jnp.sum(choose.astype(jnp.float32), axis=1).astype(jnp.bfloat16)
    local_sq = jnp.sum(resid_float * resid_float, axis=1)
    total_sq = lax.psum(local_sq, "tp")
    dim_full = residual.shape[1] * width_tp
    second_scale = lax.rsqrt(total_sq[:, None] / dim_full + norm_eps)
    gain_part = lax.dynamic_slice_in_dim(
        moe_gain, lax.axis_index("tp") * residual.shape[1], residual.shape[1], 0
    )
    expert_in = (resid_float * second_scale * gain_part.astype(jnp.float32)).astype(jnp.bfloat16)
    packed = jnp.einsum(
        "rs,rd->sd", dispatch, expert_in, preferred_element_type=jnp.float32
    ).astype(jnp.bfloat16)
    packed = packed.reshape(n_ep, exp_dev * capacity, residual.shape[1])
    arrived = lax.all_to_all(packed, "ep", split_axis=0, concat_axis=0, tiled=True)
    arrived = arrived.reshape(n_ep, exp_dev, capacity, residual.shape[1])
    fragment = lax.all_gather(arrived, "tp", axis=3, tiled=True)
    gate_part = jnp.einsum(
        "necd,efd->necf", fragment, gate_weight, preferred_element_type=jnp.float32
    )
    up_part = jnp.einsum("necd,efd->necf", fragment, up_weight, preferred_element_type=jnp.float32)
    hidden_width = (jax.nn.silu(gate_part) * up_part).astype(jnp.bfloat16)
    partial_out = jnp.einsum(
        "necf,efd->necd", hidden_width, down_weight, preferred_element_type=jnp.float32
    )
    summed = lax.psum_scatter(
        partial_out.astype(jnp.bfloat16), "tp", scatter_dimension=3, tiled=True
    )
    summed = summed.reshape(n_ep, exp_dev * capacity, summed.shape[3])
    returned = lax.all_to_all(summed, "ep", split_axis=0, concat_axis=0, tiled=True)
    returned = returned.reshape(slots_all, returned.shape[2])
    gathered_k = jnp.einsum(
        "rks,sd->rkd", choose.astype(jnp.bfloat16), returned, preferred_element_type=jnp.float32
    )
    result = (resid_float + jnp.sum(route_weight[..., None] * gathered_k, axis=1)).astype(
        jnp.bfloat16
    )
    return (result, updated_state_real, updated_state_imag)


def solution(mesh):
    n, m = mesh.shape["tp"], mesh.shape["ep"]
    small = n in (4, 8) and m in (2, 4)

    def whole(*args):
        if not small:
            return local(*args)
        return local_swaps(*args)

    return jax.shard_map(
        whole,
        mesh=mesh,
        in_specs=(
            P("ep", "tp"),
            P("ep", "tp", None),
            P("ep", "tp", None),
            P(),
            P("tp", None),
            P("tp", None),
            P("tp", None),
            P("tp"),
            P("tp", None, None),
            P("tp", None, None),
            P("tp", None, None),
            P("tp", None, None),
            P("tp"),
            P("tp", None),
            P("tp"),
            P("tp", None),
            P(),
            P("ep", None),
            P("ep", None),
            P("ep", "tp", None),
            P("ep", "tp", None),
            P("ep", "tp", None),
        ),
        out_specs=(P("ep", "tp"), P("ep", "tp", None), P("ep", "tp", None)),
        check_vma=False,
    )
```

```python
import functools
import jax
import jax.numpy as jnp
from jax import lax
from jax.experimental import pallas as pl
from jax.experimental.pallas import tpu as pltpu
from jax.sharding import PartitionSpec as P


norm_eps = 1e-06
f32 = jnp.float32
bf16 = jnp.bfloat16
NT = (((1,), (1,)), ((), ()))
NN = (((1,), (0,)), ((), ()))
WHOLE = pl.BlockSpec(memory_space=pltpu.VMEM)
FAR = pl.BlockSpec(memory_space=pltpu.HBM)
LANES = 128


def stay(x):
    return pltpu.with_memory_space_constraint(x, pltpu.HBM)


def dot(a, b, dims):
    return lax.dot_general(a, b, dims, preferred_element_type=f32)


def swap(x, axis, k):
    return lax.ppermute(x, axis, [(i, i ^ k) for i in range(lax.axis_size(axis))])


def gather_swaps(x, n):
    pieces = [None] * n
    pieces[0] = x
    for k in range(2, n, 2):
        pieces[k] = swap(x, "tp", k)
    for k in range(0, n, 2):
        pieces[k ^ 1] = swap(pieces[k], "tp", 1)
    return pieces


def pair_swaps(own, partner, n):
    other = swap(partner, "tp", 1)
    shape = own.shape[1:]
    return call(
        pair_body,
        [jax.ShapeDtypeStruct(shape, f32)] + [jax.ShapeDtypeStruct(shape, bf16)] * (n // 2 - 1),
        [WHOLE] * 2,
        limit=8 * 2**20,
    )(own, other)


def reduce_swaps(own, partner, n):
    first, *rest = pair_swaps(own, partner, n)
    return [first] + [swap(x, "tp", k) for x, k in zip(rest, range(2, n, 2))]


def pair_body(own, other, *outs):
    for i, out in enumerate(outs):
        out[...] = (own[i].astype(f32) + other[i].astype(f32)).astype(out.dtype)


def call(body, out_shape, in_specs, scratch=(), limit=None, flops=10**7):
    single = not isinstance(out_shape, (list, tuple))
    return pl.pallas_call(
        body,
        out_shape=out_shape,
        in_specs=in_specs,
        out_specs=WHOLE if single else [WHOLE] * len(out_shape),
        scratch_shapes=list(scratch),
        compiler_params=pltpu.CompilerParams(vmem_limit_bytes=limit),
        cost_estimate=pl.CostEstimate(flops=flops, bytes_accessed=10**6, transcendentals=0),
    )


def fold(x):
    total = x[:, :LANES]
    for c in range(LANES, x.shape[1], LANES):
        total = total + x[:, c : c + LANES]
    return total


def column(row):
    n = row.shape[1]
    at = lax.broadcasted_iota(jnp.int32, (n, n), 0)
    to = lax.broadcasted_iota(jnp.int32, (n, n), 1)
    return jnp.sum(jnp.where(at == to, jnp.broadcast_to(row, (n, n)), 0.0), axis=1, keepdims=True)


def place(k, width):
    return pl.ds(pl.multiple_of((lax.axis_index("tp") ^ k) * width, width), width)


def prep_body(n, cap, *refs):
    weight_hbm = refs[0]
    far = refs[1:16]
    dec_r, dec_i, bt_r, bt_i, base, mix, choose, table = refs[16:24]
    flat = refs[24:28]
    weight, tokens = refs[28:30]
    held = refs[30:44]
    sems, weight_sems, fac = refs[44:]
    held = (*held, tokens)
    copies = [pltpu.make_async_copy(a, b, sems.at[i]) for i, (a, b) in enumerate(zip(far, held))]
    for copy in copies:
        copy.start()
    weights = load(weight_hbm, weight, weight_sems, n, weight.shape[2])
    copies[13].wait()
    routes = held[13]
    slots, count = table.shape
    top = routes.shape[0]
    names = lax.broadcasted_iota(jnp.int32, (16, count), 0)
    marks = [(routes[r : r + 1, :] == names).astype(f32) for r in range(top)]
    total = marks[0]
    for r in range(1, top):
        total = total + marks[r]
    row = lax.broadcasted_iota(jnp.int32, (count, count), 0)
    col = lax.broadcasted_iota(jnp.int32, (count, count), 1)
    before = dot(total.astype(bf16), (row < col).astype(bf16), NN)
    same = (row == col).astype(bf16)
    places = lax.broadcasted_iota(jnp.int32, (slots, count), 0).astype(f32)
    used = jnp.zeros((slots, count), f32)
    for r in range(top):
        rank = jnp.sum(before * marks[r], axis=0, keepdims=True)
        slot = routes[r : r + 1, :].astype(f32) * cap + rank
        hit = (places == slot).astype(f32)
        choose[r] = dot(same, hit.astype(bf16), NT).astype(bf16)
        used = used + hit
    table[...] = used.astype(bf16)
    st_r, st_i, in_r, in_i, om_r, om_i = held[:6]
    groups, inner, entries = in_r.shape
    pack = LANES // inner
    in_r, in_i, om_r, om_i = (x for x in held[2:6])
    for i in range(2, 6):
        copies[i].wait()
    for i in (0, 1, 10, 11, 12):
        copies[i].wait()
    real, imag, log_step = held[10][...], held[11][...], held[12][...]
    step = column(jnp.exp(log_step))
    size = jnp.exp(real * step)
    angle = imag * step
    bar_r = size * jnp.cos(angle)
    bar_i = size * jnp.sin(angle)
    modulus = real * real + imag * imag
    fac_r = ((bar_r - 1.0) * real + bar_i * imag) / modulus
    fac_i = (bar_i * real - (bar_r - 1.0) * imag) / modulus
    for g in range(groups):
        cols = slice(g * entries, (g + 1) * entries)
        s_r, s_i = st_r[:, g, :], st_i[:, g, :]
        b_r, b_i = bar_r[g : g + 1, :], bar_i[g : g + 1, :]
        dec_r[:, cols] = b_r * s_r - b_i * s_i
        dec_i[:, cols] = b_r * s_i + b_i * s_r
        fac[0:1, cols] = fac_r[g : g + 1, :]
        fac[1:2, cols] = fac_i[g : g + 1, :]
    high = pack * entries
    for b in range(groups // pack):
        each = slice(b * pack, (b + 1) * pack)
        lanes = slice(b * LANES, (b + 1) * LANES)
        rows = slice(b * high, (b + 1) * high)
        b_r, b_i, c_r, c_i = (
            spread(x[each].reshape(LANES, entries), inner, pack) for x in (in_r, in_i, om_r, om_i)
        )
        f_r, f_i = fac[0:1, rows], fac[1:2, rows]
        i_r = (f_r * b_r - f_i * b_i).astype(bf16)
        i_i = (f_r * b_i + f_i * b_r).astype(bf16)
        c_r, c_i = c_r.astype(bf16), c_i.astype(bf16)
        bt_r[lanes, :] = i_r
        bt_i[lanes, :] = i_i
        mix[lanes, :] = (dot(i_r, c_r, NT) - dot(i_i, c_i, NT)).astype(bf16)
        base[:, lanes] = dot(dec_r[:, rows].astype(bf16), c_r, NT) - dot(
            dec_i[:, rows].astype(bf16), c_i, NT
        )
    for i in range(len(flat)):
        copies[6 + i].wait()
        rows = held[6 + i][...].astype(f32)
        for r in range(rows.shape[0]):
            flat[i][0:1, r * LANES : (r + 1) * LANES] = rows[r : r + 1, :]
    copies[14].wait()
    for copy in weights:
        copy.wait()


def spread(blocks, height, pack):
    rows, inner = blocks.shape
    columns = pack * inner
    at = lax.broadcasted_iota(jnp.int32, (inner, columns), 0)
    to = lax.broadcasted_iota(jnp.int32, (inner, columns), 1)
    wide = dot(blocks.astype(bf16), (to % inner == at).astype(bf16), NN)
    row = lax.broadcasted_iota(jnp.int32, (rows, columns), 0)
    col = lax.broadcasted_iota(jnp.int32, (rows, columns), 1)
    return jnp.where(row // height == col // inner, wide, 0.0)


def load(src, dst, sems, n, width):
    copies = []
    for k in range(n):
        part = src.at[:, place(k, width)] if len(src.shape) == 2 else src.at[:, :, place(k, width)]
        copies.append(pltpu.make_async_copy(part, dst.at[k], sems.at[k]))
    for copy in copies:
        copy.start()
    return copies


def mixer_sums(odd, pieces, gain, weight, start):
    total, turned, square = start
    width = pieces[0].shape[1]
    for at, piece in enumerate(pieces):
        k = 2 * at + odd
        x = piece[...].astype(f32)
        square = square + fold(x * x)
        x = (x * gain[:, place(k, width)]).astype(bf16)
        if at % 2:
            turned = turned + dot(weight[k], x, NT)
        else:
            total = total + dot(x, weight[k], NT)
    return total, turned, square


def first_body(n, *refs):
    pieces = refs[: n // 2]
    gain, weight = refs[n // 2 : n // 2 + 2]
    for out, value in zip(refs[n // 2 + 2 :], mixer_sums(0, pieces, gain, weight, (0.0, 0.0, 0.0))):
        out[...] = value


def mixer_body(n, *refs):
    pieces = refs[: n // 2]
    gain, weight, base, mix, skip, total, turned, square = refs[n // 2 : n // 2 + 8]
    driven_ref, act_ref = refs[n // 2 + 8 :]
    start = (total[...], turned[...], square[...])
    total, turned, square = mixer_sums(1, pieces, gain, weight, start)
    width = pieces[0].shape[1]
    scale = lax.rsqrt(jnp.sum(square, axis=1, keepdims=True) / (n * width) + norm_eps)
    driven = ((total + turned.T) * scale).astype(bf16)
    driven_ref[...] = driven
    for b in range(driven.shape[1] // LANES):
        lanes = slice(b * LANES, (b + 1) * LANES)
        out = base[:, lanes] + dot(driven[:, lanes], mix[lanes, :], NN)
        out = out + skip[:, lanes] * driven[:, lanes].astype(f32)
        act_ref[:, lanes] = jax.nn.gelu(out).astype(bf16)


def state_body(driven, dec_r, dec_i, bt_r, bt_i, out_r, out_i):
    groups, entries = out_r.shape[1:]
    high = bt_r.shape[1]
    pack = high // entries
    for dec, bt, out in ((dec_r, bt_r, out_r), (dec_i, bt_i, out_i)):
        for b in range(groups // pack):
            lanes = slice(b * LANES, (b + 1) * LANES)
            new = dec[:, b * high : (b + 1) * high] + dot(driven[:, lanes], bt[lanes, :], NN)
            for g in range(pack):
                out[:, b * pack + g, :] = new[:, g * entries : (g + 1) * entries]


PARTS = 8


def fetch_body(spans, *refs):
    count = len(spans)
    copies = []
    for i, (low, high) in enumerate(spans):
        src, dst, sems = refs[i], refs[count + i], refs[2 * count + i]
        step = (high - low) // PARTS
        for p in range(PARTS):
            copies.append(
                pltpu.make_async_copy(
                    src.at[pl.ds(low + p * step, step)], dst.at[pl.ds(p * step, step)], sems.at[p]
                )
            )
            copies[-1].start()
    for copy in copies:
        copy.wait()


def fetch(*sources):
    sources = [x if isinstance(x, tuple) else (x, 0, x.shape[0]) for x in sources]
    return call(
        functools.partial(fetch_body, [x[1:] for x in sources]),
        [pltpu.VMEM((high - low, x.shape[1]), bf16) for x, low, high in sources],
        [FAR] * len(sources),
        [pltpu.SemaphoreType.DMA((PARTS,))] * len(sources),
        limit=2**20,
    )(*[stay(x) for x, _, _ in sources])


def rows_of(weight, i, experts):
    height = weight.shape[0] // experts
    return slice(i * height, (i + 1) * height)


def glu_sums(odd, pieces, glu, gate, turned):
    width = pieces[0].shape[1]
    for at, piece in enumerate(pieces):
        block = glu[:, place(2 * at + odd, width)]
        if at % 2:
            turned = turned + dot(block, piece[...], NT)
        else:
            gate = gate + dot(piece[...], block, NT)
    return gate, turned


def gate_body(n, *refs):
    pieces = refs[: n // 2]
    glu, bias, gate_ref, turned_ref = refs[n // 2 :]
    gate_ref[...], turned_ref[...] = glu_sums(0, pieces, glu, bias[...], 0.0)


def glu_body(n, *refs):
    pieces = refs[: n // 2]
    own, glu, gate, turned, out_w = refs[n // 2 : n // 2 + 5]
    glued_ref, partner = refs[n // 2 + 5 :]
    gate, turned = glu_sums(1, pieces, glu, gate[...], turned[...])
    glued = (own[...].astype(f32) * jax.nn.sigmoid(gate + turned.T)).astype(bf16)
    glued_ref[...] = glued
    for k in range(1, n, 2):
        partner[k // 2] = dot(glued, out_w[:, place(k, partner.shape[2])], NN).astype(bf16)


def out_body(n, glued, out_w, own):
    for k in range(0, n, 2):
        own[k // 2] = dot(glued[...], out_w[:, place(k, own.shape[2])], NN).astype(bf16)


def merge_body(*refs):
    out = refs[-1]
    cap = refs[0].shape[1]
    for j, x in enumerate(refs[:-1]):
        out[:, j * cap : (j + 1) * cap, :] = x[...]


def dispatch_body(m, terms, *refs):
    tokens = refs[0]
    sums = refs[1 : 1 + terms]
    table = refs[1 + terms]
    resid_ref = refs[2 + terms]
    outs = refs[3 + terms :]
    mixed = sums[0][...]
    for s in sums[1:]:
        mixed = mixed + s[...].astype(f32)
    resid = (tokens[...].astype(f32) + mixed).astype(bf16)
    resid_ref[...] = resid
    experts, cap, wide = outs[0].shape
    count = experts * cap
    for j in range(m):
        at = pl.multiple_of((lax.axis_index("ep") ^ j) * count, count)
        picked = dot(table[pl.ds(at, count), :], resid, NN).astype(bf16)
        outs[j][...] = picked.reshape(experts, cap, wide)


def expert_sums(odd, near, far, gain, gate_w, up_low, up_high, i, start):
    g, u, square = start
    experts, _, width = near[0].shape
    height = gate_w.shape[0] // experts
    held = up_low.shape[0] // height
    up_w, row = (up_low, i) if i < held else (up_high, i - held)
    for at in range(len(near)):
        k = 2 * at + odd
        x = jnp.concatenate([near[at][i], far[at][i]], axis=0).astype(f32)
        square = square + fold(x * x)
        x = (x * gain[:, place(k, width)]).astype(bf16)
        g = g + dot(x, gate_w[rows_of(gate_w, i, experts), place(k, width)], NT)
        u = u + dot(up_w[row * height : (row + 1) * height, place(k, width)], x, NT)
    return g, u, square


def even_body(n, *refs):
    near, far = refs[: n // 2], refs[n // 2 : n]
    gain, gate_w, up_low, up_high, g_ref, u_ref, square_ref = refs[n:]
    for i in range(near[0].shape[0]):
        g_ref[i], u_ref[i], square_ref[i] = expert_sums(
            0, near, far, gain, gate_w, up_low, up_high, i, (0.0, 0.0, 0.0)
        )


def up_body(n, *refs):
    near, far = refs[: n // 2], refs[n // 2 : n]
    gain, gate_w, up_low, up_high, down_w, g_ref, u_ref, square_ref = refs[n : n + 8]
    later, partner = refs[n + 8 :]
    experts, count, width = near[0].shape
    for i in range(experts):
        start = (g_ref[i], u_ref[i], square_ref[i])
        g, u, square = expert_sums(1, near, far, gain, gate_w, up_low, up_high, i, start)
        scale = lax.rsqrt(jnp.sum(square, axis=1, keepdims=True) / (n * width) + norm_eps)
        hidden = (jax.nn.silu(g * scale) * (u.T * scale)).astype(bf16)
        later[i] = hidden
        for k in range(1, n, 2):
            partner[k // 2, i] = dot(hidden[count:], down_w[rows_of(down_w, i, experts), place(k, width)], NN).astype(bf16)


def down_body(n, hidden, down_w, far_own, own, partner):
    count, width = own.shape[2:]
    experts = hidden.shape[0]
    for i in range(experts):
        near, far = hidden[i, :count], hidden[i, count:]
        for k in range(0, n, 2):
            far_own[k // 2, i] = dot(far, down_w[rows_of(down_w, i, experts), place(k, width)], NN).astype(bf16)
        for k in range(1, n, 2):
            partner[k // 2, i] = dot(near, down_w[rows_of(down_w, i, experts), place(k, width)], NN).astype(bf16)
        for k in range(0, n, 2):
            own[k // 2, i] = dot(near, down_w[rows_of(down_w, i, experts), place(k, width)], NN).astype(bf16)


def total_body(m, terms, *refs):
    sums = refs[:terms]
    outs = refs[terms:]
    total = sums[0][...]
    for s in sums[1:]:
        total = total + s[...].astype(f32)
    total = total.astype(bf16)
    cap = outs[0].shape[1]
    for j in range(m):
        outs[j][...] = total[:, j * cap : (j + 1) * cap, :]


def combine_body(m, *refs):
    resid, choose, weight = refs[:3]
    back = refs[3 : 3 + m]
    out, rows = refs[3 + m :]
    experts, cap, wide = back[0].shape
    count = experts * cap
    for j in range(m):
        at = pl.multiple_of((lax.axis_index("ep") ^ j) * count, count)
        rows[pl.ds(at, count), :] = back[j][...].reshape(count, wide)
    total = resid[...].astype(f32)
    for r in range(weight.shape[0]):
        picked = dot(choose[r], rows[...], NN)
        total = total + column(weight[r : r + 1, :]) * picked
    out[...] = total.astype(bf16)


def local_swaps(
    tokens,
    state_real,
    state_imag,
    mix_gain,
    in_weight,
    eig_real,
    eig_imag,
    log_step,
    input_real,
    input_imag,
    output_matrix_real,
    output_matrix_imag,
    skip_weight,
    glu_weight,
    glu_bias,
    out_weight,
    moe_gain,
    routes,
    route_weight,
    gate_weight,
    up_weight,
    down_weight,
):
    count, wide = tokens.shape
    n = lax.axis_size("tp")
    m = lax.axis_size("ep")
    groups, entries = eig_real.shape
    inner = input_real.shape[2]
    states = groups * entries
    channels = groups * inner
    full = wide * n
    exp_dev = gate_weight.shape[0]
    experts = exp_dev * m
    top = routes.shape[1]
    cap = max(2, (3 * top * count + 2 * experts - 1) // (2 * experts))
    slots = experts * cap

    pieces = gather_swaps(tokens, n)
    pack = LANES // inner
    far = [
        state_real,
        state_imag,
        input_real.transpose(0, 2, 1),
        input_imag.transpose(0, 2, 1),
        output_matrix_real,
        output_matrix_imag,
        skip_weight.reshape(-1, LANES),
        glu_bias.reshape(-1, LANES),
        mix_gain.reshape(-1, LANES),
        moe_gain.reshape(-1, LANES),
        eig_real,
        eig_imag,
        log_step.reshape(1, groups),
        routes.T,
        tokens,
    ]
    dec_r, dec_i, bt_r, bt_i, base, mix, choose, table, skip, bias, gain1, gain2, in_w, own = call(
        functools.partial(prep_body, n, cap),
        [jax.ShapeDtypeStruct((count, states), f32)] * 2
        + [jax.ShapeDtypeStruct((channels, pack * entries), bf16)] * 2
        + [
            jax.ShapeDtypeStruct((count, channels), f32),
            jax.ShapeDtypeStruct((channels, LANES), bf16),
            jax.ShapeDtypeStruct((top, count, slots), bf16),
            jax.ShapeDtypeStruct((slots, count), bf16),
        ]
        + [jax.ShapeDtypeStruct((1, channels), f32)] * 2
        + [jax.ShapeDtypeStruct((1, full), f32)] * 2
        + [pltpu.VMEM((n, channels, wide), bf16), pltpu.VMEM((count, wide), bf16)],
        [FAR] * 16,
        [pltpu.VMEM(x.shape, x.dtype) for x in far[:-1]]
        + [pltpu.SemaphoreType.DMA((15,)), pltpu.SemaphoreType.DMA((n,))]
        + [pltpu.VMEM((2, states), f32)],
        limit=12 * 2**20,
    )(*[stay(x) for x in [in_weight] + far])
    pieces[0] = own

    partial = call(
        functools.partial(first_body, n),
        [jax.ShapeDtypeStruct(x, f32) for x in ((count, channels), (channels, count), (count, LANES))],
        [WHOLE] * (n // 2 + 2),
        limit=8 * 2**20,
    )(*pieces[::2], gain1, in_w)
    driven, activated = call(
        functools.partial(mixer_body, n),
        [jax.ShapeDtypeStruct((count, channels), bf16)] * 2,
        [WHOLE] * (n // 2 + 8),
        limit=12 * 2**20,
    )(*pieces[1::2], gain1, in_w, base, mix, skip, *partial)

    acts = gather_swaps(activated, n)
    glu_w, out_w = fetch(glu_weight, out_weight)
    block = jax.ShapeDtypeStruct((n // 2, count, wide), bf16)
    partial = call(
        functools.partial(gate_body, n),
        [jax.ShapeDtypeStruct(x, f32) for x in ((count, channels), (channels, count))],
        [WHOLE] * (n // 2 + 2),
        limit=8 * 2**20,
    )(*acts[::2], glu_w, bias)
    glued, partner = call(
        functools.partial(glu_body, n),
        [jax.ShapeDtypeStruct((count, channels), bf16), block],
        [WHOLE] * (n // 2 + 5),
        limit=12 * 2**20,
    )(*acts[1::2], acts[0], glu_w, *partial, out_w)
    sums = call(functools.partial(out_body, n), block, [WHOLE] * 2, limit=8 * 2**20)(glued, out_w)

    terms = reduce_swaps(sums, partner, n)
    hidden = gate_weight.shape[1]
    flat_up = up_weight.reshape(-1, full)
    held = (exp_dev + 1) // 2 * hidden
    gate_w, up_low = fetch(gate_weight.reshape(-1, full), (flat_up, 0, held))
    (up_high,) = fetch((flat_up, held, exp_dev * hidden))
    (down_w,) = fetch(down_weight.reshape(-1, full))
    resid, *packed = call(
        functools.partial(dispatch_body, m, len(terms)),
        [jax.ShapeDtypeStruct((count, wide), bf16)]
        + [jax.ShapeDtypeStruct((exp_dev, cap, wide), bf16)] * m,
        [WHOLE] * (2 + len(terms)),
        limit=8 * 2**20,
    )(own, *terms, table)

    arrived = [packed[0]] + [swap(packed[j], "ep", j) for j in range(1, m)]
    half = m // 2
    fragments = []
    for group in (arrived[:half], arrived[half:]):
        merged = call(
            merge_body,
            jax.ShapeDtypeStruct((exp_dev, half * cap, wide), bf16),
            [WHOLE] * half,
            limit=2**20,
        )(*group)
        fragments += gather_swaps(merged, n)
    part = jax.ShapeDtypeStruct((n // 2, exp_dev, half * cap, wide), bf16)
    near, far = fragments[:n], fragments[n:]
    rows = 2 * half * cap
    weights = (gain2, gate_w, up_low, up_high)
    partial = call(
        functools.partial(even_body, n),
        [jax.ShapeDtypeStruct((exp_dev, *x), f32) for x in ((rows, hidden), (hidden, rows), (rows, LANES))],
        [WHOLE] * (n + 4),
        limit=8 * 2**20,
    )(*near[::2], *far[::2], *weights)
    later, far_partner = call(
        functools.partial(up_body, n),
        [jax.ShapeDtypeStruct((exp_dev, rows, hidden), bf16), part],
        [WHOLE] * (n + 8),
        limit=16 * 2**20,
    )(*near[1::2], *far[1::2], *weights, down_w, *partial)
    far_own, *near_outs = call(
        functools.partial(down_body, n), [part] * 3, [WHOLE] * 2, limit=8 * 2**20
    )(later, down_w)
    far_outs = [far_own, far_partner]
    back = [None] * m
    for outs, first in ((far_outs, half), (near_outs, 0)):
        terms = reduce_swaps(*outs, n)
        totals = call(
            functools.partial(total_body, half, len(terms)),
            [jax.ShapeDtypeStruct((exp_dev, cap, wide), bf16)] * half,
            [WHOLE] * len(terms),
            limit=4 * 2**20,
        )(*terms)
        for j in range(first, first + half):
            back[j] = swap(totals[j - first], "ep", j) if j else totals[0]
    new_r, new_i = call(
        state_body,
        [jax.ShapeDtypeStruct((count, groups, entries), f32)] * 2,
        [WHOLE] * 5,
        limit=4 * 2**20,
    )(driven, dec_r, dec_i, bt_r, bt_i)
    result = call(
        functools.partial(combine_body, m),
        jax.ShapeDtypeStruct((count, wide), bf16),
        [WHOLE] * (3 + m),
        [pltpu.VMEM((slots, wide), bf16)],
        limit=8 * 2**20,
    )(resid, choose, route_weight.T, *back)
    return (
        result,
        new_r,
        new_i,
    )


def ssm_step(
    driven,
    state_real,
    state_imag,
    eig_real,
    eig_imag,
    log_step,
    input_real,
    input_imag,
    output_matrix_real,
    output_matrix_imag,
    skip_weight,
):
    highest_precision = lax.Precision.HIGHEST
    count_of_rows = driven.shape[0]
    groups = eig_real.shape[0]
    group_width = input_real.shape[2]
    time_step = jnp.exp(log_step)[:, None]
    magnitude = jnp.exp(eig_real * time_step)
    angle_now = eig_imag * time_step
    bar_real = magnitude * jnp.cos(angle_now)
    bar_imag = magnitude * jnp.sin(angle_now)
    modulus = eig_real * eig_real + eig_imag * eig_imag
    fac_real = ((bar_real - 1.0) * eig_real + bar_imag * eig_imag) / modulus
    fac_imag = (bar_imag * eig_real - (bar_real - 1.0) * eig_imag) / modulus
    ib_real = fac_real[..., None] * input_real - fac_imag[..., None] * input_imag
    ib_imag = fac_real[..., None] * input_imag + fac_imag[..., None] * input_real
    grouped = driven.astype(jnp.float32).reshape(count_of_rows, groups, group_width)
    push_real = jnp.einsum("gpc,ngc->ngp", ib_real, grouped, precision=highest_precision)
    push_imag = jnp.einsum("gpc,ngc->ngp", ib_imag, grouped, precision=highest_precision)
    updated_state_real = bar_real[None] * state_real - bar_imag[None] * state_imag + push_real
    updated_state_imag = bar_real[None] * state_imag + bar_imag[None] * state_real + push_imag
    state_readout = jnp.einsum(
        "jiy,sjy->sji", output_matrix_real, updated_state_real, precision=highest_precision
    ) - jnp.einsum(
        "jiy,sjy->sji", output_matrix_imag, updated_state_imag, precision=highest_precision
    )
    state_readout = state_readout.reshape(count_of_rows, groups * group_width) + skip_weight[
        None, :
    ] * driven.astype(jnp.float32)
    activated = jax.nn.gelu(state_readout).astype(jnp.bfloat16)
    return (updated_state_real, updated_state_imag, activated)


def local(
    tokens,
    state_real,
    state_imag,
    mix_gain,
    in_weight,
    eig_real,
    eig_imag,
    log_step,
    input_real,
    input_imag,
    output_matrix_real,
    output_matrix_imag,
    skip_weight,
    glu_weight,
    glu_bias,
    out_weight,
    moe_gain,
    routes,
    route_weight,
    gate_weight,
    up_weight,
    down_weight,
):
    count_of_rows = tokens.shape[0]
    n_ep = lax.axis_size("ep")
    width_tp = lax.axis_size("tp")
    whole_rows = lax.all_gather(tokens, "tp", axis=1, tiled=True)
    whole_float = whole_rows.astype(jnp.float32)
    first_scale = lax.rsqrt(jnp.mean(whole_float * whole_float, axis=1, keepdims=True) + norm_eps)
    normed = (whole_float * first_scale * mix_gain.astype(jnp.float32)).astype(jnp.bfloat16)
    driven = jnp.einsum("rd,cd->rc", normed, in_weight, preferred_element_type=jnp.float32).astype(
        jnp.bfloat16
    )
    updated_state_real, updated_state_imag, activated = ssm_step(
        driven,
        state_real,
        state_imag,
        eig_real,
        eig_imag,
        log_step,
        input_real,
        input_imag,
        output_matrix_real,
        output_matrix_imag,
        skip_weight,
    )
    gate_pre = (
        jnp.einsum(
            "rc,oc->ro",
            lax.all_gather(activated, "tp", axis=1, tiled=True),
            glu_weight,
            preferred_element_type=jnp.float32,
        )
        + glu_bias
    )
    glued = (activated.astype(jnp.float32) * jax.nn.sigmoid(gate_pre)).astype(jnp.bfloat16)
    partial_value = jnp.dot(glued, out_weight, preferred_element_type=jnp.float32)
    mixed = lax.psum_scatter(
        partial_value.astype(jnp.bfloat16), "tp", scatter_dimension=1, tiled=True
    ).astype(jnp.float32)
    residual = (tokens.astype(jnp.float32) + mixed).astype(jnp.bfloat16)
    resid_float = residual.astype(jnp.float32)
    exp_dev = gate_weight.shape[0]
    experts = exp_dev * n_ep
    top_count = routes.shape[1]
    capacity = max(2, (3 * top_count * count_of_rows + 2 * experts - 1) // (2 * experts))
    chosen = routes.reshape(-1)
    onehot = (chosen[:, None] == jnp.arange(experts, dtype=jnp.int32)[None, :]).astype(jnp.int32)
    rank_index = jnp.sum((jnp.cumsum(onehot, axis=0) - onehot) * onehot, axis=1)
    slot_index = (chosen * capacity + rank_index).reshape(count_of_rows, top_count)
    slots_all = experts * capacity
    choose = slot_index[:, :, None] == jnp.arange(slots_all, dtype=jnp.int32)[None, None, :]
    dispatch = jnp.sum(choose.astype(jnp.float32), axis=1).astype(jnp.bfloat16)
    local_sq = jnp.sum(resid_float * resid_float, axis=1)
    total_sq = lax.psum(local_sq, "tp")
    dim_full = residual.shape[1] * width_tp
    second_scale = lax.rsqrt(total_sq[:, None] / dim_full + norm_eps)
    gain_part = lax.dynamic_slice_in_dim(
        moe_gain, lax.axis_index("tp") * residual.shape[1], residual.shape[1], 0
    )
    expert_in = (resid_float * second_scale * gain_part.astype(jnp.float32)).astype(jnp.bfloat16)
    packed = jnp.einsum(
        "rs,rd->sd", dispatch, expert_in, preferred_element_type=jnp.float32
    ).astype(jnp.bfloat16)
    packed = packed.reshape(n_ep, exp_dev * capacity, residual.shape[1])
    arrived = lax.all_to_all(packed, "ep", split_axis=0, concat_axis=0, tiled=True)
    arrived = arrived.reshape(n_ep, exp_dev, capacity, residual.shape[1])
    fragment = lax.all_gather(arrived, "tp", axis=3, tiled=True)
    gate_part = jnp.einsum(
        "necd,efd->necf", fragment, gate_weight, preferred_element_type=jnp.float32
    )
    up_part = jnp.einsum("necd,efd->necf", fragment, up_weight, preferred_element_type=jnp.float32)
    hidden_width = (jax.nn.silu(gate_part) * up_part).astype(jnp.bfloat16)
    partial_out = jnp.einsum(
        "necf,efd->necd", hidden_width, down_weight, preferred_element_type=jnp.float32
    )
    summed = lax.psum_scatter(
        partial_out.astype(jnp.bfloat16), "tp", scatter_dimension=3, tiled=True
    )
    summed = summed.reshape(n_ep, exp_dev * capacity, summed.shape[3])
    returned = lax.all_to_all(summed, "ep", split_axis=0, concat_axis=0, tiled=True)
    returned = returned.reshape(slots_all, returned.shape[2])
    gathered_k = jnp.einsum(
        "rks,sd->rkd", choose.astype(jnp.bfloat16), returned, preferred_element_type=jnp.float32
    )
    result = (resid_float + jnp.sum(route_weight[..., None] * gathered_k, axis=1)).astype(
        jnp.bfloat16
    )
    return (result, updated_state_real, updated_state_imag)


def solution(mesh):
    n, m = mesh.shape["tp"], mesh.shape["ep"]
    small = n in (4, 8) and m in (2, 4)

    def whole(*args):
        if not small:
            return local(*args)
        return local_swaps(*args)

    return jax.shard_map(
        whole,
        mesh=mesh,
        in_specs=(
            P("ep", "tp"),
            P("ep", "tp", None),
            P("ep", "tp", None),
            P(),
            P("tp", None),
            P("tp", None),
            P("tp", None),
            P("tp"),
            P("tp", None, None),
            P("tp", None, None),
            P("tp", None, None),
            P("tp", None, None),
            P("tp"),
            P("tp", None),
            P("tp"),
            P("tp", None),
            P(),
            P("ep", None),
            P("ep", None),
            P("ep", "tp", None),
            P("ep", "tp", None),
            P("ep", "tp", None),
        ),
        out_specs=(P("ep", "tp"), P("ep", "tp", None), P("ep", "tp", None)),
        check_vma=False,
    )
```

```python
import functools
import jax
import jax.numpy as jnp
from jax import lax
from jax.experimental import pallas as pl
from jax.experimental.pallas import tpu as pltpu
from jax.sharding import PartitionSpec as P


norm_eps = 1e-06
f32 = jnp.float32
bf16 = jnp.bfloat16
NT = (((1,), (1,)), ((), ()))
NN = (((1,), (0,)), ((), ()))
WHOLE = pl.BlockSpec(memory_space=pltpu.VMEM)
FAR = pl.BlockSpec(memory_space=pltpu.HBM)
LANES = 128


def stay(x):
    return pltpu.with_memory_space_constraint(x, pltpu.HBM)


def dot(a, b, dims):
    return lax.dot_general(a, b, dims, preferred_element_type=f32)


def swap(x, axis, k):
    return lax.ppermute(x, axis, [(i, i ^ k) for i in range(lax.axis_size(axis))])


def crossings(n):
    return [0] + [k + 1 for k in range(2, n, 2)]


def gather_swaps(x, n):
    pieces = [None] * n
    pieces[0] = x
    for k in crossings(n)[1:]:
        pieces[k] = swap(x, "tp", k)
    for k in crossings(n):
        pieces[k ^ 1] = swap(pieces[k], "tp", 1)
    return pieces


def pair_swaps(own, partner, n):
    other = swap(partner, "tp", 1)
    shape = own.shape[1:]
    return call(
        pair_body,
        [jax.ShapeDtypeStruct(shape, f32)] + [jax.ShapeDtypeStruct(shape, bf16)] * (n // 2 - 1),
        [WHOLE] * 2,
        limit=8 * 2**20,
    )(own, other)


def reduce_swaps(own, partner, n):
    first, *rest = pair_swaps(own, partner, n)
    return [first] + [swap(x, "tp", k) for x, k in zip(rest, crossings(n)[1:])]


def pair_body(own, other, *outs):
    for i, out in enumerate(outs):
        out[...] = (own[i].astype(f32) + other[i].astype(f32)).astype(out.dtype)


def call(body, out_shape, in_specs, scratch=(), limit=None, flops=10**7):
    single = not isinstance(out_shape, (list, tuple))
    return pl.pallas_call(
        body,
        out_shape=out_shape,
        in_specs=in_specs,
        out_specs=WHOLE if single else [WHOLE] * len(out_shape),
        scratch_shapes=list(scratch),
        compiler_params=pltpu.CompilerParams(vmem_limit_bytes=limit),
        cost_estimate=pl.CostEstimate(flops=flops, bytes_accessed=10**6, transcendentals=0),
    )


def fold(x):
    total = x[:, :LANES]
    for c in range(LANES, x.shape[1], LANES):
        total = total + x[:, c : c + LANES]
    return total


def column(row):
    n = row.shape[1]
    at = lax.broadcasted_iota(jnp.int32, (n, n), 0)
    to = lax.broadcasted_iota(jnp.int32, (n, n), 1)
    return jnp.sum(jnp.where(at == to, jnp.broadcast_to(row, (n, n)), 0.0), axis=1, keepdims=True)


def place(k, width):
    return pl.ds(pl.multiple_of((lax.axis_index("tp") ^ k) * width, width), width)


def prep_body(n, cap, *refs):
    weight_hbm = refs[0]
    far = refs[1:16]
    dec_r, dec_i, bt_r, bt_i, base, mix, choose, table = refs[16:24]
    flat = refs[24:28]
    weight, tokens = refs[28:30]
    held = refs[30:44]
    sems, weight_sems, fac = refs[44:]
    held = (*held, tokens)
    copies = [pltpu.make_async_copy(a, b, sems.at[i]) for i, (a, b) in enumerate(zip(far, held))]
    for copy in copies:
        copy.start()
    weights = load(weight_hbm, weight, weight_sems, n, weight.shape[2])
    copies[13].wait()
    routes = held[13]
    slots, count = table.shape
    top = routes.shape[0]
    names = lax.broadcasted_iota(jnp.int32, (16, count), 0)
    marks = [(routes[r : r + 1, :] == names).astype(f32) for r in range(top)]
    total = marks[0]
    for r in range(1, top):
        total = total + marks[r]
    row = lax.broadcasted_iota(jnp.int32, (count, count), 0)
    col = lax.broadcasted_iota(jnp.int32, (count, count), 1)
    before = dot(total.astype(bf16), (row < col).astype(bf16), NN)
    same = (row == col).astype(bf16)
    places = lax.broadcasted_iota(jnp.int32, (slots, count), 0).astype(f32)
    used = jnp.zeros((slots, count), f32)
    for r in range(top):
        rank = jnp.sum(before * marks[r], axis=0, keepdims=True)
        slot = routes[r : r + 1, :].astype(f32) * cap + rank
        hit = (places == slot).astype(f32)
        choose[r] = dot(same, hit.astype(bf16), NT).astype(bf16)
        used = used + hit
    table[...] = used.astype(bf16)
    st_r, st_i, in_r, in_i, om_r, om_i = held[:6]
    groups, inner, entries = in_r.shape
    pack = LANES // inner
    in_r, in_i, om_r, om_i = (x for x in held[2:6])
    for i in range(2, 6):
        copies[i].wait()
    for i in (0, 1, 10, 11, 12):
        copies[i].wait()
    real, imag, log_step = held[10][...], held[11][...], held[12][...]
    step = column(jnp.exp(log_step))
    size = jnp.exp(real * step)
    angle = imag * step
    bar_r = size * jnp.cos(angle)
    bar_i = size * jnp.sin(angle)
    modulus = real * real + imag * imag
    fac_r = ((bar_r - 1.0) * real + bar_i * imag) / modulus
    fac_i = (bar_i * real - (bar_r - 1.0) * imag) / modulus
    for g in range(groups):
        cols = slice(g * entries, (g + 1) * entries)
        s_r, s_i = st_r[:, g, :], st_i[:, g, :]
        b_r, b_i = bar_r[g : g + 1, :], bar_i[g : g + 1, :]
        dec_r[:, cols] = b_r * s_r - b_i * s_i
        dec_i[:, cols] = b_r * s_i + b_i * s_r
        fac[0:1, cols] = fac_r[g : g + 1, :]
        fac[1:2, cols] = fac_i[g : g + 1, :]
    high = pack * entries
    for b in range(groups // pack):
        each = slice(b * pack, (b + 1) * pack)
        lanes = slice(b * LANES, (b + 1) * LANES)
        rows = slice(b * high, (b + 1) * high)
        b_r, b_i, c_r, c_i = (
            spread(x[each].reshape(LANES, entries), inner, pack) for x in (in_r, in_i, om_r, om_i)
        )
        f_r, f_i = fac[0:1, rows], fac[1:2, rows]
        i_r = (f_r * b_r - f_i * b_i).astype(bf16)
        i_i = (f_r * b_i + f_i * b_r).astype(bf16)
        c_r, c_i = c_r.astype(bf16), c_i.astype(bf16)
        bt_r[lanes, :] = i_r
        bt_i[lanes, :] = i_i
        mix[lanes, :] = (dot(i_r, c_r, NT) - dot(i_i, c_i, NT)).astype(bf16)
        base[:, lanes] = dot(dec_r[:, rows].astype(bf16), c_r, NT) - dot(
            dec_i[:, rows].astype(bf16), c_i, NT
        )
    for i in range(len(flat)):
        copies[6 + i].wait()
        rows = held[6 + i][...].astype(f32)
        for r in range(rows.shape[0]):
            flat[i][0:1, r * LANES : (r + 1) * LANES] = rows[r : r + 1, :]
    copies[14].wait()
    for copy in weights:
        copy.wait()


def spread(blocks, height, pack):
    rows, inner = blocks.shape
    columns = pack * inner
    at = lax.broadcasted_iota(jnp.int32, (inner, columns), 0)
    to = lax.broadcasted_iota(jnp.int32, (inner, columns), 1)
    wide = dot(blocks.astype(bf16), (to % inner == at).astype(bf16), NN)
    row = lax.broadcasted_iota(jnp.int32, (rows, columns), 0)
    col = lax.broadcasted_iota(jnp.int32, (rows, columns), 1)
    return jnp.where(row // height == col // inner, wide, 0.0)


def load(src, dst, sems, n, width):
    copies = []
    for k in range(n):
        part = src.at[:, place(k, width)] if len(src.shape) == 2 else src.at[:, :, place(k, width)]
        copies.append(pltpu.make_async_copy(part, dst.at[k], sems.at[k]))
    for copy in copies:
        copy.start()
    return copies


def mixer_sums(n, odd, pieces, gain, weight, start):
    total, turned, square = start
    width = pieces[0].shape[1]
    for at, (k, piece) in enumerate(zip(crossings(n), pieces)):
        k = k ^ odd
        x = piece[...].astype(f32)
        square = square + fold(x * x)
        x = (x * gain[:, place(k, width)]).astype(bf16)
        if at % 2:
            turned = turned + dot(weight[k], x, NT)
        else:
            total = total + dot(x, weight[k], NT)
    return total, turned, square


def first_body(n, *refs):
    pieces = refs[: n // 2]
    gain, weight = refs[n // 2 : n // 2 + 2]
    for out, value in zip(refs[n // 2 + 2 :], mixer_sums(n, 0, pieces, gain, weight, (0.0, 0.0, 0.0))):
        out[...] = value


def mixer_body(n, *refs):
    pieces = refs[: n // 2]
    gain, weight, base, mix, skip, total, turned, square = refs[n // 2 : n // 2 + 8]
    driven_ref, act_ref = refs[n // 2 + 8 :]
    start = (total[...], turned[...], square[...])
    total, turned, square = mixer_sums(n, 1, pieces, gain, weight, start)
    width = pieces[0].shape[1]
    scale = lax.rsqrt(jnp.sum(square, axis=1, keepdims=True) / (n * width) + norm_eps)
    driven = ((total + turned.T) * scale).astype(bf16)
    driven_ref[...] = driven
    for b in range(driven.shape[1] // LANES):
        lanes = slice(b * LANES, (b + 1) * LANES)
        out = base[:, lanes] + dot(driven[:, lanes], mix[lanes, :], NN)
        out = out + skip[:, lanes] * driven[:, lanes].astype(f32)
        act_ref[:, lanes] = jax.nn.gelu(out).astype(bf16)


def state_body(driven, dec_r, dec_i, bt_r, bt_i, out_r, out_i):
    groups, entries = out_r.shape[1:]
    high = bt_r.shape[1]
    pack = high // entries
    for dec, bt, out in ((dec_r, bt_r, out_r), (dec_i, bt_i, out_i)):
        for b in range(groups // pack):
            lanes = slice(b * LANES, (b + 1) * LANES)
            new = dec[:, b * high : (b + 1) * high] + dot(driven[:, lanes], bt[lanes, :], NN)
            for g in range(pack):
                out[:, b * pack + g, :] = new[:, g * entries : (g + 1) * entries]


PARTS = 8


def fetch_body(spans, *refs):
    count = len(spans)
    copies = []
    for i, (low, high) in enumerate(spans):
        src, dst, sems = refs[i], refs[count + i], refs[2 * count + i]
        step = (high - low) // PARTS
        for p in range(PARTS):
            copies.append(
                pltpu.make_async_copy(
                    src.at[pl.ds(low + p * step, step)], dst.at[pl.ds(p * step, step)], sems.at[p]
                )
            )
            copies[-1].start()
    for copy in copies:
        copy.wait()


def fetch(*sources):
    sources = [x if isinstance(x, tuple) else (x, 0, x.shape[0]) for x in sources]
    return call(
        functools.partial(fetch_body, [x[1:] for x in sources]),
        [pltpu.VMEM((high - low, x.shape[1]), bf16) for x, low, high in sources],
        [FAR] * len(sources),
        [pltpu.SemaphoreType.DMA((PARTS,))] * len(sources),
        limit=2**20,
    )(*[stay(x) for x, _, _ in sources])


def rows_of(weight, i, experts):
    height = weight.shape[0] // experts
    return slice(i * height, (i + 1) * height)


def glu_sums(odd, pieces, glu, gate, turned):
    width = pieces[0].shape[1]
    for at, (k, piece) in enumerate(zip(crossings(2 * len(pieces)), pieces)):
        block = glu[:, place(k ^ odd, width)]
        if at % 2:
            turned = turned + dot(block, piece[...], NT)
        else:
            gate = gate + dot(piece[...], block, NT)
    return gate, turned


def gate_body(n, *refs):
    pieces = refs[: n // 2]
    glu, bias, gate_ref, turned_ref = refs[n // 2 :]
    gate_ref[...], turned_ref[...] = glu_sums(0, pieces, glu, bias[...], 0.0)


def glu_body(n, *refs):
    pieces = refs[: n // 2]
    own, glu, gate, turned, out_w = refs[n // 2 : n // 2 + 5]
    glued_ref, partner = refs[n // 2 + 5 :]
    gate, turned = glu_sums(1, pieces, glu, gate[...], turned[...])
    glued = (own[...].astype(f32) * jax.nn.sigmoid(gate + turned.T)).astype(bf16)
    glued_ref[...] = glued
    for at, k in enumerate(crossings(n)):
        partner[at] = dot(glued, out_w[:, place(k ^ 1, partner.shape[2])], NN).astype(bf16)


def out_body(n, glued, out_w, own):
    for at, k in enumerate(crossings(n)):
        own[at] = dot(glued[...], out_w[:, place(k, own.shape[2])], NN).astype(bf16)


def merge_body(*refs):
    out = refs[-1]
    cap = refs[0].shape[1]
    for j, x in enumerate(refs[:-1]):
        out[:, j * cap : (j + 1) * cap, :] = x[...]


def dispatch_body(m, terms, *refs):
    tokens = refs[0]
    sums = refs[1 : 1 + terms]
    table = refs[1 + terms]
    resid_ref = refs[2 + terms]
    outs = refs[3 + terms :]
    mixed = sums[0][...]
    for s in sums[1:]:
        mixed = mixed + s[...].astype(f32)
    resid = (tokens[...].astype(f32) + mixed).astype(bf16)
    resid_ref[...] = resid
    experts, cap, wide = outs[0].shape
    count = experts * cap
    for j in range(m):
        at = pl.multiple_of((lax.axis_index("ep") ^ j) * count, count)
        picked = dot(table[pl.ds(at, count), :], resid, NN).astype(bf16)
        outs[j][...] = picked.reshape(experts, cap, wide)


def expert_sums(odd, near, far, gain, gate_w, up_low, up_high, i, start):
    g, u, square = start
    experts, _, width = near[0].shape
    height = gate_w.shape[0] // experts
    held = up_low.shape[0] // height
    up_w, row = (up_low, i) if i < held else (up_high, i - held)
    for at, k in enumerate(crossings(2 * len(near))):
        k = k ^ odd
        x = jnp.concatenate([near[at][i], far[at][i]], axis=0).astype(f32)
        square = square + fold(x * x)
        x = (x * gain[:, place(k, width)]).astype(bf16)
        g = g + dot(x, gate_w[rows_of(gate_w, i, experts), place(k, width)], NT)
        u = u + dot(up_w[row * height : (row + 1) * height, place(k, width)], x, NT)
    return g, u, square


def even_body(n, *refs):
    near, far = refs[: n // 2], refs[n // 2 : n]
    gain, gate_w, up_low, up_high, g_ref, u_ref, square_ref = refs[n:]
    for i in range(near[0].shape[0]):
        g_ref[i], u_ref[i], square_ref[i] = expert_sums(
            0, near, far, gain, gate_w, up_low, up_high, i, (0.0, 0.0, 0.0)
        )


def up_body(n, *refs):
    near, far = refs[: n // 2], refs[n // 2 : n]
    gain, gate_w, up_low, up_high, down_w, g_ref, u_ref, square_ref = refs[n : n + 8]
    later, partner = refs[n + 8 :]
    experts, count, width = near[0].shape
    for i in range(experts):
        start = (g_ref[i], u_ref[i], square_ref[i])
        g, u, square = expert_sums(1, near, far, gain, gate_w, up_low, up_high, i, start)
        scale = lax.rsqrt(jnp.sum(square, axis=1, keepdims=True) / (n * width) + norm_eps)
        hidden = (jax.nn.silu(g * scale) * (u.T * scale)).astype(bf16)
        later[i] = hidden
        for at, k in enumerate(crossings(n)):
            block = down_w[rows_of(down_w, i, experts), place(k ^ 1, width)]
            partner[at, i] = dot(hidden[count:], block, NN).astype(bf16)


def down_body(n, hidden, down_w, far_own, own, partner):
    count, width = own.shape[2:]
    experts = hidden.shape[0]
    for i in range(experts):
        near, far = hidden[i, :count], hidden[i, count:]
        for at, k in enumerate(crossings(n)):
            block = down_w[rows_of(down_w, i, experts), place(k, width)]
            far_own[at, i] = dot(far, block, NN).astype(bf16)
            own[at, i] = dot(near, block, NN).astype(bf16)
        for at, k in enumerate(crossings(n)):
            block = down_w[rows_of(down_w, i, experts), place(k ^ 1, width)]
            partner[at, i] = dot(near, block, NN).astype(bf16)


def total_body(m, terms, *refs):
    sums = refs[:terms]
    outs = refs[terms:]
    total = sums[0][...]
    for s in sums[1:]:
        total = total + s[...].astype(f32)
    total = total.astype(bf16)
    cap = outs[0].shape[1]
    for j in range(m):
        outs[j][...] = total[:, j * cap : (j + 1) * cap, :]


def combine_body(m, *refs):
    resid, choose, weight = refs[:3]
    back = refs[3 : 3 + m]
    out, rows = refs[3 + m :]
    experts, cap, wide = back[0].shape
    count = experts * cap
    for j in range(m):
        at = pl.multiple_of((lax.axis_index("ep") ^ j) * count, count)
        rows[pl.ds(at, count), :] = back[j][...].reshape(count, wide)
    total = resid[...].astype(f32)
    for r in range(weight.shape[0]):
        picked = dot(choose[r], rows[...], NN)
        total = total + column(weight[r : r + 1, :]) * picked
    out[...] = total.astype(bf16)


def local_swaps(
    tokens,
    state_real,
    state_imag,
    mix_gain,
    in_weight,
    eig_real,
    eig_imag,
    log_step,
    input_real,
    input_imag,
    output_matrix_real,
    output_matrix_imag,
    skip_weight,
    glu_weight,
    glu_bias,
    out_weight,
    moe_gain,
    routes,
    route_weight,
    gate_weight,
    up_weight,
    down_weight,
):
    count, wide = tokens.shape
    n = lax.axis_size("tp")
    m = lax.axis_size("ep")
    groups, entries = eig_real.shape
    inner = input_real.shape[2]
    states = groups * entries
    channels = groups * inner
    full = wide * n
    exp_dev = gate_weight.shape[0]
    experts = exp_dev * m
    top = routes.shape[1]
    cap = max(2, (3 * top * count + 2 * experts - 1) // (2 * experts))
    slots = experts * cap

    pieces = gather_swaps(tokens, n)
    pack = LANES // inner
    far = [
        state_real,
        state_imag,
        input_real.transpose(0, 2, 1),
        input_imag.transpose(0, 2, 1),
        output_matrix_real,
        output_matrix_imag,
        skip_weight.reshape(-1, LANES),
        glu_bias.reshape(-1, LANES),
        mix_gain.reshape(-1, LANES),
        moe_gain.reshape(-1, LANES),
        eig_real,
        eig_imag,
        log_step.reshape(1, groups),
        routes.T,
        tokens,
    ]
    dec_r, dec_i, bt_r, bt_i, base, mix, choose, table, skip, bias, gain1, gain2, in_w, own = call(
        functools.partial(prep_body, n, cap),
        [jax.ShapeDtypeStruct((count, states), f32)] * 2
        + [jax.ShapeDtypeStruct((channels, pack * entries), bf16)] * 2
        + [
            jax.ShapeDtypeStruct((count, channels), f32),
            jax.ShapeDtypeStruct((channels, LANES), bf16),
            jax.ShapeDtypeStruct((top, count, slots), bf16),
            jax.ShapeDtypeStruct((slots, count), bf16),
        ]
        + [jax.ShapeDtypeStruct((1, channels), f32)] * 2
        + [jax.ShapeDtypeStruct((1, full), f32)] * 2
        + [pltpu.VMEM((n, channels, wide), bf16), pltpu.VMEM((count, wide), bf16)],
        [FAR] * 16,
        [pltpu.VMEM(x.shape, x.dtype) for x in far[:-1]]
        + [pltpu.SemaphoreType.DMA((15,)), pltpu.SemaphoreType.DMA((n,))]
        + [pltpu.VMEM((2, states), f32)],
        limit=12 * 2**20,
    )(*[stay(x) for x in [in_weight] + far])
    pieces[0] = own

    partial = call(
        functools.partial(first_body, n),
        [jax.ShapeDtypeStruct(x, f32) for x in ((count, channels), (channels, count), (count, LANES))],
        [WHOLE] * (n // 2 + 2),
        limit=8 * 2**20,
    )(*[pieces[k] for k in crossings(n)], gain1, in_w)
    driven, activated = call(
        functools.partial(mixer_body, n),
        [jax.ShapeDtypeStruct((count, channels), bf16)] * 2,
        [WHOLE] * (n // 2 + 8),
        limit=12 * 2**20,
    )(*[pieces[k ^ 1] for k in crossings(n)], gain1, in_w, base, mix, skip, *partial)

    acts = gather_swaps(activated, n)
    glu_w, out_w = fetch(glu_weight, out_weight)
    block = jax.ShapeDtypeStruct((n // 2, count, wide), bf16)
    partial = call(
        functools.partial(gate_body, n),
        [jax.ShapeDtypeStruct(x, f32) for x in ((count, channels), (channels, count))],
        [WHOLE] * (n // 2 + 2),
        limit=8 * 2**20,
    )(*[acts[k] for k in crossings(n)], glu_w, bias)
    glued, partner = call(
        functools.partial(glu_body, n),
        [jax.ShapeDtypeStruct((count, channels), bf16), block],
        [WHOLE] * (n // 2 + 5),
        limit=12 * 2**20,
    )(*[acts[k ^ 1] for k in crossings(n)], acts[0], glu_w, *partial, out_w)
    sums = call(functools.partial(out_body, n), block, [WHOLE] * 2, limit=8 * 2**20)(glued, out_w)

    terms = reduce_swaps(sums, partner, n)
    hidden = gate_weight.shape[1]
    flat_up = up_weight.reshape(-1, full)
    held = (exp_dev + 1) // 2 * hidden
    gate_w, up_low = fetch(gate_weight.reshape(-1, full), (flat_up, 0, held))
    (up_high,) = fetch((flat_up, held, exp_dev * hidden))
    (down_w,) = fetch(down_weight.reshape(-1, full))
    resid, *packed = call(
        functools.partial(dispatch_body, m, len(terms)),
        [jax.ShapeDtypeStruct((count, wide), bf16)]
        + [jax.ShapeDtypeStruct((exp_dev, cap, wide), bf16)] * m,
        [WHOLE] * (2 + len(terms)),
        limit=8 * 2**20,
    )(own, *terms, table)

    arrived = [packed[0]] + [swap(packed[j], "ep", j) for j in range(1, m)]
    half = m // 2
    fragments = []
    for group in (arrived[:half], arrived[half:]):
        merged = call(
            merge_body,
            jax.ShapeDtypeStruct((exp_dev, half * cap, wide), bf16),
            [WHOLE] * half,
            limit=2**20,
        )(*group)
        fragments += gather_swaps(merged, n)
    part = jax.ShapeDtypeStruct((n // 2, exp_dev, half * cap, wide), bf16)
    near, far = fragments[:n], fragments[n:]
    rows = 2 * half * cap
    weights = (gain2, gate_w, up_low, up_high)
    partial = call(
        functools.partial(even_body, n),
        [jax.ShapeDtypeStruct((exp_dev, *x), f32) for x in ((rows, hidden), (hidden, rows), (rows, LANES))],
        [WHOLE] * (n + 4),
        limit=8 * 2**20,
    )(*[near[k] for k in crossings(n)], *[far[k] for k in crossings(n)], *weights)
    later, far_partner = call(
        functools.partial(up_body, n),
        [jax.ShapeDtypeStruct((exp_dev, rows, hidden), bf16), part],
        [WHOLE] * (n + 8),
        limit=16 * 2**20,
    )(*[near[k ^ 1] for k in crossings(n)], *[far[k ^ 1] for k in crossings(n)], *weights, down_w, *partial)
    far_own, *near_outs = call(
        functools.partial(down_body, n), [part] * 3, [WHOLE] * 2, limit=8 * 2**20
    )(later, down_w)
    far_outs = [far_own, far_partner]
    back = [None] * m
    for outs, first in ((far_outs, half), (near_outs, 0)):
        terms = reduce_swaps(*outs, n)
        totals = call(
            functools.partial(total_body, half, len(terms)),
            [jax.ShapeDtypeStruct((exp_dev, cap, wide), bf16)] * half,
            [WHOLE] * len(terms),
            limit=4 * 2**20,
        )(*terms)
        for j in range(first, first + half):
            back[j] = swap(totals[j - first], "ep", j) if j else totals[0]
    new_r, new_i = call(
        state_body,
        [jax.ShapeDtypeStruct((count, groups, entries), f32)] * 2,
        [WHOLE] * 5,
        limit=4 * 2**20,
    )(driven, dec_r, dec_i, bt_r, bt_i)
    result = call(
        functools.partial(combine_body, m),
        jax.ShapeDtypeStruct((count, wide), bf16),
        [WHOLE] * (3 + m),
        [pltpu.VMEM((slots, wide), bf16)],
        limit=8 * 2**20,
    )(resid, choose, route_weight.T, *back)
    return (
        result,
        new_r,
        new_i,
    )


def ssm_step(
    driven,
    state_real,
    state_imag,
    eig_real,
    eig_imag,
    log_step,
    input_real,
    input_imag,
    output_matrix_real,
    output_matrix_imag,
    skip_weight,
):
    highest_precision = lax.Precision.HIGHEST
    count_of_rows = driven.shape[0]
    groups = eig_real.shape[0]
    group_width = input_real.shape[2]
    time_step = jnp.exp(log_step)[:, None]
    magnitude = jnp.exp(eig_real * time_step)
    angle_now = eig_imag * time_step
    bar_real = magnitude * jnp.cos(angle_now)
    bar_imag = magnitude * jnp.sin(angle_now)
    modulus = eig_real * eig_real + eig_imag * eig_imag
    fac_real = ((bar_real - 1.0) * eig_real + bar_imag * eig_imag) / modulus
    fac_imag = (bar_imag * eig_real - (bar_real - 1.0) * eig_imag) / modulus
    ib_real = fac_real[..., None] * input_real - fac_imag[..., None] * input_imag
    ib_imag = fac_real[..., None] * input_imag + fac_imag[..., None] * input_real
    grouped = driven.astype(jnp.float32).reshape(count_of_rows, groups, group_width)
    push_real = jnp.einsum("gpc,ngc->ngp", ib_real, grouped, precision=highest_precision)
    push_imag = jnp.einsum("gpc,ngc->ngp", ib_imag, grouped, precision=highest_precision)
    updated_state_real = bar_real[None] * state_real - bar_imag[None] * state_imag + push_real
    updated_state_imag = bar_real[None] * state_imag + bar_imag[None] * state_real + push_imag
    state_readout = jnp.einsum(
        "jiy,sjy->sji", output_matrix_real, updated_state_real, precision=highest_precision
    ) - jnp.einsum(
        "jiy,sjy->sji", output_matrix_imag, updated_state_imag, precision=highest_precision
    )
    state_readout = state_readout.reshape(count_of_rows, groups * group_width) + skip_weight[
        None, :
    ] * driven.astype(jnp.float32)
    activated = jax.nn.gelu(state_readout).astype(jnp.bfloat16)
    return (updated_state_real, updated_state_imag, activated)


def local(
    tokens,
    state_real,
    state_imag,
    mix_gain,
    in_weight,
    eig_real,
    eig_imag,
    log_step,
    input_real,
    input_imag,
    output_matrix_real,
    output_matrix_imag,
    skip_weight,
    glu_weight,
    glu_bias,
    out_weight,
    moe_gain,
    routes,
    route_weight,
    gate_weight,
    up_weight,
    down_weight,
):
    count_of_rows = tokens.shape[0]
    n_ep = lax.axis_size("ep")
    width_tp = lax.axis_size("tp")
    whole_rows = lax.all_gather(tokens, "tp", axis=1, tiled=True)
    whole_float = whole_rows.astype(jnp.float32)
    first_scale = lax.rsqrt(jnp.mean(whole_float * whole_float, axis=1, keepdims=True) + norm_eps)
    normed = (whole_float * first_scale * mix_gain.astype(jnp.float32)).astype(jnp.bfloat16)
    driven = jnp.einsum("rd,cd->rc", normed, in_weight, preferred_element_type=jnp.float32).astype(
        jnp.bfloat16
    )
    updated_state_real, updated_state_imag, activated = ssm_step(
        driven,
        state_real,
        state_imag,
        eig_real,
        eig_imag,
        log_step,
        input_real,
        input_imag,
        output_matrix_real,
        output_matrix_imag,
        skip_weight,
    )
    gate_pre = (
        jnp.einsum(
            "rc,oc->ro",
            lax.all_gather(activated, "tp", axis=1, tiled=True),
            glu_weight,
            preferred_element_type=jnp.float32,
        )
        + glu_bias
    )
    glued = (activated.astype(jnp.float32) * jax.nn.sigmoid(gate_pre)).astype(jnp.bfloat16)
    partial_value = jnp.dot(glued, out_weight, preferred_element_type=jnp.float32)
    mixed = lax.psum_scatter(
        partial_value.astype(jnp.bfloat16), "tp", scatter_dimension=1, tiled=True
    ).astype(jnp.float32)
    residual = (tokens.astype(jnp.float32) + mixed).astype(jnp.bfloat16)
    resid_float = residual.astype(jnp.float32)
    exp_dev = gate_weight.shape[0]
    experts = exp_dev * n_ep
    top_count = routes.shape[1]
    capacity = max(2, (3 * top_count * count_of_rows + 2 * experts - 1) // (2 * experts))
    chosen = routes.reshape(-1)
    onehot = (chosen[:, None] == jnp.arange(experts, dtype=jnp.int32)[None, :]).astype(jnp.int32)
    rank_index = jnp.sum((jnp.cumsum(onehot, axis=0) - onehot) * onehot, axis=1)
    slot_index = (chosen * capacity + rank_index).reshape(count_of_rows, top_count)
    slots_all = experts * capacity
    choose = slot_index[:, :, None] == jnp.arange(slots_all, dtype=jnp.int32)[None, None, :]
    dispatch = jnp.sum(choose.astype(jnp.float32), axis=1).astype(jnp.bfloat16)
    local_sq = jnp.sum(resid_float * resid_float, axis=1)
    total_sq = lax.psum(local_sq, "tp")
    dim_full = residual.shape[1] * width_tp
    second_scale = lax.rsqrt(total_sq[:, None] / dim_full + norm_eps)
    gain_part = lax.dynamic_slice_in_dim(
        moe_gain, lax.axis_index("tp") * residual.shape[1], residual.shape[1], 0
    )
    expert_in = (resid_float * second_scale * gain_part.astype(jnp.float32)).astype(jnp.bfloat16)
    packed = jnp.einsum(
        "rs,rd->sd", dispatch, expert_in, preferred_element_type=jnp.float32
    ).astype(jnp.bfloat16)
    packed = packed.reshape(n_ep, exp_dev * capacity, residual.shape[1])
    arrived = lax.all_to_all(packed, "ep", split_axis=0, concat_axis=0, tiled=True)
    arrived = arrived.reshape(n_ep, exp_dev, capacity, residual.shape[1])
    fragment = lax.all_gather(arrived, "tp", axis=3, tiled=True)
    gate_part = jnp.einsum(
        "necd,efd->necf", fragment, gate_weight, preferred_element_type=jnp.float32
    )
    up_part = jnp.einsum("necd,efd->necf", fragment, up_weight, preferred_element_type=jnp.float32)
    hidden_width = (jax.nn.silu(gate_part) * up_part).astype(jnp.bfloat16)
    partial_out = jnp.einsum(
        "necf,efd->necd", hidden_width, down_weight, preferred_element_type=jnp.float32
    )
    summed = lax.psum_scatter(
        partial_out.astype(jnp.bfloat16), "tp", scatter_dimension=3, tiled=True
    )
    summed = summed.reshape(n_ep, exp_dev * capacity, summed.shape[3])
    returned = lax.all_to_all(summed, "ep", split_axis=0, concat_axis=0, tiled=True)
    returned = returned.reshape(slots_all, returned.shape[2])
    gathered_k = jnp.einsum(
        "rks,sd->rkd", choose.astype(jnp.bfloat16), returned, preferred_element_type=jnp.float32
    )
    result = (resid_float + jnp.sum(route_weight[..., None] * gathered_k, axis=1)).astype(
        jnp.bfloat16
    )
    return (result, updated_state_real, updated_state_imag)


def solution(mesh):
    n, m = mesh.shape["tp"], mesh.shape["ep"]
    small = n in (4, 8) and m in (2, 4)

    def whole(*args):
        if not small:
            return local(*args)
        return local_swaps(*args)

    return jax.shard_map(
        whole,
        mesh=mesh,
        in_specs=(
            P("ep", "tp"),
            P("ep", "tp", None),
            P("ep", "tp", None),
            P(),
            P("tp", None),
            P("tp", None),
            P("tp", None),
            P("tp"),
            P("tp", None, None),
            P("tp", None, None),
            P("tp", None, None),
            P("tp", None, None),
            P("tp"),
            P("tp", None),
            P("tp"),
            P("tp", None),
            P(),
            P("ep", None),
            P("ep", None),
            P("ep", "tp", None),
            P("ep", "tp", None),
            P("ep", "tp", None),
        ),
        out_specs=(P("ep", "tp"), P("ep", "tp", None), P("ep", "tp", None)),
        check_vma=False,
    )
```

```python
import functools
import jax
import jax.numpy as jnp
from jax import lax
from jax.experimental import pallas as pl
from jax.experimental.pallas import tpu as pltpu
from jax.sharding import PartitionSpec as P


norm_eps = 1e-06
f32 = jnp.float32
bf16 = jnp.bfloat16
NT = (((1,), (1,)), ((), ()))
NN = (((1,), (0,)), ((), ()))
WHOLE = pl.BlockSpec(memory_space=pltpu.VMEM)
FAR = pl.BlockSpec(memory_space=pltpu.HBM)
LANES = 128


def stay(x):
    return pltpu.with_memory_space_constraint(x, pltpu.HBM)


def dot(a, b, dims):
    return lax.dot_general(a, b, dims, preferred_element_type=f32)


def swap(x, axis, k):
    return lax.ppermute(x, axis, [(i, i ^ k) for i in range(lax.axis_size(axis))])


def far_swap(x, j):
    n = lax.axis_size("tp")
    total = n * lax.axis_size("ep")
    return lax.ppermute(x, ("ep", "tp"), [(i, i ^ (j * n + 1)) for i in range(total)])


def crossings(n):
    return [0] + [k + 1 for k in range(2, n, 2)]


def gather_swaps(x, n):
    pieces = [None] * n
    pieces[0] = x
    for k in crossings(n)[1:]:
        pieces[k] = swap(x, "tp", k)
    for k in crossings(n):
        pieces[k ^ 1] = swap(pieces[k], "tp", 1)
    return pieces


def pair_swaps(own, partner, n):
    other = swap(partner, "tp", 1)
    shape = own.shape[1:]
    return call(
        pair_body,
        [jax.ShapeDtypeStruct(shape, f32)] + [jax.ShapeDtypeStruct(shape, bf16)] * (n // 2 - 1),
        [WHOLE] * 2,
        limit=8 * 2**20,
    )(own, other)


def reduce_swaps(own, partner, n):
    first, *rest = pair_swaps(own, partner, n)
    return [first] + [swap(x, "tp", k) for x, k in zip(rest, crossings(n)[1:])]


def pair_body(own, other, *outs):
    for i, out in enumerate(outs):
        out[...] = (own[i].astype(f32) + other[i].astype(f32)).astype(out.dtype)


def call(body, out_shape, in_specs, scratch=(), limit=None, flops=10**7):
    single = not isinstance(out_shape, (list, tuple))
    return pl.pallas_call(
        body,
        out_shape=out_shape,
        in_specs=in_specs,
        out_specs=WHOLE if single else [WHOLE] * len(out_shape),
        scratch_shapes=list(scratch),
        compiler_params=pltpu.CompilerParams(vmem_limit_bytes=limit),
        cost_estimate=pl.CostEstimate(flops=flops, bytes_accessed=10**6, transcendentals=0),
    )


def fold(x):
    total = x[:, :LANES]
    for c in range(LANES, x.shape[1], LANES):
        total = total + x[:, c : c + LANES]
    return total


def column(row):
    n = row.shape[1]
    at = lax.broadcasted_iota(jnp.int32, (n, n), 0)
    to = lax.broadcasted_iota(jnp.int32, (n, n), 1)
    return jnp.sum(jnp.where(at == to, jnp.broadcast_to(row, (n, n)), 0.0), axis=1, keepdims=True)


def place(k, width):
    return pl.ds(pl.multiple_of((lax.axis_index("tp") ^ k) * width, width), width)


def prep_body(n, cap, *refs):
    weight_hbm = refs[0]
    far = refs[1:16]
    dec_r, dec_i, bt_r, bt_i, base, mix, choose, table = refs[16:24]
    flat = refs[24:28]
    weight, tokens = refs[28:30]
    held = refs[30:44]
    sems, weight_sems, fac = refs[44:]
    held = (*held, tokens)
    copies = [pltpu.make_async_copy(a, b, sems.at[i]) for i, (a, b) in enumerate(zip(far, held))]
    for copy in copies:
        copy.start()
    weights = load(weight_hbm, weight, weight_sems, n, weight.shape[2])
    copies[13].wait()
    routes = held[13]
    slots, count = table.shape
    top = routes.shape[0]
    names = lax.broadcasted_iota(jnp.int32, (16, count), 0)
    marks = [(routes[r : r + 1, :] == names).astype(f32) for r in range(top)]
    total = marks[0]
    for r in range(1, top):
        total = total + marks[r]
    row = lax.broadcasted_iota(jnp.int32, (count, count), 0)
    col = lax.broadcasted_iota(jnp.int32, (count, count), 1)
    before = dot(total.astype(bf16), (row < col).astype(bf16), NN)
    same = (row == col).astype(bf16)
    places = lax.broadcasted_iota(jnp.int32, (slots, count), 0).astype(f32)
    used = jnp.zeros((slots, count), f32)
    for r in range(top):
        rank = jnp.sum(before * marks[r], axis=0, keepdims=True)
        slot = routes[r : r + 1, :].astype(f32) * cap + rank
        hit = (places == slot).astype(f32)
        choose[r] = dot(same, hit.astype(bf16), NT).astype(bf16)
        used = used + hit
    table[...] = used.astype(bf16)
    st_r, st_i, in_r, in_i, om_r, om_i = held[:6]
    groups, inner, entries = in_r.shape
    pack = LANES // inner
    in_r, in_i, om_r, om_i = (x for x in held[2:6])
    for i in range(2, 6):
        copies[i].wait()
    for i in (0, 1, 10, 11, 12):
        copies[i].wait()
    real, imag, log_step = held[10][...], held[11][...], held[12][...]
    step = column(jnp.exp(log_step))
    size = jnp.exp(real * step)
    angle = imag * step
    bar_r = size * jnp.cos(angle)
    bar_i = size * jnp.sin(angle)
    modulus = real * real + imag * imag
    fac_r = ((bar_r - 1.0) * real + bar_i * imag) / modulus
    fac_i = (bar_i * real - (bar_r - 1.0) * imag) / modulus
    for g in range(groups):
        cols = slice(g * entries, (g + 1) * entries)
        s_r, s_i = st_r[:, g, :], st_i[:, g, :]
        b_r, b_i = bar_r[g : g + 1, :], bar_i[g : g + 1, :]
        dec_r[:, cols] = b_r * s_r - b_i * s_i
        dec_i[:, cols] = b_r * s_i + b_i * s_r
        fac[0:1, cols] = fac_r[g : g + 1, :]
        fac[1:2, cols] = fac_i[g : g + 1, :]
    high = pack * entries
    for b in range(groups // pack):
        each = slice(b * pack, (b + 1) * pack)
        lanes = slice(b * LANES, (b + 1) * LANES)
        rows = slice(b * high, (b + 1) * high)
        b_r, b_i, c_r, c_i = (
            spread(x[each].reshape(LANES, entries), inner, pack) for x in (in_r, in_i, om_r, om_i)
        )
        f_r, f_i = fac[0:1, rows], fac[1:2, rows]
        i_r = (f_r * b_r - f_i * b_i).astype(bf16)
        i_i = (f_r * b_i + f_i * b_r).astype(bf16)
        c_r, c_i = c_r.astype(bf16), c_i.astype(bf16)
        bt_r[lanes, :] = i_r
        bt_i[lanes, :] = i_i
        mix[lanes, :] = (dot(i_r, c_r, NT) - dot(i_i, c_i, NT)).astype(bf16)
        base[:, lanes] = dot(dec_r[:, rows].astype(bf16), c_r, NT) - dot(
            dec_i[:, rows].astype(bf16), c_i, NT
        )
    for i in range(len(flat)):
        copies[6 + i].wait()
        rows = held[6 + i][...].astype(f32)
        for r in range(rows.shape[0]):
            flat[i][0:1, r * LANES : (r + 1) * LANES] = rows[r : r + 1, :]
    copies[14].wait()
    for copy in weights:
        copy.wait()


def spread(blocks, height, pack):
    rows, inner = blocks.shape
    columns = pack * inner
    at = lax.broadcasted_iota(jnp.int32, (inner, columns), 0)
    to = lax.broadcasted_iota(jnp.int32, (inner, columns), 1)
    wide = dot(blocks.astype(bf16), (to % inner == at).astype(bf16), NN)
    row = lax.broadcasted_iota(jnp.int32, (rows, columns), 0)
    col = lax.broadcasted_iota(jnp.int32, (rows, columns), 1)
    return jnp.where(row // height == col // inner, wide, 0.0)


def load(src, dst, sems, n, width):
    copies = []
    for k in range(n):
        part = src.at[:, place(k, width)] if len(src.shape) == 2 else src.at[:, :, place(k, width)]
        copies.append(pltpu.make_async_copy(part, dst.at[k], sems.at[k]))
    for copy in copies:
        copy.start()
    return copies


def mixer_sums(n, odd, pieces, gain, weight, start):
    total, turned, square = start
    width = pieces[0].shape[1]
    for at, (k, piece) in enumerate(zip(crossings(n), pieces)):
        k = k ^ odd
        x = piece[...].astype(f32)
        square = square + fold(x * x)
        x = (x * gain[:, place(k, width)]).astype(bf16)
        if at % 2:
            turned = turned + dot(weight[k], x, NT)
        else:
            total = total + dot(x, weight[k], NT)
    return total, turned, square


def first_body(n, *refs):
    pieces = refs[: n // 2]
    gain, weight = refs[n // 2 : n // 2 + 2]
    for out, value in zip(refs[n // 2 + 2 :], mixer_sums(n, 0, pieces, gain, weight, (0.0, 0.0, 0.0))):
        out[...] = value


def mixer_body(n, *refs):
    pieces = refs[: n // 2]
    gain, weight, base, mix, skip, total, turned, square = refs[n // 2 : n // 2 + 8]
    driven_ref, act_ref = refs[n // 2 + 8 :]
    start = (total[...], turned[...], square[...])
    total, turned, square = mixer_sums(n, 1, pieces, gain, weight, start)
    width = pieces[0].shape[1]
    scale = lax.rsqrt(jnp.sum(square, axis=1, keepdims=True) / (n * width) + norm_eps)
    driven = ((total + turned.T) * scale).astype(bf16)
    driven_ref[...] = driven
    for b in range(driven.shape[1] // LANES):
        lanes = slice(b * LANES, (b + 1) * LANES)
        out = base[:, lanes] + dot(driven[:, lanes], mix[lanes, :], NN)
        out = out + skip[:, lanes] * driven[:, lanes].astype(f32)
        act_ref[:, lanes] = jax.nn.gelu(out).astype(bf16)


def state_body(driven, dec_r, dec_i, bt_r, bt_i, out_r, out_i):
    groups, entries = out_r.shape[1:]
    high = bt_r.shape[1]
    pack = high // entries
    for dec, bt, out in ((dec_r, bt_r, out_r), (dec_i, bt_i, out_i)):
        for b in range(groups // pack):
            lanes = slice(b * LANES, (b + 1) * LANES)
            new = dec[:, b * high : (b + 1) * high] + dot(driven[:, lanes], bt[lanes, :], NN)
            for g in range(pack):
                out[:, b * pack + g, :] = new[:, g * entries : (g + 1) * entries]


PARTS = 8


def fetch_body(spans, *refs):
    count = len(spans)
    copies = []
    for i, (low, high) in enumerate(spans):
        src, dst, sems = refs[i], refs[count + i], refs[2 * count + i]
        step = (high - low) // PARTS
        for p in range(PARTS):
            copies.append(
                pltpu.make_async_copy(
                    src.at[pl.ds(low + p * step, step)], dst.at[pl.ds(p * step, step)], sems.at[p]
                )
            )
            copies[-1].start()
    for copy in copies:
        copy.wait()


def fetch(*sources):
    sources = [x if isinstance(x, tuple) else (x, 0, x.shape[0]) for x in sources]
    return call(
        functools.partial(fetch_body, [x[1:] for x in sources]),
        [pltpu.VMEM((high - low, x.shape[1]), bf16) for x, low, high in sources],
        [FAR] * len(sources),
        [pltpu.SemaphoreType.DMA((PARTS,))] * len(sources),
        limit=2**20,
    )(*[stay(x) for x, _, _ in sources])


def rows_of(weight, i, experts):
    height = weight.shape[0] // experts
    return slice(i * height, (i + 1) * height)


def glu_sums(odd, pieces, glu, gate, turned):
    width = pieces[0].shape[1]
    for at, (k, piece) in enumerate(zip(crossings(2 * len(pieces)), pieces)):
        block = glu[:, place(k ^ odd, width)]
        if at % 2:
            turned = turned + dot(block, piece[...], NT)
        else:
            gate = gate + dot(piece[...], block, NT)
    return gate, turned


def gate_body(n, *refs):
    pieces = refs[: n // 2]
    glu, bias, gate_ref, turned_ref = refs[n // 2 :]
    gate_ref[...], turned_ref[...] = glu_sums(0, pieces, glu, bias[...], 0.0)


def glu_body(n, *refs):
    pieces = refs[: n // 2]
    own, glu, gate, turned, out_w = refs[n // 2 : n // 2 + 5]
    glued_ref, partner = refs[n // 2 + 5 :]
    gate, turned = glu_sums(1, pieces, glu, gate[...], turned[...])
    glued = (own[...].astype(f32) * jax.nn.sigmoid(gate + turned.T)).astype(bf16)
    glued_ref[...] = glued
    for at, k in enumerate(crossings(n)):
        partner[at] = dot(glued, out_w[:, place(k ^ 1, partner.shape[2])], NN).astype(bf16)


def out_body(n, glued, out_w, own):
    for at, k in enumerate(crossings(n)):
        own[at] = dot(glued[...], out_w[:, place(k, own.shape[2])], NN).astype(bf16)


def merge_body(*refs):
    out = refs[-1]
    cap = refs[0].shape[1]
    for j, x in enumerate(refs[:-1]):
        out[:, j * cap : (j + 1) * cap, :] = x[...]


def dispatch_body(m, terms, *refs):
    tokens = refs[0]
    sums = refs[1 : 1 + terms]
    table = refs[1 + terms]
    resid_ref = refs[2 + terms]
    outs = refs[3 + terms :]
    mixed = sums[0][...]
    for s in sums[1:]:
        mixed = mixed + s[...].astype(f32)
    resid = (tokens[...].astype(f32) + mixed).astype(bf16)
    resid_ref[...] = resid
    experts, cap, wide = outs[0].shape
    count = experts * cap
    for j in range(m):
        at = pl.multiple_of((lax.axis_index("ep") ^ j) * count, count)
        picked = dot(table[pl.ds(at, count), :], resid, NN).astype(bf16)
        outs[j][...] = picked.reshape(experts, cap, wide)


def expert_sums(odd, near, far, gain, gate_w, up_low, up_high, i, start):
    g, u, square = start
    experts, _, width = near[0].shape
    height = gate_w.shape[0] // experts
    held = up_low.shape[0] // height
    up_w, row = (up_low, i) if i < held else (up_high, i - held)
    for at, k in enumerate(crossings(2 * len(near))):
        k = k ^ odd
        x = jnp.concatenate([near[at][i], far[at][i]], axis=0).astype(f32)
        square = square + fold(x * x)
        x = (x * gain[:, place(k, width)]).astype(bf16)
        g = g + dot(x, gate_w[rows_of(gate_w, i, experts), place(k, width)], NT)
        u = u + dot(up_w[row * height : (row + 1) * height, place(k, width)], x, NT)
    return g, u, square


def even_body(n, *refs):
    near, far = refs[: n // 2], refs[n // 2 : n]
    gain, gate_w, up_low, up_high, g_ref, u_ref, square_ref = refs[n:]
    for i in range(near[0].shape[0]):
        g_ref[i], u_ref[i], square_ref[i] = expert_sums(
            1, near, far, gain, gate_w, up_low, up_high, i, (0.0, 0.0, 0.0)
        )


def up_body(n, *refs):
    near, far = refs[: n // 2], refs[n // 2 : n]
    gain, gate_w, up_low, up_high, down_w, g_ref, u_ref, square_ref = refs[n : n + 8]
    later, partner = refs[n + 8 :]
    experts, count, width = near[0].shape
    for i in range(experts):
        start = (g_ref[i], u_ref[i], square_ref[i])
        g, u, square = expert_sums(0, near, far, gain, gate_w, up_low, up_high, i, start)
        scale = lax.rsqrt(jnp.sum(square, axis=1, keepdims=True) / (n * width) + norm_eps)
        hidden = (jax.nn.silu(g * scale) * (u.T * scale)).astype(bf16)
        later[i] = hidden
        for at, k in enumerate(crossings(n)):
            block = down_w[rows_of(down_w, i, experts), place(k ^ 1, width)]
            partner[at, i] = dot(hidden[count:], block, NN).astype(bf16)


def down_body(n, hidden, down_w, far_own, own, partner):
    count, width = own.shape[2:]
    experts = hidden.shape[0]
    for i in range(experts):
        near, far = hidden[i, :count], hidden[i, count:]
        for at, k in enumerate(crossings(n)):
            block = down_w[rows_of(down_w, i, experts), place(k, width)]
            far_own[at, i] = dot(far, block, NN).astype(bf16)
            own[at, i] = dot(near, block, NN).astype(bf16)
        for at, k in enumerate(crossings(n)):
            block = down_w[rows_of(down_w, i, experts), place(k ^ 1, width)]
            partner[at, i] = dot(near, block, NN).astype(bf16)


def total_body(m, terms, *refs):
    sums = refs[:terms]
    outs = refs[terms:]
    total = sums[0][...]
    for s in sums[1:]:
        total = total + s[...].astype(f32)
    total = total.astype(bf16)
    cap = outs[0].shape[1]
    for j in range(m):
        outs[j][...] = total[:, j * cap : (j + 1) * cap, :]


def combine_body(m, *refs):
    resid, choose, weight = refs[:3]
    back = refs[3 : 3 + m]
    out, rows = refs[3 + m :]
    experts, cap, wide = back[0].shape
    count = experts * cap
    for j in range(m):
        at = pl.multiple_of((lax.axis_index("ep") ^ j) * count, count)
        rows[pl.ds(at, count), :] = back[j][...].reshape(count, wide)
    total = resid[...].astype(f32)
    for r in range(weight.shape[0]):
        picked = dot(choose[r], rows[...], NN)
        total = total + column(weight[r : r + 1, :]) * picked
    out[...] = total.astype(bf16)


def local_swaps(
    tokens,
    state_real,
    state_imag,
    mix_gain,
    in_weight,
    eig_real,
    eig_imag,
    log_step,
    input_real,
    input_imag,
    output_matrix_real,
    output_matrix_imag,
    skip_weight,
    glu_weight,
    glu_bias,
    out_weight,
    moe_gain,
    routes,
    route_weight,
    gate_weight,
    up_weight,
    down_weight,
):
    count, wide = tokens.shape
    n = lax.axis_size("tp")
    m = lax.axis_size("ep")
    groups, entries = eig_real.shape
    inner = input_real.shape[2]
    states = groups * entries
    channels = groups * inner
    full = wide * n
    exp_dev = gate_weight.shape[0]
    experts = exp_dev * m
    top = routes.shape[1]
    cap = max(2, (3 * top * count + 2 * experts - 1) // (2 * experts))
    slots = experts * cap

    pieces = gather_swaps(tokens, n)
    pack = LANES // inner
    far = [
        state_real,
        state_imag,
        input_real.transpose(0, 2, 1),
        input_imag.transpose(0, 2, 1),
        output_matrix_real,
        output_matrix_imag,
        skip_weight.reshape(-1, LANES),
        glu_bias.reshape(-1, LANES),
        mix_gain.reshape(-1, LANES),
        moe_gain.reshape(-1, LANES),
        eig_real,
        eig_imag,
        log_step.reshape(1, groups),
        routes.T,
        tokens,
    ]
    dec_r, dec_i, bt_r, bt_i, base, mix, choose, table, skip, bias, gain1, gain2, in_w, own = call(
        functools.partial(prep_body, n, cap),
        [jax.ShapeDtypeStruct((count, states), f32)] * 2
        + [jax.ShapeDtypeStruct((channels, pack * entries), bf16)] * 2
        + [
            jax.ShapeDtypeStruct((count, channels), f32),
            jax.ShapeDtypeStruct((channels, LANES), bf16),
            jax.ShapeDtypeStruct((top, count, slots), bf16),
            jax.ShapeDtypeStruct((slots, count), bf16),
        ]
        + [jax.ShapeDtypeStruct((1, channels), f32)] * 2
        + [jax.ShapeDtypeStruct((1, full), f32)] * 2
        + [pltpu.VMEM((n, channels, wide), bf16), pltpu.VMEM((count, wide), bf16)],
        [FAR] * 16,
        [pltpu.VMEM(x.shape, x.dtype) for x in far[:-1]]
        + [pltpu.SemaphoreType.DMA((15,)), pltpu.SemaphoreType.DMA((n,))]
        + [pltpu.VMEM((2, states), f32)],
        limit=12 * 2**20,
    )(*[stay(x) for x in [in_weight] + far])
    pieces[0] = own

    partial = call(
        functools.partial(first_body, n),
        [jax.ShapeDtypeStruct(x, f32) for x in ((count, channels), (channels, count), (count, LANES))],
        [WHOLE] * (n // 2 + 2),
        limit=8 * 2**20,
    )(*[pieces[k] for k in crossings(n)], gain1, in_w)
    driven, activated = call(
        functools.partial(mixer_body, n),
        [jax.ShapeDtypeStruct((count, channels), bf16)] * 2,
        [WHOLE] * (n // 2 + 8),
        limit=12 * 2**20,
    )(*[pieces[k ^ 1] for k in crossings(n)], gain1, in_w, base, mix, skip, *partial)

    acts = gather_swaps(activated, n)
    glu_w, out_w = fetch(glu_weight, out_weight)
    block = jax.ShapeDtypeStruct((n // 2, count, wide), bf16)
    partial = call(
        functools.partial(gate_body, n),
        [jax.ShapeDtypeStruct(x, f32) for x in ((count, channels), (channels, count))],
        [WHOLE] * (n // 2 + 2),
        limit=8 * 2**20,
    )(*[acts[k] for k in crossings(n)], glu_w, bias)
    glued, partner = call(
        functools.partial(glu_body, n),
        [jax.ShapeDtypeStruct((count, channels), bf16), block],
        [WHOLE] * (n // 2 + 5),
        limit=12 * 2**20,
    )(*[acts[k ^ 1] for k in crossings(n)], acts[0], glu_w, *partial, out_w)
    sums = call(functools.partial(out_body, n), block, [WHOLE] * 2, limit=8 * 2**20)(glued, out_w)

    terms = reduce_swaps(sums, partner, n)
    hidden = gate_weight.shape[1]
    flat_up = up_weight.reshape(-1, full)
    held = (exp_dev + 1) // 2 * hidden
    gate_w, up_low = fetch(gate_weight.reshape(-1, full), (flat_up, 0, held))
    (up_high,) = fetch((flat_up, held, exp_dev * hidden))
    (down_w,) = fetch(down_weight.reshape(-1, full))
    resid, *packed = call(
        functools.partial(dispatch_body, m, len(terms)),
        [jax.ShapeDtypeStruct((count, wide), bf16)]
        + [jax.ShapeDtypeStruct((exp_dev, cap, wide), bf16)] * m,
        [WHOLE] * (2 + len(terms)),
        limit=8 * 2**20,
    )(own, *terms, table)

    half = m // 2
    arrived = [packed[0]] + [swap(packed[j], "ep", j) for j in range(1, half)]
    arrived += [far_swap(packed[j], j) for j in range(half, m)]
    fragments = []
    for group in (arrived[:half], arrived[half:]):
        merged = call(
            merge_body,
            jax.ShapeDtypeStruct((exp_dev, half * cap, wide), bf16),
            [WHOLE] * half,
            limit=2**20,
        )(*group)
        fragments += gather_swaps(merged, n)
    part = jax.ShapeDtypeStruct((n // 2, exp_dev, half * cap, wide), bf16)
    near = fragments[:n]
    far = [fragments[n + (k ^ 1)] for k in range(n)]
    rows = 2 * half * cap
    weights = (gain2, gate_w, up_low, up_high)
    partial = call(
        functools.partial(even_body, n),
        [jax.ShapeDtypeStruct((exp_dev, *x), f32) for x in ((rows, hidden), (hidden, rows), (rows, LANES))],
        [WHOLE] * (n + 4),
        limit=8 * 2**20,
    )(*[near[k ^ 1] for k in crossings(n)], *[far[k ^ 1] for k in crossings(n)], *weights)
    later, far_partner = call(
        functools.partial(up_body, n),
        [jax.ShapeDtypeStruct((exp_dev, rows, hidden), bf16), part],
        [WHOLE] * (n + 8),
        limit=16 * 2**20,
    )(*[near[k] for k in crossings(n)], *[far[k] for k in crossings(n)], *weights, down_w, *partial)
    far_own, *near_outs = call(
        functools.partial(down_body, n), [part] * 3, [WHOLE] * 2, limit=8 * 2**20
    )(later, down_w)
    far_outs = [far_own, far_partner]
    back = [None] * m
    for outs, first in ((far_outs, half), (near_outs, 0)):
        terms = reduce_swaps(*outs, n)
        totals = call(
            functools.partial(total_body, half, len(terms)),
            [jax.ShapeDtypeStruct((exp_dev, cap, wide), bf16)] * half,
            [WHOLE] * len(terms),
            limit=4 * 2**20,
        )(*terms)
        for j in range(first, first + half):
            back[j] = swap(totals[j - first], "ep", j) if j else totals[0]
    new_r, new_i = call(
        state_body,
        [jax.ShapeDtypeStruct((count, groups, entries), f32)] * 2,
        [WHOLE] * 5,
        limit=4 * 2**20,
    )(driven, dec_r, dec_i, bt_r, bt_i)
    result = call(
        functools.partial(combine_body, m),
        jax.ShapeDtypeStruct((count, wide), bf16),
        [WHOLE] * (3 + m),
        [pltpu.VMEM((slots, wide), bf16)],
        limit=8 * 2**20,
    )(resid, choose, route_weight.T, *back)
    return (
        result,
        new_r,
        new_i,
    )


def ssm_step(
    driven,
    state_real,
    state_imag,
    eig_real,
    eig_imag,
    log_step,
    input_real,
    input_imag,
    output_matrix_real,
    output_matrix_imag,
    skip_weight,
):
    highest_precision = lax.Precision.HIGHEST
    count_of_rows = driven.shape[0]
    groups = eig_real.shape[0]
    group_width = input_real.shape[2]
    time_step = jnp.exp(log_step)[:, None]
    magnitude = jnp.exp(eig_real * time_step)
    angle_now = eig_imag * time_step
    bar_real = magnitude * jnp.cos(angle_now)
    bar_imag = magnitude * jnp.sin(angle_now)
    modulus = eig_real * eig_real + eig_imag * eig_imag
    fac_real = ((bar_real - 1.0) * eig_real + bar_imag * eig_imag) / modulus
    fac_imag = (bar_imag * eig_real - (bar_real - 1.0) * eig_imag) / modulus
    ib_real = fac_real[..., None] * input_real - fac_imag[..., None] * input_imag
    ib_imag = fac_real[..., None] * input_imag + fac_imag[..., None] * input_real
    grouped = driven.astype(jnp.float32).reshape(count_of_rows, groups, group_width)
    push_real = jnp.einsum("gpc,ngc->ngp", ib_real, grouped, precision=highest_precision)
    push_imag = jnp.einsum("gpc,ngc->ngp", ib_imag, grouped, precision=highest_precision)
    updated_state_real = bar_real[None] * state_real - bar_imag[None] * state_imag + push_real
    updated_state_imag = bar_real[None] * state_imag + bar_imag[None] * state_real + push_imag
    state_readout = jnp.einsum(
        "jiy,sjy->sji", output_matrix_real, updated_state_real, precision=highest_precision
    ) - jnp.einsum(
        "jiy,sjy->sji", output_matrix_imag, updated_state_imag, precision=highest_precision
    )
    state_readout = state_readout.reshape(count_of_rows, groups * group_width) + skip_weight[
        None, :
    ] * driven.astype(jnp.float32)
    activated = jax.nn.gelu(state_readout).astype(jnp.bfloat16)
    return (updated_state_real, updated_state_imag, activated)


def local(
    tokens,
    state_real,
    state_imag,
    mix_gain,
    in_weight,
    eig_real,
    eig_imag,
    log_step,
    input_real,
    input_imag,
    output_matrix_real,
    output_matrix_imag,
    skip_weight,
    glu_weight,
    glu_bias,
    out_weight,
    moe_gain,
    routes,
    route_weight,
    gate_weight,
    up_weight,
    down_weight,
):
    count_of_rows = tokens.shape[0]
    n_ep = lax.axis_size("ep")
    width_tp = lax.axis_size("tp")
    whole_rows = lax.all_gather(tokens, "tp", axis=1, tiled=True)
    whole_float = whole_rows.astype(jnp.float32)
    first_scale = lax.rsqrt(jnp.mean(whole_float * whole_float, axis=1, keepdims=True) + norm_eps)
    normed = (whole_float * first_scale * mix_gain.astype(jnp.float32)).astype(jnp.bfloat16)
    driven = jnp.einsum("rd,cd->rc", normed, in_weight, preferred_element_type=jnp.float32).astype(
        jnp.bfloat16
    )
    updated_state_real, updated_state_imag, activated = ssm_step(
        driven,
        state_real,
        state_imag,
        eig_real,
        eig_imag,
        log_step,
        input_real,
        input_imag,
        output_matrix_real,
        output_matrix_imag,
        skip_weight,
    )
    gate_pre = (
        jnp.einsum(
            "rc,oc->ro",
            lax.all_gather(activated, "tp", axis=1, tiled=True),
            glu_weight,
            preferred_element_type=jnp.float32,
        )
        + glu_bias
    )
    glued = (activated.astype(jnp.float32) * jax.nn.sigmoid(gate_pre)).astype(jnp.bfloat16)
    partial_value = jnp.dot(glued, out_weight, preferred_element_type=jnp.float32)
    mixed = lax.psum_scatter(
        partial_value.astype(jnp.bfloat16), "tp", scatter_dimension=1, tiled=True
    ).astype(jnp.float32)
    residual = (tokens.astype(jnp.float32) + mixed).astype(jnp.bfloat16)
    resid_float = residual.astype(jnp.float32)
    exp_dev = gate_weight.shape[0]
    experts = exp_dev * n_ep
    top_count = routes.shape[1]
    capacity = max(2, (3 * top_count * count_of_rows + 2 * experts - 1) // (2 * experts))
    chosen = routes.reshape(-1)
    onehot = (chosen[:, None] == jnp.arange(experts, dtype=jnp.int32)[None, :]).astype(jnp.int32)
    rank_index = jnp.sum((jnp.cumsum(onehot, axis=0) - onehot) * onehot, axis=1)
    slot_index = (chosen * capacity + rank_index).reshape(count_of_rows, top_count)
    slots_all = experts * capacity
    choose = slot_index[:, :, None] == jnp.arange(slots_all, dtype=jnp.int32)[None, None, :]
    dispatch = jnp.sum(choose.astype(jnp.float32), axis=1).astype(jnp.bfloat16)
    local_sq = jnp.sum(resid_float * resid_float, axis=1)
    total_sq = lax.psum(local_sq, "tp")
    dim_full = residual.shape[1] * width_tp
    second_scale = lax.rsqrt(total_sq[:, None] / dim_full + norm_eps)
    gain_part = lax.dynamic_slice_in_dim(
        moe_gain, lax.axis_index("tp") * residual.shape[1], residual.shape[1], 0
    )
    expert_in = (resid_float * second_scale * gain_part.astype(jnp.float32)).astype(jnp.bfloat16)
    packed = jnp.einsum(
        "rs,rd->sd", dispatch, expert_in, preferred_element_type=jnp.float32
    ).astype(jnp.bfloat16)
    packed = packed.reshape(n_ep, exp_dev * capacity, residual.shape[1])
    arrived = lax.all_to_all(packed, "ep", split_axis=0, concat_axis=0, tiled=True)
    arrived = arrived.reshape(n_ep, exp_dev, capacity, residual.shape[1])
    fragment = lax.all_gather(arrived, "tp", axis=3, tiled=True)
    gate_part = jnp.einsum(
        "necd,efd->necf", fragment, gate_weight, preferred_element_type=jnp.float32
    )
    up_part = jnp.einsum("necd,efd->necf", fragment, up_weight, preferred_element_type=jnp.float32)
    hidden_width = (jax.nn.silu(gate_part) * up_part).astype(jnp.bfloat16)
    partial_out = jnp.einsum(
        "necf,efd->necd", hidden_width, down_weight, preferred_element_type=jnp.float32
    )
    summed = lax.psum_scatter(
        partial_out.astype(jnp.bfloat16), "tp", scatter_dimension=3, tiled=True
    )
    summed = summed.reshape(n_ep, exp_dev * capacity, summed.shape[3])
    returned = lax.all_to_all(summed, "ep", split_axis=0, concat_axis=0, tiled=True)
    returned = returned.reshape(slots_all, returned.shape[2])
    gathered_k = jnp.einsum(
        "rks,sd->rkd", choose.astype(jnp.bfloat16), returned, preferred_element_type=jnp.float32
    )
    result = (resid_float + jnp.sum(route_weight[..., None] * gathered_k, axis=1)).astype(
        jnp.bfloat16
    )
    return (result, updated_state_real, updated_state_imag)


def solution(mesh):
    n, m = mesh.shape["tp"], mesh.shape["ep"]
    small = n in (4, 8) and m in (2, 4)

    def whole(*args):
        if not small:
            return local(*args)
        return local_swaps(*args)

    return jax.shard_map(
        whole,
        mesh=mesh,
        in_specs=(
            P("ep", "tp"),
            P("ep", "tp", None),
            P("ep", "tp", None),
            P(),
            P("tp", None),
            P("tp", None),
            P("tp", None),
            P("tp"),
            P("tp", None, None),
            P("tp", None, None),
            P("tp", None, None),
            P("tp", None, None),
            P("tp"),
            P("tp", None),
            P("tp"),
            P("tp", None),
            P(),
            P("ep", None),
            P("ep", None),
            P("ep", "tp", None),
            P("ep", "tp", None),
            P("ep", "tp", None),
        ),
        out_specs=(P("ep", "tp"), P("ep", "tp", None), P("ep", "tp", None)),
        check_vma=False,
    )
```
